512 devices in a mesh: sp: 16 (over z), fs: 4 (over y), tp: 8 (over x, core).
Axes of the slice: x: 4, y: 4, z: 16, core: 2. Of those that a mesh axis runs over, the one named last changes fastest.
Arguments:
- tokens: bfloat16 [4, 16384, 2048], P('fs', ('sp', 'tp')), may hold values from -6 to 6
- norm_gain: float32 [2048], replicated, may hold values from 0.1 to 1.9
- w_gate: bfloat16 [2048, 1024], P(('sp', 'fs'), 'tp'), may hold values from -0.125 to 0.125
- w_value: bfloat16 [2048, 1024], P(('sp', 'fs'), 'tp'), may hold values from -0.125 to 0.125
- w_bkey: bfloat16 [2048, 1024], P(('sp', 'fs'), 'tp'), may hold values from -0.125 to 0.125
- w_query: bfloat16 [2048, 1024], P(('sp', 'fs'), 'tp'), may hold values from -0.125 to 0.125
- w_pool_in: bfloat16 [2048, 1024], P(('sp', 'fs'), 'tp'), may hold values from -0.125 to 0.125
- w_step: bfloat16 [2048, 2, 16], replicated, may hold values from -0.125 to 0.125
- step_bias: float32 [2, 16], replicated, may hold values from -1 to 1
- decay_rate: float32 [2, 16], replicated, may hold values from 1.2207031e-06 to 0.06
- decay_shift: float32 [4, 16, 2, 16384], P('fs', 'tp', None, 'sp'), may hold values from 0 to 2.2
- conv_value: bfloat16 [5, 1024], replicated, may hold values from -2.5 to 2.5
- conv_bkey: bfloat16 [5, 1024], replicated, may hold values from -2.5 to 2.5
- conv_query: bfloat16 [5, 1024], replicated, may hold values from -2.5 to 2.5
- mix_gain: float32 [1024], replicated, may hold values from 0.1 to 1.9
- pool_mix: bfloat16 [8, 128, 128], replicated, may hold values from -0.5 to 0.5
- pool_gain: float32 [1024], replicated, may hold values from 0.1 to 1.9
- w_out_ssd: bfloat16 [1024, 2048], P('tp', ('sp', 'fs')), may hold values from -0.125 to 0.125
- w_out_pool: bfloat16 [1024, 2048], P('tp', ('sp', 'fs')), may hold values from -0.125 to 0.125
Outputs:
- mixed: bfloat16 [4, 16384, 2048], P('fs', ('sp', 'tp'))
The draws below stay inside these ranges and needn't reach their ends.
All inputs are finite; a program needn't handle non-finite values.
Results may differ from the reference program's by a relative error of at most 0.014.
Values may be sent and summed in bfloat16 or wider, within the bound.
A program may use at most 128 MiB of HBM per device.

```python
import jax
import jax.numpy as jnp
from jax import lax

D = 2048
HEAD_DIM = 64
DUALITY_HEADS = 16
GROUPS = 8
STATE = 128
CONV_WIDTH = 5
POOL_GROUPS = 8
POOL_DIM = 128
SPAN = 128
TOK_SP = 1024
SEQUENCE_LENGTH = 16384
BATCH_SEQUENCES = 4
D_SSM = 1024
D_POOL = 1024
N_TP = 8


def draw_decay_rate(key, part):
    order_key, slow_key, fast_key = jax.random.split(jax.random.fold_in(key, 11), 3)
    ranking = jax.random.permutation(order_key, 2 * DUALITY_HEADS)
    slow_count = DUALITY_HEADS
    slow_rate = jax.random.uniform(slow_key, (2 * DUALITY_HEADS,), jnp.float32, 0.02, 0.2) / SEQUENCE_LENGTH
    fast_rate = jax.random.uniform(fast_key, (2 * DUALITY_HEADS,), jnp.float32, 0.02, 0.06)
    rates = jnp.where(ranking < slow_count, slow_rate, fast_rate)
    return rates.reshape(2, DUALITY_HEADS).astype(jnp.float32)


def draw_decay_shift(key, part):
    random_keys = jax.random.split(jax.random.fold_in(key, 23), 4)
    token_position = jnp.arange(SEQUENCE_LENGTH, dtype=jnp.int32)
    segment = token_position // TOK_SP
    segments = SEQUENCE_LENGTH // TOK_SP
    low_end, high_end = (0.4, 2.5)
    factor = jnp.exp(jax.random.uniform(random_keys[0], (BATCH_SEQUENCES, DUALITY_HEADS, 2, segments), jnp.float32, jnp.log(low_end), jnp.log(high_end)))
    roughness = jax.random.uniform(random_keys[1], (BATCH_SEQUENCES, DUALITY_HEADS, 2, SEQUENCE_LENGTH), jnp.float32, 0.5, 1.5)
    reference_level = jnp.take(factor, segment, axis=3) * roughness * (0.3 / SEQUENCE_LENGTH)
    spike_places = jax.random.randint(random_keys[2], (BATCH_SEQUENCES, DUALITY_HEADS, 2, 3), 0, SEQUENCE_LENGTH)
    spike_length = jax.random.uniform(random_keys[3], (BATCH_SEQUENCES, DUALITY_HEADS, 2, 3), jnp.float32, 0.22, 0.69)
    match_count = (token_position[None, None, None, None, :] == spike_places[..., None]).astype(jnp.float32)
    spike_runs = jnp.sum(match_count * spike_length[..., None], axis=3)
    return (reference_level + spike_runs).astype(jnp.float32)


def levels(stream_key, shape, pieces, low, top_value):
    loudness = 1.0
    for dim, parts in pieces:
        steps = jax.random.uniform(jax.random.fold_in(jax.random.fold_in(stream_key, 6), dim), (parts,), jnp.float32, low / len(pieces), top_value / len(pieces))
        loudness = loudness * jnp.repeat(jnp.exp(steps), shape[dim] // parts).reshape((-1,) + (1,) * (len(shape) - 1 - dim))
    return loudness


def gaussian(own_key, extent, deviation, bound, cuts=(), held_as=jnp.bfloat16):
    array = deviation * jax.random.normal(own_key, extent, jnp.float32)
    if cuts:
        array = array * levels(own_key, extent, cuts, -0.22, 0.18)
    return jnp.clip(array, -bound, bound).astype(held_as)


def setup_inputs(seed: int = 0) -> dict:
    splits = jax.random.split(jax.random.key(seed), 20)
    tokens = gaussian(splits[0], (BATCH_SEQUENCES, SEQUENCE_LENGTH, D), 1.0, 6.0, ((0, 4), (1, 128)))
    norm_gain = jnp.clip(1.0 + 0.18 * jax.random.normal(splits[1], (D,), jnp.float32), 0.1, 1.9)
    w_gate = gaussian(splits[2], (D, D_SSM), D ** -0.5, 0.125, ((0, 64), (1, 8)))
    w_value = gaussian(splits[3], (D, D_SSM), D ** -0.5, 0.125, ((0, 64), (1, 8)))
    w_bkey = gaussian(splits[4], (D, GROUPS * STATE), D ** -0.5, 0.125, ((0, 64), (1, 8)))
    w_query = gaussian(splits[5], (D, GROUPS * STATE), D ** -0.5, 0.125, ((0, 64), (1, 8)))
    w_pool_in = gaussian(splits[6], (D, D_POOL), D ** -0.5, 0.125, ((0, 64), (1, 8)))
    w_step = gaussian(splits[7], (D, 2, DUALITY_HEADS), D ** -0.5, 0.125)
    step_bias = jnp.clip(jax.random.uniform(splits[8], (2, DUALITY_HEADS), jnp.float32, -1.0, 1.0), -1.0, 1.0)
    decay_rate = draw_decay_rate(jax.random.fold_in(splits[19], 71), 0)
    decay_shift = draw_decay_shift(jax.random.fold_in(splits[19], 71), 0)
    conv_value = gaussian(splits[11], (CONV_WIDTH, D_SSM), CONV_WIDTH ** -0.5, 2.5)
    conv_bkey = gaussian(splits[12], (CONV_WIDTH, GROUPS * STATE), CONV_WIDTH ** -0.5, 2.5)
    conv_query = gaussian(splits[13], (CONV_WIDTH, GROUPS * STATE), CONV_WIDTH ** -0.5, 2.5)
    mix_gain = jnp.clip(1.0 + 0.18 * jax.random.normal(splits[14], (D_SSM,), jnp.float32), 0.1, 1.9)
    pool_mix = gaussian(splits[15], (POOL_GROUPS, POOL_DIM, POOL_DIM), POOL_DIM ** -0.5, 0.5)
    pool_gain = jnp.clip(1.0 + 0.18 * jax.random.normal(splits[16], (D_POOL,), jnp.float32), 0.1, 1.9)
    w_out_ssd = gaussian(splits[17], (D_SSM, D), (D_SSM + D_POOL) ** -0.5, 0.125, ((0, 8), (1, 64)))
    w_out_pool = gaussian(splits[18], (D_POOL, D), (D_SSM + D_POOL) ** -0.5, 0.125, ((0, 8), (1, 64)))
    return {"tokens": tokens, "norm_gain": norm_gain, "w_gate": w_gate, "w_value": w_value, "w_bkey": w_bkey, "w_query": w_query, "w_pool_in": w_pool_in, "w_step": w_step, "step_bias": step_bias, "decay_rate": decay_rate, "decay_shift": decay_shift, "conv_value": conv_value, "conv_bkey": conv_bkey, "conv_query": conv_query, "mix_gain": mix_gain, "pool_mix": pool_mix, "pool_gain": pool_gain, "w_out_ssd": w_out_ssd, "w_out_pool": w_out_pool}


EPSILON = 1e-06
HIGHEST = lax.Precision.HIGHEST
WINDOWS = (2, 4, 8, 16)

def blockwise(values, bkeys, queries, steps, logs):
    length, heads, head_width = values.shape
    groups, state_width = (bkeys.shape[1], bkeys.shape[2])
    per_group = heads // groups
    blocks = length // SPAN
    weighted = (values * jnp.transpose(steps)[:, :, None]).reshape(blocks, SPAN, groups, per_group, head_width)
    key_blocks = bkeys.reshape(blocks, SPAN, groups, state_width)
    query_blocks = queries.reshape(blocks, SPAN, groups, state_width)
    inner = jnp.cumsum(logs.reshape(heads, blocks, SPAN), axis=-1)
    lower = jnp.tril(jnp.ones((SPAN, SPAN), dtype=bool))
    within = jnp.exp(jnp.where(lower, inner[..., :, None] - inner[..., None, :], -jnp.inf))
    within = within.reshape(groups, per_group, blocks, SPAN, SPAN)
    scores = jnp.einsum('clgn,csgn->cgls', query_blocks, key_blocks, precision=HIGHEST)
    diagonal = jnp.einsum('cgls,gkcls,csgkp->clgkp', scores, within, weighted, precision=HIGHEST)
    tails = jnp.exp(inner[..., -1:] - inner).reshape(groups, per_group, blocks, SPAN)
    ends = jnp.einsum('clgn,gkcl,clgkp->cgkpn', key_blocks, tails, weighted, precision=HIGHEST)
    totals = inner[..., -1]
    upto = jnp.cumsum(totals, axis=-1)
    before = upto - totals
    block_ids = jnp.arange(blocks, dtype=jnp.int32)
    earlier = block_ids[None, :] < block_ids[:, None]
    between = jnp.exp(jnp.where(earlier[None], before[:, :, None] - upto[:, None, :], -jnp.inf))
    between = between.reshape(groups, per_group, blocks, blocks)
    prior = jnp.einsum('gkcj,jgkpn->cgkpn', between, ends, precision=HIGHEST)
    reach = jnp.exp(inner).reshape(groups, per_group, blocks, SPAN)
    offdiag = jnp.einsum('clgn,cgkpn,gkcl->clgkp', query_blocks, prior, reach, precision=HIGHEST)
    return (diagonal + offdiag).reshape(length, heads, head_width)

def centred(projected, taps):
    margin = CONV_WIDTH // 2
    length = projected.shape[0]
    padded = jnp.pad(projected, ((margin, margin), (0, 0)))
    running = jnp.zeros(projected.shape, jnp.float32)
    for offset in range(CONV_WIDTH):
        running = running + padded[offset:offset + length].astype(jnp.float32) * taps[offset].astype(jnp.float32)
    return running

def box_mean(column, window):
    length = column.shape[0]
    prefix = jnp.pad(jnp.cumsum(column, axis=0), ((1, 0), (0, 0)))
    where_now = jnp.arange(length, dtype=jnp.int32)
    lower = jnp.clip(where_now - window // 2, 0, length).astype(jnp.int32)
    upper = jnp.clip(where_now + window - window // 2, 0, length).astype(jnp.int32)
    counts = (upper - lower).astype(jnp.float32)
    return (prefix[upper] - prefix[lower]) / counts[:, None]

def reference(tokens, norm_gain, w_gate, w_value, w_bkey, w_query, w_pool_in, w_step, step_bias, decay_rate, decay_shift, conv_value, conv_bkey, conv_query, mix_gain, pool_mix, pool_gain, w_out_ssd, w_out_pool):

    def one_sequence(paired):
        rows, shift = paired
        length = rows.shape[0]
        widened = rows.astype(jnp.float32)
        normed = (widened * lax.rsqrt(lax.optimization_barrier(jnp.mean(widened * widened, axis=-1, keepdims=True)) + EPSILON) * norm_gain).astype(jnp.bfloat16)
        gate = jnp.dot(normed, w_gate, preferred_element_type=jnp.float32).astype(jnp.bfloat16)
        value = jnp.dot(normed, w_value, preferred_element_type=jnp.float32).astype(jnp.bfloat16)
        bkey = jnp.dot(normed, w_bkey, preferred_element_type=jnp.float32).astype(jnp.bfloat16)
        query = jnp.dot(normed, w_query, preferred_element_type=jnp.float32).astype(jnp.bfloat16)
        pooled = jnp.dot(normed, w_pool_in, preferred_element_type=jnp.float32).astype(jnp.bfloat16)
        raw_steps = jnp.dot(normed, w_step.reshape(D, 2 * DUALITY_HEADS), preferred_element_type=jnp.float32)
        steps = jax.nn.softplus(raw_steps.reshape(length, 2, DUALITY_HEADS) + step_bias).transpose(1, 2, 0)
        logs = -decay_rate[:, :, None] * steps - shift.transpose(1, 0, 2)
        values = jax.nn.silu(centred(value, conv_value)).reshape(length, DUALITY_HEADS, HEAD_DIM)
        bkeys = jax.nn.silu(centred(bkey, conv_bkey)).reshape(length, GROUPS, STATE)
        queries = jax.nn.silu(centred(query, conv_query)).reshape(length, GROUPS, STATE)
        forward = blockwise(values, bkeys, queries, steps[0], logs[0])
        backward = blockwise(values[::-1], bkeys[::-1], queries[::-1], steps[1][:, ::-1], logs[1][:, ::-1])[::-1]
        heads_out = forward + backward
        gated = heads_out.reshape(length, D_SSM) * jax.nn.silu(gate.astype(jnp.float32))
        ssd_mix = (gated * lax.rsqrt(lax.optimization_barrier(jnp.mean(gated * gated, axis=-1, keepdims=True)) + EPSILON) * mix_gain).astype(jnp.bfloat16)
        pool_rows = pooled.astype(jnp.float32).reshape(length, POOL_GROUPS, POOL_DIM)
        differences = []
        for group in range(POOL_GROUPS):
            column = pool_rows[:, group]
            differences.append(box_mean(column, WINDOWS[group % 4]) - column)
        pool_diff = jnp.stack(differences, axis=1).astype(jnp.bfloat16)
        mapped = jnp.einsum('sgc,gcd->sgd', pool_diff.astype(jnp.float32), pool_mix.astype(jnp.float32))
        pool_out = (mapped.reshape(length, D_POOL) * pool_gain).astype(jnp.bfloat16)
        ssd_part = D_SSM // N_TP
        pool_part = D_POOL // N_TP
        summed = jnp.zeros((length, D), jnp.float32)
        for member in range(N_TP):
            partial_value = jnp.dot(ssd_mix[:, member * ssd_part:(member + 1) * ssd_part], w_out_ssd[member * ssd_part:(member + 1) * ssd_part], preferred_element_type=jnp.float32)
            partial_value = partial_value + jnp.dot(pool_out[:, member * pool_part:(member + 1) * pool_part], w_out_pool[member * pool_part:(member + 1) * pool_part], preferred_element_type=jnp.float32)
            rounded = lax.optimization_barrier(partial_value.astype(jnp.bfloat16))
            summed = summed + rounded.astype(jnp.float32)
        return summed.astype(jnp.bfloat16)
    return lax.map(one_sequence, (tokens, decay_shift))
```

```python
import functools

import jax
import jax.numpy as jnp
from jax import lax
from jax.experimental import pallas as pl
from jax.experimental.pallas import tpu as pltpu
from jax.sharding import PartitionSpec as P

HEAD_DIM = 64
DUALITY_HEADS = 16
GROUPS = 8
STATE = 128
CONV_WIDTH = 5
POOL_GROUPS = 8
POOL_DIM = 128
SPAN = 128
REACH = 8
D_SSM = 1024


EPSILON = 1e-06
HIGHEST = lax.Precision.HIGHEST
WINDOWS = (2, 4, 8, 16)

MESH = pl.DeviceIdType.MESH
A_COLS = 384
W_COLS = 896
HALO = 16
TOK_ROWS = 128
PIECE = 32


def remote(src, dst, send, recv, where):
    return pltpu.make_async_remote_copy(
        src_ref=src, dst_ref=dst, send_sem=send, recv_sem=recv, device_id=where, device_id_type=MESH
    )


def entry_barrier(places):
    barrier = pltpu.get_barrier_semaphore()
    for where in places:
        pl.semaphore_signal(barrier, inc=1, device_id=where, device_id_type=MESH)
    pl.semaphore_wait(barrier, len(places))


def gather_kernel(
    n_sp, n_fs, n_x,
    tok, wg, wv, wk, wq, wp, wo, wstep, gain,
    proj, raw, wout,
    tokbuf, wbuf,
    local_sem, out_sem,
    tp_sem, tm_sem, tr_sem, td_sem,
    ay_sem, azp_sem, azm_sem, bzp_sem, bzm_sem, byp_sem, bym_sem, byo_sem, h_sem,
    send_sem,
):
    z, y, t = lax.axis_index("sp"), lax.axis_index("fs"), lax.axis_index("tp")
    x, c = t // 2, t % 2
    xp, xm = (x + 1) % n_x, (x + n_x - 1) % n_x
    yp, ym = (y + 1) % n_fs, (y + n_fs - 1) % n_fs
    zp, zm = (z + 1) % n_sp, (z + n_sp - 1) % n_sp
    to_xp, to_xm, to_d = {"tp": xp * 2 + c}, {"tp": xm * 2 + c}, {"tp": x * 2 + 1 - c}
    to_yp, to_ym = {"fs": yp}, {"fs": ym}
    to_zp, to_zm = {"sp": zp}, {"sp": zm}

    def trow(xx, cc, q):
        return pl.multiple_of(HALO + (xx * 2 + cc) * TOK_ROWS + q * PIECE, 16)

    def wrow(zz, yy):
        return pl.multiple_of((zz * n_fs + yy) * PIECE, PIECE)

    def a_at(zz, yy):
        return wbuf.at[pl.ds(wrow(zz, yy), PIECE), pl.ds(0, A_COLS)]

    def b_at(zz, yy):
        return wbuf.at[pl.ds(wrow(zz, yy), PIECE), pl.ds(A_COLS, W_COLS - A_COLS)]

    def t_at(xx, cc, q, rows=PIECE):
        return tokbuf.at[pl.ds(trow(xx, cc, q), rows), :]

    locals_ = [pltpu.make_async_copy(tok.at[0], t_at(x, c, 0, TOK_ROWS), local_sem.at[0])]
    for i, w in enumerate((wg, wv, wk, wq, wp)):
        locals_.append(
            pltpu.make_async_copy(
                w, wbuf.at[pl.ds(wrow(z, y), PIECE), pl.ds(i * 128, 128)], local_sem.at[1 + i]
            )
        )
    locals_.append(
        pltpu.make_async_copy(
            wo, wbuf.at[pl.ds(wrow(z, y), PIECE), pl.ds(640, 256)], local_sem.at[6]
        )
    )
    for copy in locals_:
        copy.start()
    entry_barrier((to_xp, to_xm, to_yp, to_ym, to_zp, to_zm, to_d))

    sent = []

    def send(ref, recv, where):
        copy = remote(ref, ref, send_sem.at[len(sent)], recv, where)
        copy.start()
        sent.append(copy)

    def arrived(ref, recv):
        remote(ref, ref, send_sem.at[0], recv, to_d).wait_recv()

    for copy in locals_[1:]:
        copy.wait()
    own_a, own_b = a_at(z, y), b_at(z, y)
    send(own_a, ay_sem.at[0], to_yp)
    send(own_a, ay_sem.at[1], to_ym)
    send(own_a, azp_sem.at[4], to_zp)
    send(own_a, azm_sem.at[4], to_zm)
    send(own_b, bzp_sem.at[1], to_zp)
    send(own_b, bzm_sem.at[1], to_zm)
    locals_[0].wait()
    for q in (0, 1, 2, 3):
        send(t_at(x, c, q), tp_sem.at[q], to_xp)
    for q in (2, 3, 0, 1):
        send(t_at(x, c, q), tm_sem.at[q], to_xm)
    send(own_b, byp_sem.at[0], to_yp)
    send(own_b, bym_sem.at[0], to_ym)
    send(t_at(x, c, 0, TOK_ROWS), td_sem.at[12], to_d)

    yo = (y + 2) % n_fs
    y_of = (y, ym, yp, yo)
    arrived(a_at(z, ym), ay_sem.at[0])
    send(a_at(z, ym), ay_sem.at[2], to_yp)
    send(a_at(z, ym), azp_sem.at[5], to_zp)
    send(a_at(z, ym), azm_sem.at[5], to_zm)
    arrived(a_at(z, yp), ay_sem.at[1])
    send(a_at(z, yp), azp_sem.at[6], to_zp)
    send(a_at(z, yp), azm_sem.at[6], to_zm)
    arrived(a_at(z, yo), ay_sem.at[2])
    send(a_at(z, yo), azp_sem.at[7], to_zp)
    send(a_at(z, yo), azm_sem.at[7], to_zm)

    half = n_sp // 2

    def back(o):
        return (z + n_sp - o) % n_sp

    def relay_y(o):
        arrived(b_at(back(o), ym), byp_sem.at[o])
        if o % 2 == 0:
            send(b_at(back(o), ym), byo_sem.at[o], to_yp)
        arrived(b_at(back(o), yp), bym_sem.at[o])
        if o % 2 == 1:
            send(b_at(back(o), yp), byo_sem.at[o], to_ym)

    def token_step(k):
        if k <= 4:
            q = k - 1
            arrived(t_at(xm, c, q), tp_sem.at[q])
            if q < 2:
                send(t_at(xm, c, q), tr_sem.at[q], to_xp)
            send(t_at(xm, c, q), td_sem.at[q], to_d)
            q = (2, 3, 0, 1)[k - 1]
            arrived(t_at(xp, c, q), tm_sem.at[q])
            if q >= 2:
                send(t_at(xp, c, q), tr_sem.at[q], to_xm)
            send(t_at(xp, c, q), td_sem.at[4 + q], to_d)
        elif k <= 6:
            for q in (k - 5, k - 3):
                xo = (x + 2) % n_x
                arrived(t_at(xo, c, q), tr_sem.at[q])
                send(t_at(xo, c, q), td_sem.at[8 + q], to_d)

    pending = [0]
    for k in range(1, half + 1):
        far = k == half
        for j in range(4):
            if not far or j < 2:
                ref = a_at(back(k), y_of[j])
                arrived(ref, azp_sem.at[4 * k + j])
                if k + 1 < half or (k + 1 == half and j < 2):
                    send(ref, azp_sem.at[4 * (k + 1) + j], to_zp)
            if not far or j >= 2:
                ref = a_at((z + k) % n_sp, y_of[j])
                arrived(ref, azm_sem.at[4 * k + j])
                if k + 1 < half or (k + 1 == half and j >= 2):
                    send(ref, azm_sem.at[4 * (k + 1) + j], to_zm)
            if j == 1:
                token_step(k)
        fresh = []
        ref = b_at(back(k), y)
        arrived(ref, bzp_sem.at[k])
        if k < half:
            send(ref, bzp_sem.at[k + 1], to_zp)
        send(ref, byp_sem.at[k], to_yp)
        send(ref, bym_sem.at[k], to_ym)
        fresh.append(k)
        if not far:
            o = n_sp - k
            ref = b_at(back(o), y)
            arrived(ref, bzm_sem.at[k])
            if k + 1 < half:
                send(ref, bzm_sem.at[k + 1], to_zm)
            send(ref, byp_sem.at[o], to_yp)
            send(ref, bym_sem.at[o], to_ym)
            fresh.append(o)
        for o in pending:
            relay_y(o)
        pending = fresh

    cs = 1 - c
    arrived(t_at(x, cs, 0, TOK_ROWS), td_sem.at[12])
    for q in range(4):
        arrived(t_at(xm, cs, q), td_sem.at[q])
        arrived(t_at(xp, cs, q), td_sem.at[4 + q])
        arrived(t_at((x + 2) % n_x, cs, q), td_sem.at[8 + q])
    rows = 2 * n_x * TOK_ROWS
    last = tokbuf.at[pl.ds(rows, HALO), :]
    first = tokbuf.at[pl.ds(HALO, HALO), :]
    before = tokbuf.at[pl.ds(0, HALO), :]
    after = tokbuf.at[pl.ds(HALO + rows, HALO), :]
    halo_up = remote(last, before, send_sem.at[len(sent)], h_sem.at[0], to_zp)
    halo_up.start()
    sent.append(halo_up)
    halo_down = remote(first, after, send_sem.at[len(sent)], h_sem.at[1], to_zm)
    halo_down.start()
    sent.append(halo_down)
    for o in pending:
        relay_y(o)
    for o in range(n_sp):
        arrived(b_at(back(o), yo), byo_sem.at[o])
    to_out = pltpu.make_async_copy(wbuf.at[:, pl.ds(640, 256)], wout, out_sem)
    to_out.start()

    def project(begin, count):
        part = tokbuf[pl.ds(begin, count), :].astype(jnp.float32)
        scaling = lax.rsqrt(jnp.mean(part * part, axis=-1, keepdims=True) + EPSILON)
        normed = (part * scaling * gain[...]).astype(jnp.bfloat16)
        proj[pl.ds(begin, count), :] = jnp.dot(
            normed, wbuf[:, 0:640], preferred_element_type=jnp.float32
        ).astype(jnp.bfloat16)
        return normed

    def step(i, carry):
        begin = pl.multiple_of(HALO + i * 256, 16)
        normed = project(begin, 256)
        raw[pl.ds(pl.multiple_of(i * 256, 256), 256), :] = jnp.dot(
            normed, wstep[...], preferred_element_type=jnp.float32
        )
        return carry

    lax.fori_loop(0, rows // 256, step, 0)
    remote(before, before, send_sem.at[0], h_sem.at[0], to_d).wait_recv()
    remote(after, after, send_sem.at[0], h_sem.at[1], to_d).wait_recv()
    project(0, HALO)
    project(HALO + rows, HALO)
    to_out.wait()
    for copy in sent:
        copy.wait_send()


N_SENDS = 191


def gather_and_project(n_sp, n_fs, n_x, tok, ws, wo, wstep, gain):
    rows = 2 * n_x * TOK_ROWS
    any_spec = pl.BlockSpec(memory_space=pl.ANY)
    vmem = pl.BlockSpec(memory_space=pltpu.VMEM)
    dma = pltpu.SemaphoreType.DMA
    return pl.pallas_call(
        functools.partial(gather_kernel, n_sp, n_fs, n_x),
        out_shape=(
            jax.ShapeDtypeStruct((rows + 2 * HALO, 640), jnp.bfloat16),
            jax.ShapeDtypeStruct((rows, 128), jnp.float32),
            jax.ShapeDtypeStruct((2048, 256), jnp.bfloat16),
        ),
        in_specs=[any_spec] * 7 + [vmem, vmem],
        out_specs=(vmem, vmem, any_spec),
        scratch_shapes=[
            pltpu.VMEM((rows + 2 * HALO, 2048), jnp.bfloat16),
            pltpu.VMEM((2048, W_COLS), jnp.bfloat16),
            dma((7,)),
            dma,
            dma((4,)), dma((4,)), dma((4,)), dma((13,)),
            dma((3,)), dma((36,)), dma((36,)), dma((9,)), dma((9,)),
            dma((16,)), dma((16,)), dma((16,)), dma((2,)),
            dma((N_SENDS,)),
        ],
        compiler_params=pltpu.CompilerParams(
            collective_id=0, has_side_effects=True, vmem_limit_bytes=48 * 1024 * 1024
        ),
        name="gather_and_project",
    )(tok, *ws, wo, wstep, gain)


def turned_gather(arrays, axis, dims):
    turned = [jnp.moveaxis(a, dim, 0) for a, dim in zip(arrays, dims)]
    both = jnp.concatenate([t.reshape(len(t), -1) for t in turned], axis=1)
    out, at, gathered = (lax.all_gather(both, axis, axis=0, tiled=True), 0, [])
    for t, dim in zip(turned, dims):
        slab = out[:, at : at + t[0].size].reshape(-1, *t.shape[1:])
        gathered.append(jnp.moveaxis(slab, 0, dim))
        at += t[0].size
    return tuple(gathered)


def padded_2(cells, sides, width):
    for axis, dim in sides:
        count = lax.axis_size(axis)
        ends = count - 1
        head = lax.slice_in_dim(cells, 0, width, axis=dim)
        tail = lax.slice_in_dim(cells, cells.shape[dim] - width, cells.shape[dim], axis=dim)
        cells = jnp.concatenate(
            [
                lax.ppermute(tail, axis, [(i, (i + 1) % count) for i in range(ends)]),
                cells,
                lax.ppermute(head, axis, [((i + 1) % count, i) for i in range(ends)]),
            ],
            axis=dim,
        )
    return cells


def from_everyone(x, axis):
    length = lax.axis_size(axis)
    return lax.all_to_all(jnp.broadcast_to(x[None], (length, *x.shape)), axis, 0, 0, tiled=True)


def gathered_once(x, axis):
    leaves = jax.tree.leaves(x)
    sequence = sorted(range(len(leaves)), key=lambda k: -leaves[k].size)
    width = (1, *leaves[sequence[0]].shape)[-1]
    lines = [
        jnp.pad(leaves[k].reshape(-1), (0, -leaves[k].size % width)).reshape(-1, width)
        for k in sequence
    ]
    both, at, found = (from_everyone(jnp.concatenate(lines), axis), 0, {})
    for k, line in zip(sequence, lines):
        slab = both[:, at : at + len(line)].reshape(len(both), -1)
        found[k] = slab[:, : leaves[k].size].reshape(-1, *leaves[k].shape)
        at += len(line)
    numbers = iter(range(len(leaves)))
    return jax.tree.map(lambda _: found[next(numbers)], x)


def joined_by_halves(pieces, combine):
    while len(jax.tree.leaves(pieces)[0]) > 1:
        pieces = jax.vmap(combine)(
            *(jax.tree.map(lambda part: part[side::2], pieces) for side in (0, 1))
        )
    return jax.tree.map(lambda part: part[0], pieces)


def carried_in(x, axis, combine, identity, reverse):
    length, here = (lax.axis_size(axis), lax.axis_index(axis))
    passed = jnp.arange(length) > here if reverse else jnp.arange(length) < here

    def kept(part, zero, own):
        part = jnp.where(
            passed.reshape(-1, *(1 for _ in own.shape)),
            part.astype(own.dtype),
            jnp.asarray(zero, own.dtype),
        )
        return part[::-1] if reverse else part

    pieces = gathered_once(
        jax.tree.map(lambda part, kind: part.astype(kind), x, (jnp.bfloat16, jnp.bfloat16)), axis
    )
    return joined_by_halves(jax.tree.map(kept, pieces, identity, x), combine)


def over_copies(x, axis):
    return from_everyone(x, axis).sum(axis=0)


def cut_along(x, dim, length):
    before, after = (x.shape[:dim], x.shape[dim + 1 :])
    return jnp.moveaxis(x.reshape(*before, length, -1, *after), dim, 0)


def sent_and_summed(x, axis, dim):
    tiles = cut_along(x, dim, lax.axis_size(axis))
    arrived = lax.all_to_all(tiles, axis, split_axis=0, concat_axis=0, tiled=True)
    return arrived.astype(jnp.float32).sum(axis=0)


def local_pass(values, bkeys, queries, steps, logs):
    length, heads, head_width = values.shape
    groups, state_width = (bkeys.shape[1], bkeys.shape[2])
    per_group = heads // groups
    blocks = length // SPAN
    weighted = (values * jnp.transpose(steps)[:, :, None]).reshape(
        blocks, SPAN, groups, per_group, head_width
    )
    key_blocks = bkeys.reshape(blocks, SPAN, groups, state_width)
    query_blocks = queries.reshape(blocks, SPAN, groups, state_width)
    inner = jnp.cumsum(logs.reshape(heads, blocks, SPAN), axis=-1)
    lower = jnp.tril(jnp.ones((SPAN, SPAN), dtype=bool))
    within = jnp.exp(jnp.where(lower, inner[..., :, None] - inner[..., None, :], -jnp.inf))
    within = within.reshape(groups, per_group, blocks, SPAN, SPAN)
    scores = jnp.einsum("clgn,csgn->cgls", query_blocks, key_blocks, precision=HIGHEST)
    diagonal = jnp.einsum("cgls,gkcls,csgkp->clgkp", scores, within, weighted, precision=HIGHEST)
    tails = jnp.exp(inner[..., -1:] - inner).reshape(groups, per_group, blocks, SPAN)
    ends = jnp.einsum("clgn,gkcl,clgkp->cgkpn", key_blocks, tails, weighted, precision=HIGHEST)
    totals = inner[..., -1]
    upto = jnp.cumsum(totals, axis=-1)
    before = upto - totals
    block_ids = jnp.arange(blocks, dtype=jnp.int32)
    earlier = block_ids[None, :] < block_ids[:, None]
    between = jnp.exp(jnp.where(earlier[None], before[:, :, None] - upto[:, None, :], -jnp.inf))
    between = between.reshape(groups, per_group, blocks, blocks)
    prior = jnp.einsum("gkcj,jgkpn->cgkpn", between, ends, precision=HIGHEST)
    reach = jnp.exp(inner).reshape(groups, per_group, blocks, SPAN)
    offdiag = jnp.einsum("clgn,cgkpn,gkcl->clgkp", query_blocks, prior, reach, precision=HIGHEST)
    outputs = (diagonal + offdiag).reshape(length, heads, head_width)
    last_weight = jnp.exp(upto[:, -1:] - upto).reshape(groups, per_group, blocks)
    final = jnp.einsum("gkj,jgkpn->gkpn", last_weight, ends, precision=HIGHEST)
    final = final.reshape(heads, head_width, state_width)
    token_position = (before[:, :, None] + inner).reshape(heads, length)
    return (outputs, final, upto[:, -1], token_position)


def apply_carry(queries, incoming, token_position):
    length, groups, state_width = queries.shape
    heads, head_width = (incoming.shape[0], incoming.shape[1])
    per_group = heads // groups
    reach = jnp.exp(token_position).reshape(groups, per_group, length)
    carried = jnp.einsum(
        "lgn,gkpn,gkl->lgkp",
        queries,
        incoming.reshape(groups, per_group, head_width, state_width),
        reach,
        precision=HIGHEST,
    )
    return carried.reshape(length, heads, head_width)


def chain_combine(earlier, later):
    return (earlier[0] + later[0], jnp.exp(later[0])[:, None, None] * earlier[1] + later[1])


def local(
    tokens,
    norm_gain,
    w_gate,
    w_value,
    w_bkey,
    w_query,
    w_pool_in,
    w_step,
    step_bias,
    decay_rate,
    decay_shift,
    conv_value,
    conv_bkey,
    conv_query,
    mix_gain,
    pool_mix,
    pool_gain,
    w_out_ssd,
    w_out_pool,
):
    tp_count = lax.axis_size("tp")
    sp_count = lax.axis_size("sp")
    tp_rank = lax.axis_index("tp")
    sp_rank = lax.axis_index("sp")
    heads_dev = DUALITY_HEADS // tp_count
    groups_dev = GROUPS // tp_count
    pools_dev = POOL_GROUPS // tp_count
    width_ssd = heads_dev * HEAD_DIM
    width_key = groups_dev * STATE
    width_pool = pools_dev * POOL_DIM
    step_cols = lax.dynamic_slice_in_dim(w_step, tp_rank * heads_dev, heads_dev, 2)
    step_cols = jnp.pad(step_cols.reshape(w_step.shape[0], 2 * heads_dev), ((0, 0), (0, 124)))
    out_turned = jnp.concatenate([w_out_ssd.T, w_out_pool.T], axis=1)
    projected, raw_steps, wout = gather_and_project(
        sp_count, lax.axis_size("fs"), tp_count // 2,
        tokens, (w_gate, w_value, w_bkey, w_query, w_pool_in), out_turned, step_cols,
        norm_gain[None],
    )
    raw_steps = raw_steps[:, : 2 * heads_dev]
    length = raw_steps.shape[0]
    stored = projected[HALO : HALO + length]
    row_ids = jnp.arange(length + 2 * REACH)
    inside = ((row_ids >= REACH) | (sp_rank > 0)) & (
        (row_ids < REACH + length) | (sp_rank < sp_count - 1)
    )
    padded = jnp.where(
        inside[:, None], projected[HALO - REACH : HALO + REACH + length, width_ssd:], 0
    )
    conv_cols = width_ssd + 2 * width_key
    taps = jnp.concatenate(
        [
            lax.dynamic_slice_in_dim(conv_value, tp_rank * width_ssd, width_ssd, 1),
            lax.dynamic_slice_in_dim(conv_bkey, tp_rank * width_key, width_key, 1),
            lax.dynamic_slice_in_dim(conv_query, tp_rank * width_key, width_key, 1),
        ],
        axis=1,
    ).astype(jnp.float32)
    margin = CONV_WIDTH // 2
    convolved = jnp.zeros((length, conv_cols), jnp.float32)
    for offset in range(CONV_WIDTH):
        begin = REACH - margin + offset
        convolved = (
            convolved
            + padded[begin : begin + length, :conv_cols].astype(jnp.float32) * taps[offset]
        )
    activated = jax.nn.silu(convolved)
    values = activated[:, :width_ssd].reshape(length, heads_dev, HEAD_DIM)
    bkeys = activated[:, width_ssd : width_ssd + width_key].reshape(length, groups_dev, STATE)
    queries = activated[:, width_ssd + width_key :].reshape(length, groups_dev, STATE)
    bias_dev = lax.dynamic_slice_in_dim(step_bias, tp_rank * heads_dev, heads_dev, 1)
    rate_dev = lax.dynamic_slice_in_dim(decay_rate, tp_rank * heads_dev, heads_dev, 1)
    steps = jax.nn.softplus(raw_steps.reshape(length, 2, heads_dev) + bias_dev).transpose(1, 2, 0)
    logs = -rate_dev[:, :, None] * steps - decay_shift[0].transpose(1, 0, 2)
    forward_out, forward_final, forward_total, forward_pos = local_pass(
        values, bkeys, queries, steps[0], logs[0]
    )
    backward_out, backward_final, backward_total, backward_pos = local_pass(
        values[::-1], bkeys[::-1], queries[::-1], steps[1][:, ::-1], logs[1][:, ::-1]
    )
    identity = (jnp.zeros_like(forward_total), jnp.zeros_like(forward_final))
    forward_in = carried_in((forward_total, forward_final), "sp", chain_combine, identity, False)[1]
    backward_in = carried_in((backward_total, backward_final), "sp", chain_combine, identity, True)[
        1
    ]
    forward_out = forward_out + apply_carry(queries, forward_in, forward_pos)
    backward_out = backward_out + apply_carry(queries[::-1], backward_in, backward_pos)
    heads_out = forward_out + backward_out[::-1]
    gated = heads_out.reshape(length, width_ssd) * jax.nn.silu(
        stored[:, :width_ssd].astype(jnp.float32)
    )
    squares = over_copies(jnp.sum(gated * gated, axis=-1), "tp")
    gain_dev = lax.dynamic_slice_in_dim(mix_gain, tp_rank * width_ssd, width_ssd, 0)
    ssd_mix = (gated * lax.rsqrt(squares / D_SSM + EPSILON)[:, None] * gain_dev).astype(
        jnp.bfloat16
    )
    pool_rows = padded[:, conv_cols:].astype(jnp.float32)
    own_rows = pool_rows[REACH : REACH + length]
    where_global = sp_rank * length + jnp.arange(length, dtype=jnp.int32)
    seq_length = length * sp_count
    window_means = []
    for window in WINDOWS:
        running = jnp.zeros((length, width_pool), jnp.float32)
        for offset in range(-(window // 2), window - window // 2):
            running = running + pool_rows[REACH + offset : REACH + offset + length]
        lower = jnp.clip(where_global - window // 2, 0, seq_length)
        upper = jnp.clip(where_global + window - window // 2, 0, seq_length)
        window_means.append(running / (upper - lower).astype(jnp.float32)[:, None])
    stacked = jnp.stack(window_means).reshape(4, length, pools_dev, POOL_DIM)
    group_ids = tp_rank * pools_dev + jnp.arange(pools_dev, dtype=jnp.int32)
    selector = (jnp.arange(4, dtype=jnp.int32)[:, None] == (group_ids % 4)[None, :]).astype(
        jnp.float32
    )
    means = jnp.sum(stacked * selector[:, None, :, None], axis=0)
    differences = (means - own_rows.reshape(length, pools_dev, POOL_DIM)).astype(jnp.bfloat16)
    pool_weights = lax.dynamic_slice_in_dim(pool_mix, tp_rank * pools_dev, pools_dev, 0)
    mapped = jnp.einsum(
        "rgc,gcd->rgd", differences, pool_weights, preferred_element_type=jnp.float32
    )
    pool_gain_dev = lax.dynamic_slice_in_dim(pool_gain, tp_rank * width_pool, width_pool, 0)
    pool_out = (mapped.reshape(length, width_pool) * pool_gain_dev).astype(jnp.bfloat16)
    out_ssd_rows = wout[:, :width_ssd].T
    out_pool_rows = wout[:, width_ssd:].T
    summed = sent_and_summed(
        (
            jnp.dot(ssd_mix, out_ssd_rows, preferred_element_type=jnp.float32)
            + jnp.dot(pool_out, out_pool_rows, preferred_element_type=jnp.float32)
        ).astype(jnp.bfloat16),
        "tp",
        0,
    )
    return summed.astype(jnp.bfloat16)[None]


def solution(mesh):
    return jax.shard_map(
        local,
        mesh=mesh,
        in_specs=(
            P("fs", ("sp", "tp"), None),
            P(),
            P(("sp", "fs"), "tp"),
            P(("sp", "fs"), "tp"),
            P(("sp", "fs"), "tp"),
            P(("sp", "fs"), "tp"),
            P(("sp", "fs"), "tp"),
            P(),
            P(),
            P(),
            P("fs", "tp", None, "sp"),
            P(),
            P(),
            P(),
            P(),
            P(),
            P(),
            P("tp", ("sp", "fs")),
            P("tp", ("sp", "fs")),
        ),
        out_specs=P("fs", ("sp", "tp"), None),
        check_vma=False,
    )
```

```python
import functools

import jax
import jax.numpy as jnp
from jax import lax
from jax.experimental import pallas as pl
from jax.experimental.pallas import tpu as pltpu
from jax.sharding import PartitionSpec as P

DUALITY_HEADS = 16
STATE = 128
SPAN = 128
D_SSM = 1024
EPSILON = 1e-06
HIGHEST = lax.Precision.HIGHEST

MESH = pl.DeviceIdType.MESH
A_COLS = 384
W_COLS = 896
HALO = 16
TOK_ROWS = 128
PIECE = 32


def remote(src, dst, send, recv, where):
    return pltpu.make_async_remote_copy(
        src_ref=src, dst_ref=dst, send_sem=send, recv_sem=recv, device_id=where, device_id_type=MESH
    )


def entry_barrier(places):
    barrier = pltpu.get_barrier_semaphore()
    for where in places:
        pl.semaphore_signal(barrier, inc=1, device_id=where, device_id_type=MESH)
    pl.semaphore_wait(barrier, len(places))


def gather_kernel(
    n_sp, n_fs, n_x,
    tok, wg, wv, wk, wq, wp, wo, wstep, gain,
    proj, raw, wout,
    tokbuf, wbuf,
    local_sem, out_sem,
    tp_sem, tm_sem, tr_sem, td_sem,
    ay_sem, azp_sem, azm_sem, bzp_sem, bzm_sem, byp_sem, bym_sem, byo_sem, h_sem,
    send_sem,
):
    z, y, t = lax.axis_index("sp"), lax.axis_index("fs"), lax.axis_index("tp")
    x, c = t // 2, t % 2
    xp, xm = (x + 1) % n_x, (x + n_x - 1) % n_x
    yp, ym = (y + 1) % n_fs, (y + n_fs - 1) % n_fs
    zp, zm = (z + 1) % n_sp, (z + n_sp - 1) % n_sp
    to_xp, to_xm, to_d = {"tp": xp * 2 + c}, {"tp": xm * 2 + c}, {"tp": x * 2 + 1 - c}
    to_yp, to_ym = {"fs": yp}, {"fs": ym}
    to_zp, to_zm = {"sp": zp}, {"sp": zm}

    def trow(xx, cc, q):
        return pl.multiple_of(HALO + (xx * 2 + cc) * TOK_ROWS + q * PIECE, 16)

    def wrow(zz, yy):
        return pl.multiple_of((zz * n_fs + yy) * PIECE, PIECE)

    def a_at(zz, yy):
        return wbuf.at[pl.ds(wrow(zz, yy), PIECE), pl.ds(0, A_COLS)]

    def b_at(zz, yy):
        return wbuf.at[pl.ds(wrow(zz, yy), PIECE), pl.ds(A_COLS, W_COLS - A_COLS)]

    def t_at(xx, cc, q, rows=PIECE):
        return tokbuf.at[pl.ds(trow(xx, cc, q), rows), :]

    locals_ = [pltpu.make_async_copy(tok.at[0], t_at(x, c, 0, TOK_ROWS), local_sem.at[0])]
    for i, w in enumerate((wg, wv, wk, wq, wp)):
        locals_.append(
            pltpu.make_async_copy(
                w, wbuf.at[pl.ds(wrow(z, y), PIECE), pl.ds(i * 128, 128)], local_sem.at[1 + i]
            )
        )
    locals_.append(
        pltpu.make_async_copy(
            wo, wbuf.at[pl.ds(wrow(z, y), PIECE), pl.ds(640, 256)], local_sem.at[6]
        )
    )
    for copy in locals_:
        copy.start()
    entry_barrier((to_xp, to_xm, to_yp, to_ym, to_zp, to_zm, to_d))

    sent = []

    def send(ref, recv, where):
        copy = remote(ref, ref, send_sem.at[len(sent)], recv, where)
        copy.start()
        sent.append(copy)

    def arrived(ref, recv):
        remote(ref, ref, send_sem.at[0], recv, to_d).wait_recv()

    for copy in locals_[1:]:
        copy.wait()
    own_a, own_b = a_at(z, y), b_at(z, y)
    send(own_a, ay_sem.at[0], to_yp)
    send(own_a, ay_sem.at[1], to_ym)
    send(own_a, azp_sem.at[4], to_zp)
    send(own_a, azm_sem.at[4], to_zm)
    send(own_b, bzp_sem.at[1], to_zp)
    send(own_b, bzm_sem.at[1], to_zm)
    locals_[0].wait()
    for q in (0, 1, 2, 3):
        send(t_at(x, c, q), tp_sem.at[q], to_xp)
    for q in (2, 3, 0, 1):
        send(t_at(x, c, q), tm_sem.at[q], to_xm)
    send(own_b, byp_sem.at[0], to_yp)
    send(own_b, bym_sem.at[0], to_ym)
    send(t_at(x, c, 0, TOK_ROWS), td_sem.at[12], to_d)

    yo = (y + 2) % n_fs
    y_of = (y, ym, yp, yo)
    arrived(a_at(z, ym), ay_sem.at[0])
    send(a_at(z, ym), ay_sem.at[2], to_yp)
    send(a_at(z, ym), azp_sem.at[5], to_zp)
    send(a_at(z, ym), azm_sem.at[5], to_zm)
    arrived(a_at(z, yp), ay_sem.at[1])
    send(a_at(z, yp), azp_sem.at[6], to_zp)
    send(a_at(z, yp), azm_sem.at[6], to_zm)
    arrived(a_at(z, yo), ay_sem.at[2])
    send(a_at(z, yo), azp_sem.at[7], to_zp)
    send(a_at(z, yo), azm_sem.at[7], to_zm)

    half = n_sp // 2

    def back(o):
        return (z + n_sp - o) % n_sp

    def relay_y(o):
        arrived(b_at(back(o), ym), byp_sem.at[o])
        if o % 2 == 0:
            send(b_at(back(o), ym), byo_sem.at[o], to_yp)
        arrived(b_at(back(o), yp), bym_sem.at[o])
        if o % 2 == 1:
            send(b_at(back(o), yp), byo_sem.at[o], to_ym)

    def token_step(k):
        if k <= 4:
            q = k - 1
            arrived(t_at(xm, c, q), tp_sem.at[q])
            if q < 2:
                send(t_at(xm, c, q), tr_sem.at[q], to_xp)
            send(t_at(xm, c, q), td_sem.at[q], to_d)
            q = (2, 3, 0, 1)[k - 1]
            arrived(t_at(xp, c, q), tm_sem.at[q])
            if q >= 2:
                send(t_at(xp, c, q), tr_sem.at[q], to_xm)
            send(t_at(xp, c, q), td_sem.at[4 + q], to_d)
        elif k <= 6:
            for q in (k - 5, k - 3):
                xo = (x + 2) % n_x
                arrived(t_at(xo, c, q), tr_sem.at[q])
                send(t_at(xo, c, q), td_sem.at[8 + q], to_d)

    pending = [0]
    for k in range(1, half + 1):
        far = k == half
        for j in range(4):
            if not far or j < 2:
                ref = a_at(back(k), y_of[j])
                arrived(ref, azp_sem.at[4 * k + j])
                if k + 1 < half or (k + 1 == half and j < 2):
                    send(ref, azp_sem.at[4 * (k + 1) + j], to_zp)
            if not far or j >= 2:
                ref = a_at((z + k) % n_sp, y_of[j])
                arrived(ref, azm_sem.at[4 * k + j])
                if k + 1 < half or (k + 1 == half and j >= 2):
                    send(ref, azm_sem.at[4 * (k + 1) + j], to_zm)
            if j == 1:
                token_step(k)
        fresh = []
        ref = b_at(back(k), y)
        arrived(ref, bzp_sem.at[k])
        if k < half:
            send(ref, bzp_sem.at[k + 1], to_zp)
        send(ref, byp_sem.at[k], to_yp)
        send(ref, bym_sem.at[k], to_ym)
        fresh.append(k)
        if not far:
            o = n_sp - k
            ref = b_at(back(o), y)
            arrived(ref, bzm_sem.at[k])
            if k + 1 < half:
                send(ref, bzm_sem.at[k + 1], to_zm)
            send(ref, byp_sem.at[o], to_yp)
            send(ref, bym_sem.at[o], to_ym)
            fresh.append(o)
        for o in pending:
            relay_y(o)
        pending = fresh

    cs = 1 - c
    arrived(t_at(x, cs, 0, TOK_ROWS), td_sem.at[12])
    for q in range(4):
        arrived(t_at(xm, cs, q), td_sem.at[q])
        arrived(t_at(xp, cs, q), td_sem.at[4 + q])
        arrived(t_at((x + 2) % n_x, cs, q), td_sem.at[8 + q])
    rows = 2 * n_x * TOK_ROWS
    last = tokbuf.at[pl.ds(rows, HALO), :]
    first = tokbuf.at[pl.ds(HALO, HALO), :]
    before = tokbuf.at[pl.ds(0, HALO), :]
    after = tokbuf.at[pl.ds(HALO + rows, HALO), :]
    halo_up = remote(last, before, send_sem.at[len(sent)], h_sem.at[0], to_zp)
    halo_up.start()
    sent.append(halo_up)
    halo_down = remote(first, after, send_sem.at[len(sent)], h_sem.at[1], to_zm)
    halo_down.start()
    sent.append(halo_down)
    for o in pending:
        relay_y(o)
    for o in range(n_sp):
        arrived(b_at(back(o), yo), byo_sem.at[o])
    to_out = pltpu.make_async_copy(wbuf.at[:, pl.ds(640, 256)], wout, out_sem)
    to_out.start()

    def project(begin, count):
        part = tokbuf[pl.ds(begin, count), :].astype(jnp.float32)
        scaling = lax.rsqrt(jnp.mean(part * part, axis=-1, keepdims=True) + EPSILON)
        normed = (part * scaling * gain[...]).astype(jnp.bfloat16)
        proj[pl.ds(begin, count), :] = jnp.dot(
            normed, wbuf[:, 0:640], preferred_element_type=jnp.float32
        ).astype(jnp.bfloat16)
        return normed

    def step(i, carry):
        begin = pl.multiple_of(HALO + i * 256, 16)
        normed = project(begin, 256)
        raw[pl.ds(pl.multiple_of(i * 256, 256), 256), :] = jnp.dot(
            normed, wstep[...], preferred_element_type=jnp.float32
        )
        return carry

    lax.fori_loop(0, rows // 256, step, 0)
    remote(before, before, send_sem.at[0], h_sem.at[0], to_d).wait_recv()
    remote(after, after, send_sem.at[0], h_sem.at[1], to_d).wait_recv()
    project(0, HALO)
    project(HALO + rows, HALO)
    to_out.wait()
    for copy in sent:
        copy.wait_send()


N_SENDS = 191


def gather_and_project(n_sp, n_fs, n_x, tok, ws, wo, wstep, gain):
    rows = 2 * n_x * TOK_ROWS
    any_spec = pl.BlockSpec(memory_space=pl.ANY)
    vmem = pl.BlockSpec(memory_space=pltpu.VMEM)
    dma = pltpu.SemaphoreType.DMA
    return pl.pallas_call(
        functools.partial(gather_kernel, n_sp, n_fs, n_x),
        out_shape=(
            jax.ShapeDtypeStruct((rows + 2 * HALO, 640), jnp.bfloat16),
            jax.ShapeDtypeStruct((rows, 128), jnp.float32),
            jax.ShapeDtypeStruct((2048, 256), jnp.bfloat16),
        ),
        in_specs=[any_spec] * 7 + [vmem, vmem],
        out_specs=(vmem, vmem, any_spec),
        scratch_shapes=[
            pltpu.VMEM((rows + 2 * HALO, 2048), jnp.bfloat16),
            pltpu.VMEM((2048, W_COLS), jnp.bfloat16),
            dma((7,)),
            dma,
            dma((4,)), dma((4,)), dma((4,)), dma((13,)),
            dma((3,)), dma((36,)), dma((36,)), dma((9,)), dma((9,)),
            dma((16,)), dma((16,)), dma((16,)), dma((2,)),
            dma((N_SENDS,)),
        ],
        compiler_params=pltpu.CompilerParams(
            collective_id=0, has_side_effects=True, vmem_limit_bytes=48 * 1024 * 1024
        ),
        name="gather_and_project",
    )(tok, *ws, wo, wstep, gain)


NT = (((1,), (1,)), ((), ()))
TN = (((0,), (0,)), ((), ()))
N_BLOCKS = 8
MSG = STATE + 16


def silu(v):
    return v / (1.0 + jnp.exp(-v))


def mix_kernel(
    n_sp, n_x,
    proj, raw, wout, bias, rate, shift, tap_v, tap_k, tap_q, mgain, pmix, pgain,
    out,
    p32, xbuf, kbuf, qbuf, ends, ybuf, mix,
    incl, excl, itot, etot, msg_out, msg_in, ss_out, ss_in,
    d_out, d_in, r_out, r_in, n_out, n_in,
    msg_send, msg_recv, ss_send, ss_recv, d_send, d_recv, r_send, r_recv, n_send, n_recv,
):
    f32, bf16 = jnp.float32, jnp.bfloat16
    z, t = lax.axis_index("sp"), lax.axis_index("tp")
    x, c = t // 2, t % 2
    n_tp = 2 * n_x
    xp, xm, xo = (x + 1) % n_x, (x + n_x - 1) % n_x, (x + 2) % n_x
    to_xp, to_xm, to_d = {"tp": xp * 2 + c}, {"tp": xm * 2 + c}, {"tp": x * 2 + 1 - c}
    distances = [1, 2, 4, 8]
    barrier = pltpu.get_barrier_semaphore()
    partners = [{"tp": (t + r) % n_tp} for r in range(1, n_tp)]
    partners += [{"sp": (z + d) % n_sp} for d in distances]
    partners += [{"sp": (z + n_sp - d) % n_sp} for d in distances if 2 * d != n_sp]
    for where in partners:
        pl.semaphore_signal(barrier, inc=1, device_id=where, device_id_type=MESH)

    lane0 = pl.multiple_of(t * 128, 128)
    rows = N_BLOCKS * SPAN
    p32[...] = proj[:, 128:640].astype(f32)

    @pl.when(z == 0)
    def _():
        p32[0:HALO, :] = jnp.zeros((HALO, 512), f32)

    @pl.when(z == n_sp - 1)
    def _():
        p32[HALO + rows : HALO + rows + HALO, :] = jnp.zeros((HALO, 512), f32)

    row8 = lax.broadcasted_iota(jnp.int32, (8, 128), 0)

    def by_kind(parts):
        found = jnp.zeros((8, 128), f32)
        for i, part in enumerate(parts):
            found = jnp.where(row8 == i, part, found)
        return found

    kinds = ((0, 0), (0, 1), (1, 0), (1, 1))
    bias8 = by_kind([bias[r, 2 * t + h] for r, h in kinds])
    rate8 = by_kind([rate[r, 2 * t + h] for r, h in kinds])
    steps_l, logs_l = [], []
    for b in range(N_BLOCKS):
        cols = raw[b * SPAN : (b + 1) * SPAN, :].T[0:8, :] + bias8
        steps = jnp.maximum(cols, 0.0) + jnp.log1p(jnp.exp(-jnp.abs(cols)))
        moved = by_kind([shift[0, h, r : r + 1, b * SPAN : (b + 1) * SPAN] for r, h in kinds])
        steps_l.append(steps)
        logs_l.append(jnp.where(row8 < 4, -rate8 * steps - moved, 0.0))
    steps = jnp.concatenate(steps_l, axis=0)
    logs = jnp.concatenate(logs_l, axis=0)
    lane = lax.broadcasted_iota(jnp.int32, (64, 128), 1)
    kind = lax.broadcasted_iota(jnp.int32, (64, 128), 0) % 8
    prefix, suffix = logs, logs
    for k in (1, 2, 4, 8, 16, 32, 64):
        prefix = prefix + jnp.where(lane >= k, pltpu.roll(prefix, k, 1), 0.0)
        suffix = suffix + jnp.where(lane < 128 - k, pltpu.roll(suffix, 128 - k, 1), 0.0)
    cum = jnp.where(kind < 2, prefix, suffix)
    total = jnp.broadcast_to(jnp.sum(logs, axis=1, keepdims=True), (64, 128))
    tail = jnp.exp(jnp.minimum(total - cum, 0.0)) * steps
    decay = jnp.exp(total)
    cum_tail_t = jnp.concatenate([cum, tail], axis=0).T
    reach_t = jnp.concatenate([jnp.exp(cum), jnp.zeros((64, 128), f32)], axis=0).T

    def wide(cols, b, first):
        j = b * 8 + first
        left = jnp.broadcast_to(cols[:, j : j + 1], (128, 64))
        right = jnp.broadcast_to(cols[:, j + 1 : j + 2], (128, 64))
        return jnp.concatenate([left, right], axis=1)

    def tall(rows_, b, first):
        j = b * 8 + first
        top = jnp.broadcast_to(rows_[j : j + 1, :], (64, 128))
        bottom = jnp.broadcast_to(rows_[j + 1 : j + 2, :], (64, 128))
        return jnp.concatenate([top, bottom], axis=0)

    def window(b, j):
        begin = HALO - 8 + b * SPAN
        return p32[begin : begin + SPAN + 16, j * 128 : (j + 1) * 128]

    def conv(b, j, taps):
        v = window(b, j)
        weights = taps[:, pl.ds(lane0, 128)].astype(f32)
        total_ = v * weights[2:3, :]
        for i in (0, 1, 3, 4):
            total_ = total_ + pltpu.roll(v, (2 - i) % (SPAN + 16), 0) * weights[i : i + 1, :]
        return silu(total_[8 : 8 + SPAN, :])

    for b in range(N_BLOCKS):
        at = slice(b * SPAN, (b + 1) * SPAN)
        values = conv(b, 0, tap_v)
        keys = conv(b, 1, tap_k).astype(bf16)
        xbuf[at, :] = values
        kbuf[at, :] = keys
        both = jnp.concatenate(
            [values * wide(cum_tail_t, b, 64), values * wide(cum_tail_t, b, 66)], axis=1
        )
        ends[b] = lax.dot_general(both.astype(bf16), keys, TN, preferred_element_type=f32)

    forward = ends[0, 0:128, :]
    backward = ends[N_BLOCKS - 1, 128:256, :]
    for i in range(1, N_BLOCKS):
        b = N_BLOCKS - 1 - i
        forward = forward * tall(decay, i, 0) + ends[i, 0:128, :]
        backward = backward * tall(decay, b, 2) + ends[b, 128:256, :]
    sums = total[0:8, :]
    for b in range(1, N_BLOCKS):
        sums = sums + total[b * 8 : b * 8 + 8, :]
    incl[0] = forward
    incl[1] = backward
    excl[...] = jnp.zeros_like(excl)
    itot[...] = jnp.broadcast_to(sums[None], (2, 8, 128))
    etot[...] = jnp.zeros_like(etot)

    def heads_decay(logs8, direction):
        return jnp.exp(tall(logs8, 0, 2 * direction))

    def exchange(i):
        d = distances[i]
        for way in (0, 1):
            there = z + d if way == 0 else z - d
            ok = there < n_sp if way == 0 else there >= 0
            logs8 = itot[way]
            high = logs8.astype(bf16)
            low = (logs8 - high.astype(f32)).astype(bf16)
            msg_out[way, i, 0:STATE, :] = incl[way].astype(bf16)
            msg_out[way, i, STATE:MSG, :] = jnp.concatenate([high, low], axis=0)
            where = {"sp": (z + d) % n_sp if way == 0 else (z + n_sp - d) % n_sp}

            @pl.when(ok)
            def _():
                remote(
                    msg_out.at[way, i], msg_in.at[way, i],
                    msg_send.at[way, i], msg_recv.at[way, i], where,
                ).start()

    def combine(i):
        d = distances[i]
        for way in (0, 1):
            ok = z >= d if way == 0 else z + d < n_sp

            @pl.when(ok)
            def _():
                remote(
                    msg_out.at[way, i], msg_in.at[way, i],
                    msg_send.at[way, i], msg_recv.at[way, i], to_d,
                ).wait_recv()
                state = msg_in[way, i, 0:STATE, :].astype(f32)
                pair = msg_in[way, i, STATE:MSG, :].astype(f32)
                logs8 = pair[0:8, :] + pair[8:16, :]
                excl[way] = excl[way] + heads_decay(etot[way], way) * state
                etot[way] = etot[way] + logs8
                incl[way] = incl[way] + heads_decay(itot[way], way) * state
                itot[way] = itot[way] + logs8

    row = lax.broadcasted_iota(jnp.int32, (128, 128), 0)
    col = lax.broadcasted_iota(jnp.int32, (128, 128), 1)

    def within(b):
        at = slice(b * SPAN, (b + 1) * SPAN)
        queries = conv(b, 2, tap_q).astype(bf16)
        qbuf[at, :] = queries
        scores = lax.dot_general(queries, kbuf[at, :], NT, preferred_element_type=f32)
        masked = []
        for h in (0, 1):
            jf, jb = b * 8 + h, b * 8 + 2 + h
            ahead = cum_tail_t[:, jf : jf + 1] - cum[jf : jf + 1, :]
            behind = cum_tail_t[:, jb : jb + 1] - cum[jb : jb + 1, :]
            gaps = jnp.where(col < row, ahead, jnp.where(col > row, behind, 0.0))
            df, db = steps[jf : jf + 1, :], steps[jb : jb + 1, :]
            sizes = jnp.where(col < row, df, jnp.where(col > row, db, df + db))
            masked.append((scores * jnp.exp(jnp.minimum(gaps, 0.0)) * sizes).astype(bf16))
        values = xbuf[at, :]
        stacked = jnp.concatenate(
            [jnp.where(col < 64, values, 0.0), jnp.where(col >= 64, values, 0.0)], axis=0
        ).astype(bf16)
        ybuf[at, :] = jnp.dot(
            jnp.concatenate(masked, axis=1), stacked, preferred_element_type=f32
        )

    def pool(b):
        at = slice(b * SPAN, (b + 1) * SPAN)
        n = SPAN + 16
        v = window(b, 3)
        w2 = v + pltpu.roll(v, 1, 0)
        w4 = pltpu.roll(w2, 1, 0) + pltpu.roll(w2, n - 1, 0)
        w8 = pltpu.roll(w4, 2, 0) + pltpu.roll(w4, n - 2, 0)
        w16 = pltpu.roll(w8, 4, 0) + pltpu.roll(w8, n - 4, 0)
        which = t % 4
        summed = jnp.where(
            which == 0, w2, jnp.where(which == 1, w4, jnp.where(which == 2, w8, w16))
        )[8 : 8 + SPAN, :]
        reach = jnp.where(which == 0, 1, jnp.where(which == 1, 2, jnp.where(which == 2, 4, 8)))
        place = z * rows + b * SPAN + row
        upper = jnp.minimum(place + reach, n_sp * rows)
        lower = jnp.maximum(place - reach, 0)
        differences = summed / (upper - lower).astype(f32) - v[8 : 8 + SPAN, :]
        mapped = jnp.dot(differences.astype(bf16), pmix[t], preferred_element_type=f32)
        mix[at, 128:256] = (mapped * pgain[:, pl.ds(lane0, 128)]).astype(bf16)

    pl.semaphore_wait(barrier, len(partners))
    exchange(0)
    within(0)
    within(1)
    combine(0)
    exchange(1)
    within(2)
    within(3)
    combine(1)
    exchange(2)
    within(4)
    within(5)
    within(6)
    within(7)
    combine(2)
    exchange(3)
    for b in range(N_BLOCKS):
        pool(b)
    combine(3)

    forward, backward = excl[0], excl[1]
    entering = [None] * N_BLOCKS
    leaving = [None] * N_BLOCKS
    for i in range(N_BLOCKS):
        b = N_BLOCKS - 1 - i
        entering[i] = forward.astype(bf16)
        leaving[b] = backward.astype(bf16)
        forward = forward * tall(decay, i, 0) + ends[i, 0:128, :]
        backward = backward * tall(decay, b, 2) + ends[b, 128:256, :]
    squares = []
    for b in range(N_BLOCKS):
        at = slice(b * SPAN, (b + 1) * SPAN)
        states = jnp.concatenate([entering[b], leaving[b]], axis=0)
        carried = lax.dot_general(qbuf[at, :], states, NT, preferred_element_type=f32)
        heads_out = (
            ybuf[at, :]
            + carried[:, 0:128] * wide(reach_t, b, 0)
            + carried[:, 128:256] * wide(reach_t, b, 2)
        )
        gate = proj[HALO + b * SPAN : HALO + (b + 1) * SPAN, 0:128].astype(f32)
        gated = heads_out * silu(gate)
        ybuf[at, :] = gated
        squares.append(
            lax.dot_general(
                jnp.ones((8, 128), f32), gated * gated, NT,
                precision=HIGHEST, preferred_element_type=f32,
            )[0:1, :]
        )
    own_squares = jnp.concatenate(squares, axis=0)
    ss_out[...] = own_squares
    ss_copies = []
    for r in range(1, n_tp):
        copy = remote(
            ss_out, ss_in.at[r - 1], ss_send.at[r - 1], ss_recv.at[r - 1],
            {"tp": (t + r) % n_tp},
        )
        copy.start()
        ss_copies.append(copy)
    all_squares = own_squares
    for r in range(1, n_tp):
        ss_copies[r - 1].wait_recv()
        all_squares = all_squares + ss_in[r - 1]
    scale = lax.rsqrt(all_squares / D_SSM + EPSILON)
    scale_t = jnp.concatenate([scale, jnp.zeros((120, 128), f32)], axis=0).T
    gain = mgain[:, pl.ds(lane0, 128)]
    for b in range(N_BLOCKS):
        at = slice(b * SPAN, (b + 1) * SPAN)
        mix[at, 0:128] = (ybuf[at, :] * scale_t[:, b : b + 1] * gain).astype(bf16)

    def partial(xx, cc, begin=0, count=TOK_ROWS):
        at = pl.multiple_of((xx * 2 + cc) * TOK_ROWS + begin, 16)
        return lax.dot_general(
            mix[pl.ds(at, count), :], wout[...], NT, preferred_element_type=f32
        )

    half = TOK_ROWS // 2
    d_copies = []
    for i, xx in enumerate((xo, xp, xm, x)):
        d_out[i] = partial(xx, 1 - c).astype(bf16)
        copy = remote(d_out.at[i], d_in.at[i], d_send.at[i], d_recv.at[i], to_d)
        copy.start()
        d_copies.append(copy)

    def chip(i, xx, begin, count=half):
        return partial(xx, c, begin, count) + d_in[i, begin : begin + count, :].astype(f32)

    def send(i, value, where, out_ref, in_ref, send_sem, recv_sem):
        out_ref[i] = value.astype(bf16)
        copy = remote(out_ref.at[i], in_ref.at[i], send_sem.at[i], recv_sem.at[i], where)
        copy.start()
        return copy

    relay = (r_out, r_in, r_send, r_recv)
    near = (n_out, n_in, n_send, n_recv)
    d_copies[0].wait_recv()
    relay_p = send(0, chip(0, xo, 0), to_xp, *relay)
    relay_m = send(1, chip(0, xo, half), to_xm, *relay)
    d_copies[1].wait_recv()
    dir_p = send(0, chip(1, xp, half), to_xp, *near)
    d_copies[2].wait_recv()
    dir_m = send(1, chip(2, xm, 0), to_xm, *near)
    relay_p.wait_recv()
    comb_p = send(2, chip(1, xp, 0) + r_in[0].astype(f32), to_xp, *near)
    relay_m.wait_recv()
    comb_m = send(3, chip(2, xm, half) + r_in[1].astype(f32), to_xm, *near)
    d_copies[3].wait_recv()
    top, bottom = chip(3, x, 0), chip(3, x, half)
    dir_p.wait_recv()
    dir_m.wait_recv()
    bottom = bottom + n_in[0].astype(f32)
    top = top + n_in[1].astype(f32)
    comb_p.wait_recv()
    out[0, 0:half, :] = (top + n_in[2].astype(f32)).astype(bf16)
    comb_m.wait_recv()
    out[0, half:TOK_ROWS, :] = (bottom + n_in[3].astype(f32)).astype(bf16)

    for i, d in enumerate(distances):
        for way in (0, 1):
            ok = z + d < n_sp if way == 0 else z >= d

            @pl.when(ok)
            def _():
                remote(
                    msg_out.at[way, i], msg_in.at[way, i],
                    msg_send.at[way, i], msg_recv.at[way, i], to_d,
                ).wait_send()

    for copy in ss_copies + d_copies + [relay_p, relay_m, dir_p, dir_m, comb_p, comb_m]:
        copy.wait_send()


def mixed_and_summed(
    n_sp, n_x, proj, raw, wout, bias, rate, shift, tap_v, tap_k, tap_q, mgain, pmix, pgain
):
    vmem = pl.BlockSpec(memory_space=pltpu.VMEM)
    smem = pl.BlockSpec(memory_space=pltpu.SMEM)
    dma = pltpu.SemaphoreType.DMA
    f32, bf16 = jnp.float32, jnp.bfloat16
    rows = N_BLOCKS * SPAN
    half = TOK_ROWS // 2
    return pl.pallas_call(
        functools.partial(mix_kernel, n_sp, n_x),
        out_shape=jax.ShapeDtypeStruct((1, TOK_ROWS, 2048), bf16),
        in_specs=[vmem] * 3 + [smem] * 2 + [vmem] * 7,
        out_specs=vmem,
        scratch_shapes=[
            pltpu.VMEM((rows + 2 * HALO, 512), f32),
            pltpu.VMEM((rows, 128), f32),
            pltpu.VMEM((rows, 128), bf16),
            pltpu.VMEM((rows, 128), bf16),
            pltpu.VMEM((N_BLOCKS, 256, 128), f32),
            pltpu.VMEM((rows, 128), f32),
            pltpu.VMEM((rows, 256), bf16),
            pltpu.VMEM((2, 128, 128), f32),
            pltpu.VMEM((2, 128, 128), f32),
            pltpu.VMEM((2, 8, 128), f32),
            pltpu.VMEM((2, 8, 128), f32),
            pltpu.VMEM((2, 4, MSG, 128), bf16),
            pltpu.VMEM((2, 4, MSG, 128), bf16),
            pltpu.VMEM((8, 128), f32),
            pltpu.VMEM((7, 8, 128), f32),
            pltpu.VMEM((4, TOK_ROWS, 2048), bf16),
            pltpu.VMEM((4, TOK_ROWS, 2048), bf16),
            pltpu.VMEM((2, half, 2048), bf16),
            pltpu.VMEM((2, half, 2048), bf16),
            pltpu.VMEM((4, half, 2048), bf16),
            pltpu.VMEM((4, half, 2048), bf16),
            dma((2, 4)), dma((2, 4)), dma((7,)), dma((7,)),
            dma((4,)), dma((4,)), dma((2,)), dma((2,)), dma((4,)), dma((4,)),
        ],
        compiler_params=pltpu.CompilerParams(
            collective_id=1, has_side_effects=True, vmem_limit_bytes=56 * 1024 * 1024
        ),
        name="mixed_and_summed",
    )(proj, raw, wout, bias, rate, shift, tap_v, tap_k, tap_q, mgain, pmix, pgain)


def local(
    tokens, norm_gain, w_gate, w_value, w_bkey, w_query, w_pool_in, w_step, step_bias,
    decay_rate, decay_shift, conv_value, conv_bkey, conv_query, mix_gain, pool_mix, pool_gain,
    w_out_ssd, w_out_pool,
):
    n_tp, n_sp, n_fs = lax.axis_size("tp"), lax.axis_size("sp"), lax.axis_size("fs")
    heads_dev = DUALITY_HEADS // n_tp
    step_cols = lax.dynamic_slice_in_dim(w_step, lax.axis_index("tp") * heads_dev, heads_dev, 2)
    step_cols = jnp.pad(step_cols.reshape(w_step.shape[0], 2 * heads_dev), ((0, 0), (0, 124)))
    out_turned = jnp.concatenate([w_out_ssd.T, w_out_pool.T], axis=1)
    projected, raw_steps, wout = gather_and_project(
        n_sp, n_fs, n_tp // 2, tokens, (w_gate, w_value, w_bkey, w_query, w_pool_in),
        out_turned, step_cols, norm_gain[None],
    )
    return mixed_and_summed(
        n_sp, n_tp // 2, projected, raw_steps, wout, step_bias, decay_rate, decay_shift,
        conv_value, conv_bkey, conv_query, mix_gain[None], pool_mix, pool_gain[None],
    )


def solution(mesh):
    return jax.shard_map(
        local,
        mesh=mesh,
        in_specs=(
            P("fs", ("sp", "tp"), None),
            P(),
            P(("sp", "fs"), "tp"),
            P(("sp", "fs"), "tp"),
            P(("sp", "fs"), "tp"),
            P(("sp", "fs"), "tp"),
            P(("sp", "fs"), "tp"),
            P(),
            P(),
            P(),
            P("fs", "tp", None, "sp"),
            P(),
            P(),
            P(),
            P(),
            P(),
            P(),
            P("tp", ("sp", "fs")),
            P("tp", ("sp", "fs")),
        ),
        out_specs=P("fs", ("sp", "tp"), None),
        check_vma=False,
    )
```

```python
import functools

import jax
import jax.numpy as jnp
from jax import lax
from jax.experimental import pallas as pl
from jax.experimental.pallas import tpu as pltpu
from jax.sharding import PartitionSpec as P

DUALITY_HEADS = 16
STATE = 128
SPAN = 128
D_SSM = 1024
EPSILON = 1e-06
HIGHEST = lax.Precision.HIGHEST

MESH = pl.DeviceIdType.MESH
HALO = 16
TOK_ROWS = 128
PIECE = 32
NT = (((1,), (1,)), ((), ()))
TN = (((0,), (0,)), ((), ()))
N_BLOCKS = 8
MSG = 64 + 16


def remote(src, dst, send, recv, where):
    return pltpu.make_async_remote_copy(
        src_ref=src, dst_ref=dst, send_sem=send, recv_sem=recv, device_id=where, device_id_type=MESH
    )


def silu(v):
    return v / (1.0 + jnp.exp(-v))


class Rings:
    def __init__(self, buf, a_cols, b_cols, sems, send_sem, place, sizes):
        self.buf, self.a_cols, self.b_cols = buf, a_cols, b_cols
        self.ay, self.azp, self.azm, self.bzp, self.bzm, self.byp, self.bym, self.byo = sems
        self.send_sem, self.sent = send_sem, []
        self.z, self.y = place
        self.n_sp, self.n_fs = sizes
        z, y, n_sp, n_fs = self.z, self.y, *sizes
        self.yp, self.ym, self.yo = (y + 1) % n_fs, (y + n_fs - 1) % n_fs, (y + 2) % n_fs
        self.to_yp, self.to_ym = {"fs": self.yp}, {"fs": self.ym}
        self.to_zp, self.to_zm = {"sp": (z + 1) % n_sp}, {"sp": (z + n_sp - 1) % n_sp}
        self.half = n_sp // 2
        self.pending = [0]

    def at(self, zz, yy, cols):
        row = pl.multiple_of((zz * self.n_fs + yy) * PIECE, PIECE)
        return self.buf.at[pl.ds(row, PIECE), pl.ds(*cols)]

    def a(self, zz, yy):
        return self.at(zz, yy, self.a_cols)

    def b(self, zz, yy):
        return self.at(zz, yy, self.b_cols)

    def send(self, ref, recv, where):
        copy = remote(ref, ref, self.send_sem.at[len(self.sent)], recv, where)
        copy.start()
        self.sent.append(copy)

    def arrived(self, ref, recv):
        remote(ref, ref, self.send_sem.at[0], recv, self.to_yp).wait_recv()

    def begin(self):
        own_a, own_b = self.a(self.z, self.y), self.b(self.z, self.y)
        self.send(own_b, self.bzp.at[1], self.to_zp)
        self.send(own_b, self.bzm.at[1], self.to_zm)
        self.send(own_a, self.ay.at[0], self.to_yp)
        self.send(own_a, self.ay.at[1], self.to_ym)
        self.send(own_a, self.azp.at[4], self.to_zp)
        self.send(own_a, self.azm.at[4], self.to_zm)
        self.send(own_b, self.byp.at[0], self.to_yp)
        self.send(own_b, self.bym.at[0], self.to_ym)

    def spread(self):
        for j, yy in ((1, self.ym), (2, self.yp), (3, self.yo)):
            ref = self.a(self.z, yy)
            self.arrived(ref, self.ay.at[j - 1])
            if j == 1:
                self.send(ref, self.ay.at[2], self.to_yp)
            self.send(ref, self.azp.at[4 + j], self.to_zp)
            self.send(ref, self.azm.at[4 + j], self.to_zm)

    def back(self, o):
        return (self.z + self.n_sp - o) % self.n_sp

    def relay(self, o):
        low, high = self.b(self.back(o), self.ym), self.b(self.back(o), self.yp)
        self.arrived(low, self.byp.at[o])
        if o % 2 == 0:
            self.send(low, self.byo.at[o], self.to_yp)
        self.arrived(high, self.bym.at[o])
        if o % 2 == 1:
            self.send(high, self.byo.at[o], self.to_ym)

    def relay_pending(self):
        for o in self.pending:
            self.relay(o)
        self.pending = []

    def step(self, k, between=None):
        half, fresh = self.half, []
        far = k == half
        for o, recv, onward, where in (
            (k, self.bzp, k < half, self.to_zp),
            (self.n_sp - k, self.bzm, k + 1 < half, self.to_zm),
        ):
            if o in fresh:
                continue
            ref = self.b(self.back(o), self.y)
            self.arrived(ref, recv.at[k])
            if onward:
                self.send(ref, recv.at[k + 1], where)
            self.send(ref, self.byp.at[o], self.to_yp)
            self.send(ref, self.bym.at[o], self.to_ym)
            fresh.append(o)
        y_of = (self.y, self.ym, self.yp, self.yo)
        for j in range(4):
            for recv, zz, mine, where in (
                (self.azp, self.back(k), j < 2, self.to_zp),
                (self.azm, (self.z + k) % self.n_sp, j >= 2, self.to_zm),
            ):
                if far and not mine:
                    continue
                ref = self.a(zz, y_of[j])
                self.arrived(ref, recv.at[4 * k + j])
                if k + 1 < half or (k + 1 == half and mine):
                    self.send(ref, recv.at[4 * (k + 1) + j], where)
            if j == 1:
                self.relay_pending()
                if between is not None:
                    between()
        self.pending = fresh

    def finish(self):
        self.relay_pending()
        for o in range(self.n_sp):
            self.arrived(self.b(self.back(o), self.yo), self.byo.at[o])


def mixer_kernel(
    n_sp, n_fs, n_x,
    tok, wg, wv, wk, wq, wp, wo, wstep, gain,
    bias, rate, shift, tap_v, tap_k, tap_q, mgain, pmix, pgain,
    out,
    tokbuf, normbuf, wbuf, wout, gates, raw,
    p32, xbuf, kbuf, qbuf, ends, ybuf, mix,
    incl, excl, itot, etot, msg_out, msg_in, ss_out, ss_in,
    d_out, d_in, r_out, r_in, n_out, n_in,
    local_sem, tp_sem, tm_sem, tr_sem, td_sem, h_sem, t_send,
    w_ay, w_azp, w_azm, w_bzp, w_bzm, w_byp, w_bym, w_byo, w_send,
    o_ay, o_azp, o_azm, o_bzp, o_bzm, o_byp, o_bym, o_byo, o_send,
    msg_send, msg_recv, ss_send, ss_recv, d_send, d_recv, r_send, r_recv, n_send, n_recv,
):
    f32, bf16 = jnp.float32, jnp.bfloat16
    z, y, t = lax.axis_index("sp"), lax.axis_index("fs"), lax.axis_index("tp")
    x, c = t // 2, t % 2
    n_tp = 2 * n_x
    xp, xm, xo = (x + 1) % n_x, (x + n_x - 1) % n_x, (x + 2) % n_x
    to_xp, to_xm, to_d = {"tp": xp * 2 + c}, {"tp": xm * 2 + c}, {"tp": x * 2 + 1 - c}
    to_zp, to_zm = {"sp": (z + 1) % n_sp}, {"sp": (z + n_sp - 1) % n_sp}
    distances = [1, 2, 4, 8]
    rows = N_BLOCKS * SPAN

    w_rings = Rings(
        wbuf, (0, 256), (256, 384),
        (w_ay, w_azp, w_azm, w_bzp, w_bzm, w_byp, w_bym, w_byo), w_send, (z, y), (n_sp, n_fs),
    )
    o_rings = Rings(
        wout, (0, 128), (128, 128),
        (o_ay, o_azp, o_azm, o_bzp, o_bzm, o_byp, o_bym, o_byo), o_send, (z, y), (n_sp, n_fs),
    )

    def t_at(xx, cc, q=0, count=PIECE):
        row = pl.multiple_of(HALO + (xx * 2 + cc) * TOK_ROWS + q * PIECE, 16)
        return tokbuf.at[pl.ds(row, count), :]

    own_row = pl.ds(pl.multiple_of((z * n_fs + y) * PIECE, PIECE), PIECE)
    locals_ = [
        pltpu.make_async_copy(w, wbuf.at[own_row, pl.ds(i * 128, 128)], local_sem.at[i])
        for i, w in enumerate((wg, wv, wk, wq, wp))
    ]
    locals_.append(pltpu.make_async_copy(tok.at[0], t_at(x, c, 0, TOK_ROWS), local_sem.at[5]))
    locals_.append(pltpu.make_async_copy(wo, wout.at[own_row, :], local_sem.at[6]))
    locals_.append(pltpu.make_async_copy(wstep, wbuf.at[:, pl.ds(640, 128)], local_sem.at[7]))
    for copy in locals_:
        copy.start()

    barrier = pltpu.get_barrier_semaphore()
    partners = [{"tp": (t + r) % n_tp} for r in range(1, n_tp)]
    partners += [{"sp": (z + d) % n_sp} for d in distances]
    partners += [{"sp": (z + n_sp - d) % n_sp} for d in distances if 2 * d != n_sp]
    partners += [w_rings.to_yp, w_rings.to_ym]
    for where in partners:
        pl.semaphore_signal(barrier, inc=1, device_id=where, device_id_type=MESH)
    pl.semaphore_wait(barrier, len(partners))

    t_sent = []

    def t_go(src, dst, recv, where):
        copy = remote(src, dst, t_send.at[len(t_sent)], recv, where)
        copy.start()
        t_sent.append(copy)

    def t_came(ref, recv):
        remote(ref, ref, t_send.at[0], recv, to_d).wait_recv()

    def relay_tokens(xx, q, recv, where, onward, slot):
        ref = t_at(xx, c, q)
        t_came(ref, recv)
        if onward:
            t_go(ref, ref, tr_sem.at[q], where)
        t_go(ref, ref, td_sem.at[slot + q], to_d)

    def norm_rows(begin, count):
        part = tokbuf[pl.ds(begin, count), :].astype(f32)
        scaling = lax.rsqrt(jnp.mean(part * part, axis=-1, keepdims=True) + EPSILON)
        normbuf[pl.ds(begin, count), :] = (part * scaling * gain[...]).astype(bf16)

    def norm_block(xx, cc):
        norm_rows(pl.multiple_of(HALO + (xx * 2 + cc) * TOK_ROWS, 16), TOK_ROWS)

    cs = 1 - c

    def token_step(k):
        if k <= 4:
            q = k - 1
            relay_tokens(xm, q, tp_sem.at[q], to_xp, q < 2, 0)
            q = (2, 3, 0, 1)[k - 1]
            relay_tokens(xp, q, tm_sem.at[q], to_xm, q >= 2, 4)
            if k == 2:
                norm_block(x, c)
            if k == 3:
                t_came(t_at(x, cs, 0, TOK_ROWS), td_sem.at[12])
                norm_block(x, cs)
        elif k <= 6:
            for q in (k - 5, k - 3):
                relay_tokens(xo, q, tr_sem.at[q], to_d, False, 8)
            norm_block(xm if k == 5 else xp, c)
        elif k == 7:
            for q in range(4):
                t_came(t_at(xm, cs, q), td_sem.at[q])
                t_came(t_at(xp, cs, q), td_sem.at[4 + q])
            norm_block(xm, cs)
            norm_block(xp, cs)
        else:
            norm_block(xo, c)

    for copy in locals_[:5]:
        copy.wait()
    w_rings.begin()
    locals_[5].wait()
    for q in (0, 1, 2, 3):
        t_go(t_at(x, c, q), t_at(x, c, q), tp_sem.at[q], to_xp)
    for q in (2, 3, 0, 1):
        t_go(t_at(x, c, q), t_at(x, c, q), tm_sem.at[q], to_xm)
    t_go(t_at(x, c, 0, TOK_ROWS), t_at(x, c, 0, TOK_ROWS), td_sem.at[12], to_d)
    w_rings.spread()
    for k in range(1, n_sp // 2 + 1):
        w_rings.step(k, functools.partial(token_step, k))
    for q in range(4):
        t_came(t_at(xo, cs, q), td_sem.at[8 + q])
    before, after = tokbuf.at[pl.ds(0, HALO), :], tokbuf.at[pl.ds(HALO + rows, HALO), :]
    t_go(tokbuf.at[pl.ds(rows, HALO), :], before, h_sem.at[0], to_zp)
    t_go(tokbuf.at[pl.ds(HALO, HALO), :], after, h_sem.at[1], to_zm)
    w_rings.relay_pending()
    locals_[6].wait()
    o_rings.begin()
    norm_block(xo, cs)
    locals_[7].wait()
    w_rings.finish()

    def rounded(v):
        return v.astype(bf16).astype(f32)

    def project(i):
        at = HALO + i * 256
        dots = jnp.dot(normbuf[at : at + 256, :], wbuf[...], preferred_element_type=f32)
        gates[i * 256 : (i + 1) * 256, :] = dots[:, 0:128].astype(bf16)
        p32[at : at + 256, :] = rounded(dots[:, 128:640])
        raw[i * 256 : (i + 1) * 256, :] = dots[:, 640:768]

    project(0)
    o_rings.spread()
    project(1)
    project(2)
    o_rings.step(1)
    project(3)
    t_came(before, h_sem.at[0])
    t_came(after, h_sem.at[1])
    for begin, real in ((0, z > 0), (HALO + rows, z < n_sp - 1)):
        norm_rows(begin, HALO)
        edge = jnp.dot(
            normbuf[begin : begin + HALO, :], wbuf[:, 128:640], preferred_element_type=f32
        )
        p32[begin : begin + HALO, :] = jnp.where(real, rounded(edge), 0.0)
    o_rings.step(2)

    lane0 = pl.multiple_of(t * 128, 128)
    row8 = lax.broadcasted_iota(jnp.int32, (8, 128), 0)

    def by_kind(parts):
        found = jnp.zeros((8, 128), f32)
        for i, part in enumerate(parts):
            found = jnp.where(row8 == i, part, found)
        return found

    kinds = ((0, 0), (0, 1), (1, 0), (1, 1))
    bias8 = by_kind([bias[r, 2 * t + h] for r, h in kinds])
    rate8 = by_kind([rate[r, 2 * t + h] for r, h in kinds])
    steps_l, logs_l = [], []
    for b in range(N_BLOCKS):
        cols = raw[b * SPAN : (b + 1) * SPAN, :].T[0:8, :] + bias8
        steps = jnp.maximum(cols, 0.0) + jnp.log1p(jnp.exp(-jnp.abs(cols)))
        moved = by_kind([shift[0, h, r : r + 1, b * SPAN : (b + 1) * SPAN] for r, h in kinds])
        steps_l.append(steps)
        logs_l.append(jnp.where(row8 < 4, -rate8 * steps - moved, 0.0))
    steps = jnp.concatenate(steps_l, axis=0)
    logs = jnp.concatenate(logs_l, axis=0)
    lane = lax.broadcasted_iota(jnp.int32, (64, 128), 1)
    kind = lax.broadcasted_iota(jnp.int32, (64, 128), 0) % 8
    prefix, suffix = logs, logs
    for k in (1, 2, 4, 8, 16, 32, 64):
        prefix = prefix + jnp.where(lane >= k, pltpu.roll(prefix, k, 1), 0.0)
        suffix = suffix + jnp.where(lane < 128 - k, pltpu.roll(suffix, 128 - k, 1), 0.0)
    cum = jnp.where(kind < 2, prefix, suffix)
    total = jnp.broadcast_to(jnp.sum(logs, axis=1, keepdims=True), (64, 128))
    tail = jnp.exp(jnp.minimum(total - cum, 0.0)) * steps
    decay = jnp.exp(total)
    cum_tail_t = jnp.concatenate([cum, tail], axis=0).T
    reach_t = jnp.concatenate([jnp.exp(cum), jnp.zeros((64, 128), f32)], axis=0).T

    def wide(cols, b, first):
        j = b * 8 + first
        left = jnp.broadcast_to(cols[:, j : j + 1], (128, 64))
        right = jnp.broadcast_to(cols[:, j + 1 : j + 2], (128, 64))
        return jnp.concatenate([left, right], axis=1)

    def tall(rows_, b, first):
        j = b * 8 + first
        top = jnp.broadcast_to(rows_[j : j + 1, :], (64, 128))
        bottom = jnp.broadcast_to(rows_[j + 1 : j + 2, :], (64, 128))
        return jnp.concatenate([top, bottom], axis=0)

    def window(b, j):
        begin = HALO - 8 + b * SPAN
        return p32[begin : begin + SPAN + 16, j * 128 : (j + 1) * 128]

    def conv(b, j, taps):
        v = window(b, j)
        weights = taps[:, pl.ds(lane0, 128)].astype(f32)
        total_ = v * weights[2:3, :]
        for i in (0, 1, 3, 4):
            total_ = total_ + pltpu.roll(v, (2 - i) % (SPAN + 16), 0) * weights[i : i + 1, :]
        return silu(total_[8 : 8 + SPAN, :])

    for b in range(N_BLOCKS):
        at = slice(b * SPAN, (b + 1) * SPAN)
        values = conv(b, 0, tap_v)
        keys = conv(b, 1, tap_k).astype(bf16)
        xbuf[at, :] = values
        kbuf[at, :] = keys
        both = jnp.concatenate(
            [values * wide(cum_tail_t, b, 64), values * wide(cum_tail_t, b, 66)], axis=1
        )
        ends[b] = lax.dot_general(both.astype(bf16), keys, TN, preferred_element_type=f32)
        if b == 4:
            o_rings.step(3)

    forward = ends[0, 0:128, :]
    backward = ends[N_BLOCKS - 1, 128:256, :]
    for i in range(1, N_BLOCKS):
        b = N_BLOCKS - 1 - i
        forward = forward * tall(decay, i, 0) + ends[i, 0:128, :]
        backward = backward * tall(decay, b, 2) + ends[b, 128:256, :]
    sums = total[0:8, :]
    for b in range(1, N_BLOCKS):
        sums = sums + total[b * 8 : b * 8 + 8, :]
    incl[0] = forward
    incl[1] = backward
    excl[...] = jnp.zeros_like(excl)
    itot[...] = jnp.broadcast_to(sums[None], (4, 8, 128))
    etot[...] = jnp.zeros_like(etot)

    def message(way, h, i, where):
        return remote(
            msg_out.at[way, h, i], msg_in.at[way, h, i],
            msg_send.at[way, h, i], msg_recv.at[way, h, i], where,
        )

    def exchange(i, h):
        d = distances[i]
        for way in (0, 1):
            ok = z + d < n_sp if way == 0 else z >= d
            logs8 = itot[2 * way + h]
            high = logs8.astype(bf16)
            low = (logs8 - high.astype(f32)).astype(bf16)
            msg_out[way, h, i, 0:64, :] = incl[way, h * 64 : (h + 1) * 64, :].astype(bf16)
            msg_out[way, h, i, 64:MSG, :] = jnp.concatenate([high, low], axis=0)
            where = {"sp": (z + d) % n_sp if way == 0 else (z + n_sp - d) % n_sp}

            @pl.when(ok)
            def _():
                message(way, h, i, where).start()

    def combine(i, h):
        d = distances[i]
        for way in (0, 1):
            ok = z >= d if way == 0 else z + d < n_sp
            s, r, part = 2 * way + h, 2 * way + h, slice(h * 64, (h + 1) * 64)

            @pl.when(ok)
            def _():
                message(way, h, i, to_d).wait_recv()
                state = msg_in[way, h, i, 0:64, :].astype(f32)
                pair = msg_in[way, h, i, 64:MSG, :].astype(f32)
                logs8 = pair[0:8, :] + pair[8:16, :]
                incl[way, part, :] = incl[way, part, :] + jnp.exp(itot[s][r : r + 1, :]) * state
                itot[s] = itot[s] + logs8
                excl[way, part, :] = excl[way, part, :] + jnp.exp(etot[s][r : r + 1, :]) * state
                etot[s] = etot[s] + logs8

    row = lax.broadcasted_iota(jnp.int32, (128, 128), 0)
    col = lax.broadcasted_iota(jnp.int32, (128, 128), 1)

    def within(b):
        at = slice(b * SPAN, (b + 1) * SPAN)
        queries = conv(b, 2, tap_q).astype(bf16)
        qbuf[at, :] = queries
        scores = lax.dot_general(queries, kbuf[at, :], NT, preferred_element_type=f32)
        masked = []
        for h in (0, 1):
            jf, jb = b * 8 + h, b * 8 + 2 + h
            ahead = cum_tail_t[:, jf : jf + 1] - cum[jf : jf + 1, :]
            behind = cum_tail_t[:, jb : jb + 1] - cum[jb : jb + 1, :]
            gaps = jnp.where(col < row, ahead, jnp.where(col > row, behind, 0.0))
            df, db = steps[jf : jf + 1, :], steps[jb : jb + 1, :]
            sizes = jnp.where(col < row, df, jnp.where(col > row, db, df + db))
            masked.append((scores * jnp.exp(jnp.minimum(gaps, 0.0)) * sizes).astype(bf16))
        values = xbuf[at, :]
        stacked = jnp.concatenate(
            [jnp.where(col < 64, values, 0.0), jnp.where(col >= 64, values, 0.0)], axis=0
        ).astype(bf16)
        ybuf[at, :] = jnp.dot(
            jnp.concatenate(masked, axis=1), stacked, preferred_element_type=f32
        )

    def pool(b):
        at = slice(b * SPAN, (b + 1) * SPAN)
        n = SPAN + 16
        v = window(b, 3)
        w2 = v + pltpu.roll(v, 1, 0)
        w4 = pltpu.roll(w2, 1, 0) + pltpu.roll(w2, n - 1, 0)
        w8 = pltpu.roll(w4, 2, 0) + pltpu.roll(w4, n - 2, 0)
        w16 = pltpu.roll(w8, 4, 0) + pltpu.roll(w8, n - 4, 0)
        which = t % 4
        summed = jnp.where(
            which == 0, w2, jnp.where(which == 1, w4, jnp.where(which == 2, w8, w16))
        )[8 : 8 + SPAN, :]
        reach = jnp.where(which == 0, 1, jnp.where(which == 1, 2, jnp.where(which == 2, 4, 8)))
        place = z * rows + b * SPAN + row
        upper = jnp.minimum(place + reach, n_sp * rows)
        lower = jnp.maximum(place - reach, 0)
        differences = summed / (upper - lower).astype(f32) - v[8 : 8 + SPAN, :]
        mapped = jnp.dot(differences.astype(bf16), pmix[t], preferred_element_type=f32)
        mix[at, 128:256] = (mapped * pgain[:, pl.ds(lane0, 128)]).astype(bf16)

    def turn(i):
        for h in (0, 1):
            combine(i, h)
            if i + 1 < len(distances):
                exchange(i + 1, h)

    exchange(0, 0)
    exchange(0, 1)
    within(0)
    within(1)
    turn(0)
    o_rings.step(4)
    within(2)
    within(3)
    turn(1)
    o_rings.step(5)
    within(4)
    within(5)
    o_rings.step(6)
    within(6)
    within(7)
    turn(2)
    for b in range(N_BLOCKS):
        pool(b)
        if b == 2:
            o_rings.step(7)
        if b == 5:
            o_rings.step(8)
    o_rings.finish()
    turn(3)

    forward, backward = excl[0], excl[1]
    entering = [None] * N_BLOCKS
    leaving = [None] * N_BLOCKS
    for i in range(N_BLOCKS):
        b = N_BLOCKS - 1 - i
        entering[i] = forward.astype(bf16)
        leaving[b] = backward.astype(bf16)
        forward = forward * tall(decay, i, 0) + ends[i, 0:128, :]
        backward = backward * tall(decay, b, 2) + ends[b, 128:256, :]
    squares = []
    for b in range(N_BLOCKS):
        at = slice(b * SPAN, (b + 1) * SPAN)
        states = jnp.concatenate([entering[b], leaving[b]], axis=0)
        carried = lax.dot_general(qbuf[at, :], states, NT, preferred_element_type=f32)
        heads_out = (
            ybuf[at, :]
            + carried[:, 0:128] * wide(reach_t, b, 0)
            + carried[:, 128:256] * wide(reach_t, b, 2)
        )
        gated = heads_out * silu(gates[at, :].astype(f32))
        ybuf[at, :] = gated
        squares.append(
            lax.dot_general(
                jnp.ones((8, 128), f32), gated * gated, NT,
                precision=HIGHEST, preferred_element_type=f32,
            )[0:1, :]
        )
    own_squares = jnp.concatenate(squares, axis=0)
    ss_out[...] = own_squares
    ss_copies = []
    for r in range(1, n_tp):
        copy = remote(
            ss_out, ss_in.at[r - 1], ss_send.at[r - 1], ss_recv.at[r - 1],
            {"tp": (t + r) % n_tp},
        )
        copy.start()
        ss_copies.append(copy)
    all_squares = own_squares
    for r in range(1, n_tp):
        ss_copies[r - 1].wait_recv()
        all_squares = all_squares + ss_in[r - 1]
    scale = lax.rsqrt(all_squares / D_SSM + EPSILON)
    scale_t = jnp.concatenate([scale, jnp.zeros((120, 128), f32)], axis=0).T
    mix_gain_here = mgain[:, pl.ds(lane0, 128)]
    for b in range(N_BLOCKS):
        at = slice(b * SPAN, (b + 1) * SPAN)
        mix[at, 0:128] = (ybuf[at, :] * scale_t[:, b : b + 1] * mix_gain_here).astype(bf16)

    def partial(xx, cc, begin=0, count=TOK_ROWS):
        at = pl.multiple_of((xx * 2 + cc) * TOK_ROWS + begin, 16)
        return lax.dot_general(
            mix[pl.ds(at, count), :], wout[...], NT, preferred_element_type=f32
        )

    half = TOK_ROWS // 2
    d_copies = []
    for i, xx in enumerate((xo, xp, xm, x)):
        d_out[i] = partial(xx, 1 - c).astype(bf16)
        copy = remote(d_out.at[i], d_in.at[i], d_send.at[i], d_recv.at[i], to_d)
        copy.start()
        d_copies.append(copy)

    def chip(i, xx, begin, count=half):
        return partial(xx, c, begin, count) + d_in[i, begin : begin + count, :].astype(f32)

    def send(i, value, where, out_ref, in_ref, send_sem, recv_sem):
        out_ref[i] = value.astype(bf16)
        copy = remote(out_ref.at[i], in_ref.at[i], send_sem.at[i], recv_sem.at[i], where)
        copy.start()
        return copy

    relay = (r_out, r_in, r_send, r_recv)
    near = (n_out, n_in, n_send, n_recv)
    d_copies[0].wait_recv()
    relay_p = send(0, chip(0, xo, 0), to_xp, *relay)
    relay_m = send(1, chip(0, xo, half), to_xm, *relay)
    d_copies[1].wait_recv()
    dir_p = send(0, chip(1, xp, half), to_xp, *near)
    d_copies[2].wait_recv()
    dir_m = send(1, chip(2, xm, 0), to_xm, *near)
    relay_p.wait_recv()
    comb_p = send(2, chip(1, xp, 0) + r_in[0].astype(f32), to_xp, *near)
    relay_m.wait_recv()
    comb_m = send(3, chip(2, xm, half) + r_in[1].astype(f32), to_xm, *near)
    d_copies[3].wait_recv()
    top, bottom = chip(3, x, 0), chip(3, x, half)
    dir_p.wait_recv()
    dir_m.wait_recv()
    bottom = bottom + n_in[0].astype(f32)
    top = top + n_in[1].astype(f32)
    comb_p.wait_recv()
    out[0, 0:half, :] = (top + n_in[2].astype(f32)).astype(bf16)
    comb_m.wait_recv()
    out[0, half:TOK_ROWS, :] = (bottom + n_in[3].astype(f32)).astype(bf16)

    for i, d in enumerate(distances):
        for way in (0, 1):
            ok = z + d < n_sp if way == 0 else z >= d

            @pl.when(ok)
            def _():
                for h in (0, 1):
                    message(way, h, i, to_d).wait_send()

    last = [relay_p, relay_m, dir_p, dir_m, comb_p, comb_m]
    for copy in t_sent + w_rings.sent + o_rings.sent + ss_copies + d_copies + last:
        copy.wait_send()


N_TOKEN_SENDS = 27
N_RING_SENDS = 127


def mixer(n_sp, n_fs, n_x, *operands):
    any_spec = pl.BlockSpec(memory_space=pl.ANY)
    vmem = pl.BlockSpec(memory_space=pltpu.VMEM)
    smem = pl.BlockSpec(memory_space=pltpu.SMEM)
    dma = pltpu.SemaphoreType.DMA
    f32, bf16 = jnp.float32, jnp.bfloat16
    rows = N_BLOCKS * SPAN
    half = TOK_ROWS // 2

    def ring_sems():
        return [dma((n,)) for n in (3, 36, 36, 9, 9, 16, 16, 16, N_RING_SENDS)]

    return pl.pallas_call(
        functools.partial(mixer_kernel, n_sp, n_fs, n_x),
        out_shape=jax.ShapeDtypeStruct((1, TOK_ROWS, 2048), bf16),
        in_specs=[any_spec] * 8 + [vmem] + [smem] * 2 + [vmem] * 7,
        out_specs=vmem,
        scratch_shapes=[
            pltpu.VMEM((rows + 2 * HALO, 2048), bf16),
            pltpu.VMEM((rows + 2 * HALO, 2048), bf16),
            pltpu.VMEM((2048, 768), bf16),
            pltpu.VMEM((2048, 256), bf16),
            pltpu.VMEM((rows, 128), bf16),
            pltpu.VMEM((rows, 128), f32),
            pltpu.VMEM((rows + 2 * HALO, 512), f32),
            pltpu.VMEM((rows, 128), f32),
            pltpu.VMEM((rows, 128), bf16),
            pltpu.VMEM((rows, 128), bf16),
            pltpu.VMEM((N_BLOCKS, 256, 128), f32),
            pltpu.VMEM((rows, 128), f32),
            pltpu.VMEM((rows, 256), bf16),
            pltpu.VMEM((2, 128, 128), f32),
            pltpu.VMEM((2, 128, 128), f32),
            pltpu.VMEM((4, 8, 128), f32),
            pltpu.VMEM((4, 8, 128), f32),
            pltpu.VMEM((2, 2, 4, MSG, 128), bf16),
            pltpu.VMEM((2, 2, 4, MSG, 128), bf16),
            pltpu.VMEM((8, 128), f32),
            pltpu.VMEM((7, 8, 128), f32),
            pltpu.VMEM((4, TOK_ROWS, 2048), bf16),
            pltpu.VMEM((4, TOK_ROWS, 2048), bf16),
            pltpu.VMEM((2, half, 2048), bf16),
            pltpu.VMEM((2, half, 2048), bf16),
            pltpu.VMEM((4, half, 2048), bf16),
            pltpu.VMEM((4, half, 2048), bf16),
            dma((8,)), dma((4,)), dma((4,)), dma((4,)), dma((13,)), dma((2,)),
            dma((N_TOKEN_SENDS,)),
            *ring_sems(),
            *ring_sems(),
            dma((2, 2, 4)), dma((2, 2, 4)), dma((7,)), dma((7,)),
            dma((4,)), dma((4,)), dma((2,)), dma((2,)), dma((4,)), dma((4,)),
        ],
        compiler_params=pltpu.CompilerParams(
            collective_id=0, has_side_effects=True, vmem_limit_bytes=56 * 1024 * 1024
        ),
        name="mixer",
    )(*operands)


def local(
    tokens, norm_gain, w_gate, w_value, w_bkey, w_query, w_pool_in, w_step, step_bias,
    decay_rate, decay_shift, conv_value, conv_bkey, conv_query, mix_gain, pool_mix, pool_gain,
    w_out_ssd, w_out_pool,
):
    n_tp, n_sp, n_fs = lax.axis_size("tp"), lax.axis_size("sp"), lax.axis_size("fs")
    heads_dev = DUALITY_HEADS // n_tp
    step_cols = lax.dynamic_slice_in_dim(w_step, lax.axis_index("tp") * heads_dev, heads_dev, 2)
    step_cols = jnp.pad(step_cols.reshape(w_step.shape[0], 2 * heads_dev), ((0, 0), (0, 124)))
    out_turned = jnp.concatenate([w_out_ssd.T, w_out_pool.T], axis=1)
    return mixer(
        n_sp, n_fs, n_tp // 2, tokens, w_gate, w_value, w_bkey, w_query, w_pool_in,
        out_turned, step_cols, norm_gain[None], step_bias, decay_rate, decay_shift,
        conv_value, conv_bkey, conv_query, mix_gain[None], pool_mix, pool_gain[None],
    )


def solution(mesh):
    return jax.shard_map(
        local,
        mesh=mesh,
        in_specs=(
            P("fs", ("sp", "tp"), None),
            P(),
            P(("sp", "fs"), "tp"),
            P(("sp", "fs"), "tp"),
            P(("sp", "fs"), "tp"),
            P(("sp", "fs"), "tp"),
            P(("sp", "fs"), "tp"),
            P(),
            P(),
            P(),
            P("fs", "tp", None, "sp"),
            P(),
            P(),
            P(),
            P(),
            P(),
            P(),
            P("tp", ("sp", "fs")),
            P("tp", ("sp", "fs")),
        ),
        out_specs=P("fs", ("sp", "tp"), None),
        check_vma=False,
    )
```

```python
import functools

import jax
import jax.numpy as jnp
from jax import lax
from jax.experimental import pallas as pl
from jax.experimental.pallas import tpu as pltpu
from jax.sharding import PartitionSpec as P

DUALITY_HEADS = 16
STATE = 128
SPAN = 128
D_SSM = 1024
EPSILON = 1e-06
HIGHEST = lax.Precision.HIGHEST

MESH = pl.DeviceIdType.MESH
HALO = 16
TOK_ROWS = 128
PIECE = 32
NT = (((1,), (1,)), ((), ()))
TN = (((0,), (0,)), ((), ()))
N_BLOCKS = 8
MSG = 64 + 16


def remote(src, dst, send, recv, where):
    return pltpu.make_async_remote_copy(
        src_ref=src, dst_ref=dst, send_sem=send, recv_sem=recv, device_id=where, device_id_type=MESH
    )


def silu(v):
    return v / (1.0 + jnp.exp(-v))


class Rings:

    def __init__(self, buf, a_cols, b_cols, sems, send_sem, place, sizes):
        self.buf, self.a_cols, self.b_cols = buf, a_cols, b_cols
        self.ay, self.azp, self.azm, self.bzp, self.bzm, self.byp, self.bym, self.byo = sems
        self.send_sem, self.sent = send_sem, []
        self.z, self.y = place
        self.n_sp, self.n_fs = sizes
        z, y, n_sp, n_fs = self.z, self.y, *sizes
        self.yp, self.ym, self.yo = (y + 1) % n_fs, (y + n_fs - 1) % n_fs, (y + 2) % n_fs
        self.to_yp, self.to_ym = {"fs": self.yp}, {"fs": self.ym}
        self.to_zp, self.to_zm = {"sp": (z + 1) % n_sp}, {"sp": (z + n_sp - 1) % n_sp}
        self.to_zpp, self.to_zmm = {"sp": (z + 2) % n_sp}, {"sp": (z + n_sp - 2) % n_sp}
        self.half = n_sp // 2
        self.pending = [0]

    def at(self, zz, yy, cols):
        row = pl.multiple_of((zz * self.n_fs + yy) * PIECE, PIECE)
        return self.buf.at[pl.ds(row, PIECE), pl.ds(*cols)]

    def a(self, zz, yy):
        return self.at(zz, yy, self.a_cols)

    def b(self, zz, yy):
        return self.at(zz, yy, self.b_cols)

    def send(self, ref, recv, where):
        copy = remote(ref, ref, self.send_sem.at[len(self.sent)], recv, where)
        copy.start()
        self.sent.append(copy)

    def arrived(self, ref, recv):
        remote(ref, ref, self.send_sem.at[0], recv, self.to_yp).wait_recv()

    def begin(self):
        own_b = self.b(self.z, self.y)
        self.send(own_b, self.bzp.at[2], self.to_zpp)
        self.send(own_b, self.bzm.at[2], self.to_zmm)
        self.send(own_b, self.bzp.at[1], self.to_zp)
        self.send(own_b, self.bzm.at[1], self.to_zm)
        if self.a_cols is not None:
            own_a = self.a(self.z, self.y)
            self.send(own_a, self.ay.at[0], self.to_yp)
            self.send(own_a, self.ay.at[1], self.to_ym)
            self.outward(own_a, 0)
        self.send(own_b, self.byp.at[0], self.to_yp)
        self.send(own_b, self.bym.at[0], self.to_ym)

    def outward(self, ref, j):
        self.send(ref, self.azp.at[8 + j], self.to_zpp)
        self.send(ref, self.azm.at[8 + j], self.to_zmm)
        self.send(ref, self.azp.at[4 + j], self.to_zp)
        self.send(ref, self.azm.at[4 + j], self.to_zm)

    def spread(self):
        for j, yy in ((1, self.ym), (2, self.yp), (3, self.yo)):
            ref = self.a(self.z, yy)
            self.arrived(ref, self.ay.at[j - 1])
            if j == 1:
                self.send(ref, self.ay.at[2], self.to_yp)
            self.outward(ref, j)

    def back(self, o):
        return (self.z + self.n_sp - o) % self.n_sp

    def relay(self, o):
        low, high = self.b(self.back(o), self.ym), self.b(self.back(o), self.yp)
        self.arrived(low, self.byp.at[o])
        if o % 2 == 0:
            self.send(low, self.byo.at[o], self.to_yp)
        self.arrived(high, self.bym.at[o])
        if o % 2 == 1:
            self.send(high, self.byo.at[o], self.to_ym)

    def relay_pending(self):
        for o in self.pending:
            self.relay(o)
        self.pending = []

    def step(self, k, between=None):
        half, fresh = self.half, []
        far = k == half
        for o, recv, mine, where in (
            (k, self.bzp, True, self.to_zpp),
            (self.n_sp - k, self.bzm, False, self.to_zmm),
        ):
            if o in fresh:
                continue
            ref = self.b(self.back(o), self.y)
            self.arrived(ref, recv.at[k])
            if k + 2 < half or (k + 2 == half and mine):
                self.send(ref, recv.at[k + 2], where)
            self.send(ref, self.byp.at[o], self.to_yp)
            self.send(ref, self.bym.at[o], self.to_ym)
            fresh.append(o)
        y_of = (self.y, self.ym, self.yp, self.yo)
        for j in range(4):
            for recv, zz, mine, where in (
                (self.azp, self.back(k), j < 2, self.to_zpp),
                (self.azm, (self.z + k) % self.n_sp, j >= 2, self.to_zmm),
            ):
                if self.a_cols is None or (far and not mine):
                    continue
                ref = self.a(zz, y_of[j])
                self.arrived(ref, recv.at[4 * k + j])
                if k + 2 < half or (k + 2 == half and mine):
                    self.send(ref, recv.at[4 * (k + 2) + j], where)
            if j == 1:
                self.relay_pending()
                if between is not None:
                    between()
        self.pending = fresh

    def finish(self):
        self.relay_pending()
        for o in range(self.n_sp):
            self.arrived(self.b(self.back(o), self.yo), self.byo.at[o])


def mixer_kernel(
    n_sp, n_fs, n_x,
    tok, wg, wv, wk, wq, wp, wo_s, wo_p, wstep_in, gain_in,
    bias_in, rate_in, shift_in, tap_v_in, tap_k_in, tap_q_in, mgain_in, pmix_in, pgain_in,
    out,
    wo_2, wstep, gain, bias, rate, shift, tap_v, tap_k, tap_q, mgain, pmix, pgain, small_sem,
    tokbuf, normbuf, wbuf, wout, gates, raw,
    p32, xbuf, kbuf, qbuf, ends, ybuf, mix,
    incl, excl, itot, etot, msg_out, msg_in, ss_out, ss_in,
    d_out, d_in, r_out, r_in, n_out, n_in,
    local_sem, tp_sem, tm_sem, tr_sem, td_sem, h_sem, t_send,
    w_ay, w_azp, w_azm, w_bzp, w_bzm, w_byp, w_bym, w_byo, w_send,
    o_bzp, o_bzm, o_byp, o_bym, o_byo, o_send,
    msg_send, msg_recv, ss_send, ss_recv, d_send, d_recv, r_send, r_recv, n_send, n_recv,
):
    f32, bf16 = jnp.float32, jnp.bfloat16
    z, y, t = lax.axis_index("sp"), lax.axis_index("fs"), lax.axis_index("tp")
    x, c = t // 2, t % 2
    n_tp = 2 * n_x
    xp, xm, xo = (x + 1) % n_x, (x + n_x - 1) % n_x, (x + 2) % n_x
    to_xp, to_xm, to_d = {"tp": xp * 2 + c}, {"tp": xm * 2 + c}, {"tp": x * 2 + 1 - c}
    to_zp, to_zm = {"sp": (z + 1) % n_sp}, {"sp": (z + n_sp - 1) % n_sp}
    distances = [1, 2, 4, 8]
    rows = N_BLOCKS * SPAN

    w_rings = Rings(
        wbuf, (0, 128), (128, 512),
        (w_ay, w_azp, w_azm, w_bzp, w_bzm, w_byp, w_bym, w_byo), w_send, (z, y), (n_sp, n_fs),
    )
    o_rings = Rings(
        wout, None, (0, 256),
        (None, None, None, o_bzp, o_bzm, o_byp, o_bym, o_byo), o_send, (z, y), (n_sp, n_fs),
    )

    def t_at(xx, cc, q=0, count=PIECE):
        row = pl.multiple_of(HALO + (xx * 2 + cc) * TOK_ROWS + q * PIECE, 16)
        return tokbuf.at[pl.ds(row, count), :]

    own_row = pl.ds(pl.multiple_of((z * n_fs + y) * PIECE, PIECE), PIECE)
    locals_ = [
        pltpu.make_async_copy(w, wbuf.at[own_row, pl.ds(i * 128, 128)], local_sem.at[i])
        for i, w in enumerate((wg, wv, wk, wq, wp))
    ]
    locals_.append(pltpu.make_async_copy(tok.at[0], t_at(x, c, 0, TOK_ROWS), local_sem.at[5]))
    lane0 = pl.multiple_of(t * 128, 128)
    here = pl.ds(lane0, 128)
    small = [
        pltpu.make_async_copy(src, dst, small_sem.at[i])
        for i, (src, dst) in enumerate(
            (
                (gain_in, gain), (wo_s, wo_2.at[0]), (wo_p, wo_2.at[1]), (wstep_in, wstep),
                (bias_in, bias), (rate_in, rate), (shift_in, shift),
                (tap_v_in.at[:, here], tap_v), (tap_k_in.at[:, here], tap_k),
                (tap_q_in.at[:, here], tap_q), (mgain_in.at[:, here], mgain),
                (pmix_in.at[t], pmix), (pgain_in.at[:, here], pgain),
            )
        )
    ]
    for copy in locals_ + small:
        copy.start()

    barrier = pltpu.get_barrier_semaphore()
    partners = [
        to_xp, to_xm, to_d, to_zp, to_zm, w_rings.to_zpp, w_rings.to_zmm,
        w_rings.to_yp, w_rings.to_ym,
    ]
    for where in partners:
        pl.semaphore_signal(barrier, inc=1, device_id=where, device_id_type=MESH)
    pl.semaphore_wait(barrier, len(partners))

    t_sent = []

    def t_go(src, dst, recv, where):
        copy = remote(src, dst, t_send.at[len(t_sent)], recv, where)
        copy.start()
        t_sent.append(copy)

    def t_came(ref, recv):
        remote(ref, ref, t_send.at[0], recv, to_d).wait_recv()

    def relay_tokens(xx, q, recv, where, onward, slot):
        ref = t_at(xx, c, q)
        t_came(ref, recv)
        if onward:
            t_go(ref, ref, tr_sem.at[q], where)
        t_go(ref, ref, td_sem.at[slot + q], to_d)

    def norm_rows(begin, count):
        part = tokbuf[pl.ds(begin, count), :].astype(f32)
        scaling = lax.rsqrt(jnp.mean(part * part, axis=-1, keepdims=True) + EPSILON)
        normbuf[pl.ds(begin, count), :] = (part * scaling * gain[...]).astype(bf16)

    def norm_block(xx, cc):
        norm_rows(pl.multiple_of(HALO + (xx * 2 + cc) * TOK_ROWS, 16), TOK_ROWS)

    cs = 1 - c

    def token_step(k):
        if k <= 4:
            q = k - 1
            relay_tokens(xm, q, tp_sem.at[q], to_xp, q < 2, 0)
            q = (2, 3, 0, 1)[k - 1]
            relay_tokens(xp, q, tm_sem.at[q], to_xm, q >= 2, 4)
            if k == 2:
                norm_block(x, c)
            if k == 3:
                t_came(t_at(x, cs, 0, TOK_ROWS), td_sem.at[12])
                norm_block(x, cs)
        elif k <= 6:
            for q in (k - 5, k - 3):
                relay_tokens(xo, q, tr_sem.at[q], to_d, False, 8)
            norm_block(xm if k == 5 else xp, c)
        elif k == 7:
            for q in range(4):
                t_came(t_at(xm, cs, q), td_sem.at[q])
                t_came(t_at(xp, cs, q), td_sem.at[4 + q])
            norm_block(xm, cs)
            norm_block(xp, cs)
        else:
            norm_block(xo, c)

    for copy in locals_[:5]:
        copy.wait()
    w_rings.begin()
    locals_[5].wait()
    for q in (0, 1, 2, 3):
        t_go(t_at(x, c, q), t_at(x, c, q), tp_sem.at[q], to_xp)
    for q in (2, 3, 0, 1):
        t_go(t_at(x, c, q), t_at(x, c, q), tm_sem.at[q], to_xm)
    t_go(t_at(x, c, 0, TOK_ROWS), t_at(x, c, 0, TOK_ROWS), td_sem.at[12], to_d)
    w_rings.spread()
    for copy in small:
        copy.wait()
    for i in (0, 1):
        turned = jnp.concatenate([wo_2[i].astype(f32), jnp.zeros((128, 96), f32)], axis=1).T
        wout[own_row, i * 128 : (i + 1) * 128] = turned[0:PIECE, :].astype(bf16)
    wbuf[:, 640:768] = jnp.concatenate([wstep[...], jnp.zeros((2048, 124), bf16)], axis=1)
    for k in range(1, n_sp // 2 + 1):
        w_rings.step(k, functools.partial(token_step, k))
    for q in range(4):
        t_came(t_at(xo, cs, q), td_sem.at[8 + q])
    before, after = tokbuf.at[pl.ds(0, HALO), :], tokbuf.at[pl.ds(HALO + rows, HALO), :]
    t_go(tokbuf.at[pl.ds(rows, HALO), :], before, h_sem.at[0], to_zp)
    t_go(tokbuf.at[pl.ds(HALO, HALO), :], after, h_sem.at[1], to_zm)
    w_rings.relay_pending()
    o_rings.begin()
    norm_block(xo, cs)
    w_rings.finish()

    def rounded(v):
        return v.astype(bf16).astype(f32)

    def project(i):
        at = HALO + i * 256
        dots = jnp.dot(normbuf[at : at + 256, :], wbuf[...], preferred_element_type=f32)
        gates[i * 256 : (i + 1) * 256, :] = dots[:, 0:128].astype(bf16)
        p32[at : at + 256, :] = rounded(dots[:, 128:640])
        raw[i * 256 : (i + 1) * 256, :] = dots[:, 640:768]

    project(0)
    project(1)
    project(2)
    project(3)
    t_came(before, h_sem.at[0])
    t_came(after, h_sem.at[1])
    for begin, real in ((0, z > 0), (HALO + rows, z < n_sp - 1)):
        norm_rows(begin, HALO)
        edge = jnp.dot(
            normbuf[begin : begin + HALO, :], wbuf[:, 128:640], preferred_element_type=f32
        )
        p32[begin : begin + HALO, :] = jnp.where(real, rounded(edge), 0.0)

    row8 = lax.broadcasted_iota(jnp.int32, (8, 128), 0)

    def by_kind(parts):
        found = jnp.zeros((8, 128), f32)
        for i, part in enumerate(parts):
            found = jnp.where(row8 == i, part, found)
        return found

    kinds = ((0, 0), (0, 1), (1, 0), (1, 1))
    bias8 = by_kind([bias[r, 2 * t + h] for r, h in kinds])
    rate8 = by_kind([rate[r, 2 * t + h] for r, h in kinds])
    steps_l, logs_l = [], []
    for b in range(N_BLOCKS):
        cols = raw[b * SPAN : (b + 1) * SPAN, :].T[0:8, :] + bias8
        steps = jnp.maximum(cols, 0.0) + jnp.log1p(jnp.exp(-jnp.abs(cols)))
        moved = by_kind([shift[0, h, r : r + 1, b * SPAN : (b + 1) * SPAN] for r, h in kinds])
        steps_l.append(steps)
        logs_l.append(jnp.where(row8 < 4, -rate8 * steps - moved, 0.0))
    steps = jnp.concatenate(steps_l, axis=0)
    logs = jnp.concatenate(logs_l, axis=0)
    lane = lax.broadcasted_iota(jnp.int32, (64, 128), 1)
    kind = lax.broadcasted_iota(jnp.int32, (64, 128), 0) % 8
    prefix, suffix = logs, logs
    for k in (1, 2, 4, 8, 16, 32, 64):
        prefix = prefix + jnp.where(lane >= k, pltpu.roll(prefix, k, 1), 0.0)
        suffix = suffix + jnp.where(lane < 128 - k, pltpu.roll(suffix, 128 - k, 1), 0.0)
    cum = jnp.where(kind < 2, prefix, suffix)
    total = jnp.broadcast_to(jnp.sum(logs, axis=1, keepdims=True), (64, 128))
    tail = jnp.exp(jnp.minimum(total - cum, 0.0)) * steps
    decay = jnp.exp(total)
    cum_tail_t = jnp.concatenate([cum, tail], axis=0).T
    reach_t = jnp.concatenate([jnp.exp(cum), jnp.zeros((64, 128), f32)], axis=0).T

    def wide(cols, b, first):
        j = b * 8 + first
        left = jnp.broadcast_to(cols[:, j : j + 1], (128, 64))
        right = jnp.broadcast_to(cols[:, j + 1 : j + 2], (128, 64))
        return jnp.concatenate([left, right], axis=1)

    def tall(rows_, b, first):
        j = b * 8 + first
        top = jnp.broadcast_to(rows_[j : j + 1, :], (64, 128))
        bottom = jnp.broadcast_to(rows_[j + 1 : j + 2, :], (64, 128))
        return jnp.concatenate([top, bottom], axis=0)

    def window(b, j):
        begin = HALO - 8 + b * SPAN
        return p32[begin : begin + SPAN + 16, j * 128 : (j + 1) * 128]

    def conv(b, j, taps):
        v = window(b, j)
        weights = taps[...].astype(f32)
        total_ = v * weights[2:3, :]
        for i in (0, 1, 3, 4):
            total_ = total_ + pltpu.roll(v, (2 - i) % (SPAN + 16), 0) * weights[i : i + 1, :]
        return silu(total_[8 : 8 + SPAN, :])

    for b in range(N_BLOCKS):
        at = slice(b * SPAN, (b + 1) * SPAN)
        values = conv(b, 0, tap_v)
        keys = conv(b, 1, tap_k).astype(bf16)
        xbuf[at, :] = values
        kbuf[at, :] = keys
        both = jnp.concatenate(
            [values * wide(cum_tail_t, b, 64), values * wide(cum_tail_t, b, 66)], axis=1
        )
        ends[b] = lax.dot_general(both.astype(bf16), keys, TN, preferred_element_type=f32)

    forward = ends[0, 0:128, :]
    backward = ends[N_BLOCKS - 1, 128:256, :]
    for i in range(1, N_BLOCKS):
        b = N_BLOCKS - 1 - i
        forward = forward * tall(decay, i, 0) + ends[i, 0:128, :]
        backward = backward * tall(decay, b, 2) + ends[b, 128:256, :]
    sums = total[0:8, :]
    for b in range(1, N_BLOCKS):
        sums = sums + total[b * 8 : b * 8 + 8, :]
    incl[0] = forward
    incl[1] = backward
    excl[...] = jnp.zeros_like(excl)
    itot[...] = jnp.broadcast_to(sums[None], (4, 8, 128))
    etot[...] = jnp.zeros_like(etot)

    def message(way, h, i, where):
        return remote(
            msg_out.at[way, h, i], msg_in.at[way, h, i],
            msg_send.at[way, h, i], msg_recv.at[way, h, i], where,
        )

    def exchange(i, h):
        d = distances[i]
        for way in (0, 1):
            ok = z + d < n_sp if way == 0 else z >= d
            logs8 = itot[2 * way + h]
            high = logs8.astype(bf16)
            low = (logs8 - high.astype(f32)).astype(bf16)
            msg_out[way, h, i, 0:64, :] = incl[way, h * 64 : (h + 1) * 64, :].astype(bf16)
            msg_out[way, h, i, 64:MSG, :] = jnp.concatenate([high, low], axis=0)
            where = {"sp": (z + d) % n_sp if way == 0 else (z + n_sp - d) % n_sp}

            @pl.when(ok)
            def _():
                message(way, h, i, where).start()

    def combine(i, h):
        d = distances[i]
        for way in (0, 1):
            ok = z >= d if way == 0 else z + d < n_sp
            s, r, part = 2 * way + h, 2 * way + h, slice(h * 64, (h + 1) * 64)

            @pl.when(ok)
            def _():
                message(way, h, i, to_d).wait_recv()
                state = msg_in[way, h, i, 0:64, :].astype(f32)
                pair = msg_in[way, h, i, 64:MSG, :].astype(f32)
                logs8 = pair[0:8, :] + pair[8:16, :]
                incl[way, part, :] = incl[way, part, :] + jnp.exp(itot[s][r : r + 1, :]) * state
                itot[s] = itot[s] + logs8
                excl[way, part, :] = excl[way, part, :] + jnp.exp(etot[s][r : r + 1, :]) * state
                etot[s] = etot[s] + logs8

    row = lax.broadcasted_iota(jnp.int32, (128, 128), 0)
    col = lax.broadcasted_iota(jnp.int32, (128, 128), 1)

    def within(b):
        at = slice(b * SPAN, (b + 1) * SPAN)
        queries = conv(b, 2, tap_q).astype(bf16)
        qbuf[at, :] = queries
        scores = lax.dot_general(queries, kbuf[at, :], NT, preferred_element_type=f32)
        masked = []
        for h in (0, 1):
            jf, jb = b * 8 + h, b * 8 + 2 + h
            ahead = cum_tail_t[:, jf : jf + 1] - cum[jf : jf + 1, :]
            behind = cum_tail_t[:, jb : jb + 1] - cum[jb : jb + 1, :]
            gaps = jnp.where(col < row, ahead, jnp.where(col > row, behind, 0.0))
            df, db = steps[jf : jf + 1, :], steps[jb : jb + 1, :]
            sizes = jnp.where(col < row, df, jnp.where(col > row, db, df + db))
            masked.append((scores * jnp.exp(jnp.minimum(gaps, 0.0)) * sizes).astype(bf16))
        values = xbuf[at, :]
        stacked = jnp.concatenate(
            [jnp.where(col < 64, values, 0.0), jnp.where(col >= 64, values, 0.0)], axis=0
        ).astype(bf16)
        ybuf[at, :] = jnp.dot(
            jnp.concatenate(masked, axis=1), stacked, preferred_element_type=f32
        )

    def pool(b):
        at = slice(b * SPAN, (b + 1) * SPAN)
        n = SPAN + 16
        v = window(b, 3)
        w2 = v + pltpu.roll(v, 1, 0)
        w4 = pltpu.roll(w2, 1, 0) + pltpu.roll(w2, n - 1, 0)
        w8 = pltpu.roll(w4, 2, 0) + pltpu.roll(w4, n - 2, 0)
        w16 = pltpu.roll(w8, 4, 0) + pltpu.roll(w8, n - 4, 0)
        which = t % 4
        summed = jnp.where(
            which == 0, w2, jnp.where(which == 1, w4, jnp.where(which == 2, w8, w16))
        )[8 : 8 + SPAN, :]
        reach = jnp.where(which == 0, 1, jnp.where(which == 1, 2, jnp.where(which == 2, 4, 8)))
        place = z * rows + b * SPAN + row
        upper = jnp.minimum(place + reach, n_sp * rows)
        lower = jnp.maximum(place - reach, 0)
        differences = summed / (upper - lower).astype(f32) - v[8 : 8 + SPAN, :]
        mapped = jnp.dot(differences.astype(bf16), pmix[...], preferred_element_type=f32)
        mix[at, 128:256] = (mapped * pgain[...]).astype(bf16)

    def turn(i):
        for h in (0, 1):
            combine(i, h)
            if i + 1 < len(distances):
                exchange(i + 1, h)

    exchange(0, 0)
    exchange(0, 1)
    o_rings.step(1)
    o_rings.step(2)
    within(0)
    within(1)
    turn(0)
    o_rings.step(3)
    o_rings.step(4)
    within(2)
    within(3)
    turn(1)
    o_rings.step(5)
    o_rings.step(6)
    within(4)
    within(5)
    within(6)
    within(7)
    turn(2)
    o_rings.step(7)
    o_rings.step(8)
    for b in range(N_BLOCKS):
        pool(b)
    o_rings.finish()
    turn(3)

    forward, backward = excl[0], excl[1]
    entering = [None] * N_BLOCKS
    leaving = [None] * N_BLOCKS
    for i in range(N_BLOCKS):
        b = N_BLOCKS - 1 - i
        entering[i] = forward.astype(bf16)
        leaving[b] = backward.astype(bf16)
        forward = forward * tall(decay, i, 0) + ends[i, 0:128, :]
        backward = backward * tall(decay, b, 2) + ends[b, 128:256, :]
    squares = []
    for b in range(N_BLOCKS):
        at = slice(b * SPAN, (b + 1) * SPAN)
        states = jnp.concatenate([entering[b], leaving[b]], axis=0)
        carried = lax.dot_general(qbuf[at, :], states, NT, preferred_element_type=f32)
        heads_out = (
            ybuf[at, :]
            + carried[:, 0:128] * wide(reach_t, b, 0)
            + carried[:, 128:256] * wide(reach_t, b, 2)
        )
        gated = heads_out * silu(gates[at, :].astype(f32))
        ybuf[at, :] = gated
        squares.append(
            lax.dot_general(
                jnp.ones((8, 128), f32), gated * gated, NT,
                precision=HIGHEST, preferred_element_type=f32,
            )[0:1, :]
        )
    own_squares = jnp.concatenate(squares, axis=0)
    ss_out[...] = own_squares
    ss_copies = []
    for r in range(1, n_tp):
        copy = remote(
            ss_out, ss_in.at[r - 1], ss_send.at[r - 1], ss_recv.at[r - 1],
            {"tp": (t + r) % n_tp},
        )
        copy.start()
        ss_copies.append(copy)
    all_squares = own_squares
    for r in range(1, n_tp):
        ss_copies[r - 1].wait_recv()
        all_squares = all_squares + ss_in[r - 1]
    scale = lax.rsqrt(all_squares / D_SSM + EPSILON)
    scale_t = jnp.concatenate([scale, jnp.zeros((120, 128), f32)], axis=0).T
    mix_gain_here = mgain[...]
    for b in range(N_BLOCKS):
        at = slice(b * SPAN, (b + 1) * SPAN)
        mix[at, 0:128] = (ybuf[at, :] * scale_t[:, b : b + 1] * mix_gain_here).astype(bf16)

    def partial(xx, cc, begin=0, count=TOK_ROWS):
        at = pl.multiple_of((xx * 2 + cc) * TOK_ROWS + begin, 16)
        return lax.dot_general(
            mix[pl.ds(at, count), :], wout[...], NT, preferred_element_type=f32
        )

    half = TOK_ROWS // 2
    d_copies = []
    for i, xx in enumerate((xo, xp, xm, x)):
        d_out[i] = partial(xx, 1 - c).astype(bf16)
        copy = remote(d_out.at[i], d_in.at[i], d_send.at[i], d_recv.at[i], to_d)
        copy.start()
        d_copies.append(copy)

    def chip(i, xx, begin, count=half):
        return partial(xx, c, begin, count) + d_in[i, begin : begin + count, :].astype(f32)

    def send(i, value, where, out_ref, in_ref, send_sem, recv_sem):
        out_ref[i] = value.astype(bf16)
        copy = remote(out_ref.at[i], in_ref.at[i], send_sem.at[i], recv_sem.at[i], where)
        copy.start()
        return copy

    relay = (r_out, r_in, r_send, r_recv)
    near = (n_out, n_in, n_send, n_recv)
    d_copies[0].wait_recv()
    relay_p = send(0, chip(0, xo, 0), to_xp, *relay)
    relay_m = send(1, chip(0, xo, half), to_xm, *relay)
    d_copies[1].wait_recv()
    dir_p = send(0, chip(1, xp, half), to_xp, *near)
    d_copies[2].wait_recv()
    dir_m = send(1, chip(2, xm, 0), to_xm, *near)
    relay_p.wait_recv()
    comb_p = send(2, chip(1, xp, 0) + r_in[0].astype(f32), to_xp, *near)
    relay_m.wait_recv()
    comb_m = send(3, chip(2, xm, half) + r_in[1].astype(f32), to_xm, *near)
    d_copies[3].wait_recv()
    top, bottom = chip(3, x, 0), chip(3, x, half)
    dir_p.wait_recv()
    dir_m.wait_recv()
    bottom = bottom + n_in[0].astype(f32)
    top = top + n_in[1].astype(f32)
    comb_p.wait_recv()
    out[0, 0:half, :] = (top + n_in[2].astype(f32)).astype(bf16)
    comb_m.wait_recv()
    out[0, half:TOK_ROWS, :] = (bottom + n_in[3].astype(f32)).astype(bf16)

    for i, d in enumerate(distances):
        for way in (0, 1):
            ok = z + d < n_sp if way == 0 else z >= d

            @pl.when(ok)
            def _():
                for h in (0, 1):
                    message(way, h, i, to_d).wait_send()

    last = [relay_p, relay_m, dir_p, dir_m, comb_p, comb_m]
    for copy in t_sent + w_rings.sent + o_rings.sent + ss_copies + d_copies + last:
        copy.wait_send()


N_TOKEN_SENDS = 27
N_RING_SENDS = 127


def mixer(n_sp, n_fs, n_x, *operands):
    any_spec = pl.BlockSpec(memory_space=pl.ANY)
    vmem = pl.BlockSpec(memory_space=pltpu.VMEM)
    dma = pltpu.SemaphoreType.DMA
    f32, bf16 = jnp.float32, jnp.bfloat16
    rows = N_BLOCKS * SPAN
    half = TOK_ROWS // 2

    def ring_sems(counts):
        return [dma((n,)) for n in counts]

    return pl.pallas_call(
        functools.partial(mixer_kernel, n_sp, n_fs, n_x),
        out_shape=jax.ShapeDtypeStruct((1, TOK_ROWS, 2048), bf16),
        in_specs=[any_spec] * 19,
        out_specs=vmem,
        scratch_shapes=[
            pltpu.VMEM((2, 128, 32), bf16),
            pltpu.VMEM((2048, 4), bf16),
            pltpu.VMEM((1, 2048), f32),
            pltpu.SMEM((2, 16), f32),
            pltpu.SMEM((2, 16), f32),
            pltpu.VMEM((1, 2, 2, 1024), f32),
            pltpu.VMEM((5, 128), bf16),
            pltpu.VMEM((5, 128), bf16),
            pltpu.VMEM((5, 128), bf16),
            pltpu.VMEM((1, 128), f32),
            pltpu.VMEM((128, 128), bf16),
            pltpu.VMEM((1, 128), f32),
            dma((13,)),
            pltpu.VMEM((rows + 2 * HALO, 2048), bf16),
            pltpu.VMEM((rows + 2 * HALO, 2048), bf16),
            pltpu.VMEM((2048, 768), bf16),
            pltpu.VMEM((2048, 256), bf16),
            pltpu.VMEM((rows, 128), bf16),
            pltpu.VMEM((rows, 128), f32),
            pltpu.VMEM((rows + 2 * HALO, 512), f32),
            pltpu.VMEM((rows, 128), f32),
            pltpu.VMEM((rows, 128), bf16),
            pltpu.VMEM((rows, 128), bf16),
            pltpu.VMEM((N_BLOCKS, 256, 128), f32),
            pltpu.VMEM((rows, 128), f32),
            pltpu.VMEM((rows, 256), bf16),
            pltpu.VMEM((2, 128, 128), f32),
            pltpu.VMEM((2, 128, 128), f32),
            pltpu.VMEM((4, 8, 128), f32),
            pltpu.VMEM((4, 8, 128), f32),
            pltpu.VMEM((2, 2, 4, MSG, 128), bf16),
            pltpu.VMEM((2, 2, 4, MSG, 128), bf16),
            pltpu.VMEM((8, 128), f32),
            pltpu.VMEM((7, 8, 128), f32),
            pltpu.VMEM((4, TOK_ROWS, 2048), bf16),
            pltpu.VMEM((4, TOK_ROWS, 2048), bf16),
            pltpu.VMEM((2, half, 2048), bf16),
            pltpu.VMEM((2, half, 2048), bf16),
            pltpu.VMEM((4, half, 2048), bf16),
            pltpu.VMEM((4, half, 2048), bf16),
            dma((6,)), dma((4,)), dma((4,)), dma((4,)), dma((13,)), dma((2,)),
            dma((N_TOKEN_SENDS,)),
            *ring_sems((3, 36, 36, 9, 9, 16, 16, 16, N_RING_SENDS)),
            *ring_sems((9, 9, 16, 16, 16, N_RING_SENDS)),
            dma((2, 2, 4)), dma((2, 2, 4)), dma((7,)), dma((7,)),
            dma((4,)), dma((4,)), dma((2,)), dma((2,)), dma((4,)), dma((4,)),
        ],
        compiler_params=pltpu.CompilerParams(
            collective_id=0, has_side_effects=True, vmem_limit_bytes=56 * 1024 * 1024
        ),
        name="mixer",
    )(*operands)


def local(
    tokens, norm_gain, w_gate, w_value, w_bkey, w_query, w_pool_in, w_step, step_bias,
    decay_rate, decay_shift, conv_value, conv_bkey, conv_query, mix_gain, pool_mix, pool_gain,
    w_out_ssd, w_out_pool,
):
    n_tp, n_sp, n_fs = lax.axis_size("tp"), lax.axis_size("sp"), lax.axis_size("fs")
    heads_dev = DUALITY_HEADS // n_tp
    step_cols = lax.dynamic_slice_in_dim(w_step, lax.axis_index("tp") * heads_dev, heads_dev, 2)
    step_cols = step_cols.reshape(w_step.shape[0], 2 * heads_dev)
    return mixer(
        n_sp, n_fs, n_tp // 2, tokens, w_gate, w_value, w_bkey, w_query, w_pool_in,
        w_out_ssd, w_out_pool, step_cols, norm_gain[None], step_bias, decay_rate, decay_shift,
        conv_value, conv_bkey, conv_query, mix_gain[None], pool_mix, pool_gain[None],
    )


def solution(mesh):
    return jax.shard_map(
        local,
        mesh=mesh,
        in_specs=(
            P("fs", ("sp", "tp"), None),
            P(),
            P(("sp", "fs"), "tp"),
            P(("sp", "fs"), "tp"),
            P(("sp", "fs"), "tp"),
            P(("sp", "fs"), "tp"),
            P(("sp", "fs"), "tp"),
            P(),
            P(),
            P(),
            P("fs", "tp", None, "sp"),
            P(),
            P(),
            P(),
            P(),
            P(),
            P(),
            P("tp", ("sp", "fs")),
            P("tp", ("sp", "fs")),
        ),
        out_specs=P("fs", ("sp", "tp"), None),
        check_vma=False,
    )
```

```python
import functools

import jax
import jax.numpy as jnp
from jax import lax
from jax.experimental import pallas as pl
from jax.experimental.pallas import tpu as pltpu
from jax.sharding import PartitionSpec as P

DUALITY_HEADS = 16
STATE = 128
SPAN = 128
D_SSM = 1024
EPSILON = 1e-06
HIGHEST = lax.Precision.HIGHEST

MESH = pl.DeviceIdType.MESH
HALO = 16
TOK_ROWS = 128
PIECE = 32
NT = (((1,), (1,)), ((), ()))
TN = (((0,), (0,)), ((), ()))
N_BLOCKS = 8
MSG = 64 + 16


def remote(src, dst, send, recv, where):
    return pltpu.make_async_remote_copy(
        src_ref=src, dst_ref=dst, send_sem=send, recv_sem=recv, device_id=where, device_id_type=MESH
    )


def silu(v):
    return v / (1.0 + jnp.exp(-v))


class Rings:

    def __init__(self, buf, cols, stride, sems, send_sem, place, sizes):
        self.buf, self.cols, self.stride = buf, cols, stride
        self.zp_sem, self.zm_sem, self.yp_sem, self.ym_sem, self.yo_sem = sems
        self.send_sem, self.sent = send_sem, []
        self.z, self.y = place
        self.n_sp, self.n_fs = sizes
        z, y, n_sp, n_fs = self.z, self.y, *sizes
        self.yp, self.ym, self.yo = (y + 1) % n_fs, (y + n_fs - 1) % n_fs, (y + 2) % n_fs
        self.to_yp, self.to_ym = {"fs": self.yp}, {"fs": self.ym}
        self.half = n_sp // 2

    def at(self, o, yy):
        zz = (self.z + self.n_sp - o) % self.n_sp
        row = pl.multiple_of((zz * self.n_fs + yy) * PIECE, PIECE)
        return self.buf.at[pl.ds(row, PIECE), pl.ds(*self.cols)]

    def send(self, ref, recv, where):
        copy = remote(ref, ref, self.send_sem.at[len(self.sent)], recv, where)
        copy.start()
        self.sent.append(copy)

    def arrived(self, ref, recv):
        remote(ref, ref, self.send_sem.at[0], recv, self.to_yp).wait_recv()

    def up(self, ref, k, stride):
        if k <= self.half:
            self.send(ref, self.zp_sem.at[k], {"sp": (self.z + stride) % self.n_sp})

    def down(self, ref, k, stride):
        if k < self.half:
            self.send(ref, self.zm_sem.at[k], {"sp": (self.z + self.n_sp - stride) % self.n_sp})

    def begin(self):
        own = self.at(0, self.y)
        for k in range(self.stride, 0, -1):
            self.up(own, k, k)
            self.down(own, k, k)

    def places(self, k):
        if k == 0:
            return (0,)
        return (k, self.n_sp - k) if k < self.half else (k,)

    def along_z(self, k):
        ref = self.at(k, self.y)
        self.arrived(ref, self.zp_sem.at[k])
        self.up(ref, k + self.stride, self.stride)
        if k < self.half:
            ref = self.at(self.n_sp - k, self.y)
            self.arrived(ref, self.zm_sem.at[k])
            self.down(ref, k + self.stride, self.stride)

    def along_y(self, k):
        for o in self.places(k):
            ref = self.at(o, self.y)
            self.send(ref, self.yp_sem.at[o], self.to_yp)
            self.send(ref, self.ym_sem.at[o], self.to_ym)

    def relay(self, k):
        for o in self.places(k):
            low, high = self.at(o, self.ym), self.at(o, self.yp)
            self.arrived(low, self.yp_sem.at[o])
            if o % 2 == 0:
                self.send(low, self.yo_sem.at[o], self.to_yp)
            self.arrived(high, self.ym_sem.at[o])
            if o % 2 == 1:
                self.send(high, self.yo_sem.at[o], self.to_ym)

    def finish(self):
        for o in range(self.n_sp):
            self.arrived(self.at(o, self.yo), self.yo_sem.at[o])


def mixer_kernel(
    n_sp, n_fs, n_x,
    tok, wg, wv, wk, wq, wp, wo_s, wo_p, wstep_in, gain_in,
    bias_in, rate_in, shift_in, tap_v_in, tap_k_in, tap_q_in, mgain_in, pmix_in, pgain_in,
    out,
    wo_2, wstep, gain, bias, rate, shift, tap_v, tap_k, tap_q, mgain, pmix, pgain, small_sem,
    tokbuf, normbuf, wbuf, obuf, gates, raw,
    p32, xbuf, kbuf, qbuf, ends, ybuf, mix,
    incl, excl, itot, etot, msg_out, msg_in, ss_out, ss_in,
    d_out, d_in, r_out, r_in, n_out, n_in,
    local_sem, tp_sem, tm_sem, tr_sem, td_sem, h_sem, t_send,
    w_zp, w_zm, w_yp, w_ym, w_yo, w_send,
    o_zp, o_zm, o_yp, o_ym, o_yo, o_send,
    msg_send, msg_recv, ss_send, ss_recv, d_send, d_recv, r_send, r_recv, n_send, n_recv,
):
    f32, bf16 = jnp.float32, jnp.bfloat16
    z, y, t = lax.axis_index("sp"), lax.axis_index("fs"), lax.axis_index("tp")
    x, c = t // 2, t % 2
    n_tp = 2 * n_x
    xp, xm, xo = (x + 1) % n_x, (x + n_x - 1) % n_x, (x + 2) % n_x
    to_xp, to_xm, to_d = {"tp": xp * 2 + c}, {"tp": xm * 2 + c}, {"tp": x * 2 + 1 - c}
    to_zp, to_zm = {"sp": (z + 1) % n_sp}, {"sp": (z + n_sp - 1) % n_sp}
    distances = [1, 2, 4, 8]
    rows = N_BLOCKS * SPAN

    w_rings = Rings(
        wbuf, (0, 256), 2, (w_zp, w_zm, w_yp, w_ym, w_yo), w_send, (z, y), (n_sp, n_fs)
    )
    o_rings = Rings(
        obuf, (0, 640), 2, (o_zp, o_zm, o_yp, o_ym, o_yo), o_send, (z, y), (n_sp, n_fs)
    )

    def t_at(xx, cc, q=0, count=PIECE):
        row = pl.multiple_of(HALO + (xx * 2 + cc) * TOK_ROWS + q * PIECE, 16)
        return tokbuf.at[pl.ds(row, count), :]

    own_row = pl.ds(pl.multiple_of((z * n_fs + y) * PIECE, PIECE), PIECE)
    shards = (
        (wv, wbuf, 0), (wk, wbuf, 1), (wg, obuf, 0), (wq, obuf, 1), (wp, obuf, 2)
    )
    locals_ = [
        pltpu.make_async_copy(w, buf.at[own_row, pl.ds(i * 128, 128)], local_sem.at[n])
        for n, (w, buf, i) in enumerate(shards)
    ]
    locals_.append(pltpu.make_async_copy(tok.at[0], t_at(x, c, 0, TOK_ROWS), local_sem.at[5]))
    lane0 = pl.multiple_of(t * 128, 128)
    here = pl.ds(lane0, 128)
    small = [
        pltpu.make_async_copy(src, dst, small_sem.at[i])
        for i, (src, dst) in enumerate(
            (
                (gain_in, gain), (wo_s, wo_2.at[0]), (wo_p, wo_2.at[1]), (wstep_in, wstep),
                (bias_in, bias), (rate_in, rate), (shift_in, shift),
                (tap_v_in.at[:, here], tap_v), (tap_k_in.at[:, here], tap_k),
                (tap_q_in.at[:, here], tap_q), (mgain_in.at[:, here], mgain),
                (pmix_in.at[t], pmix), (pgain_in.at[:, here], pgain),
            )
        )
    ]
    for copy in locals_ + small:
        copy.start()

    barrier = pltpu.get_barrier_semaphore()
    partners = [
        to_xp, to_xm, to_d, to_zp, to_zm, {"sp": (z + 2) % n_sp}, {"sp": (z + n_sp - 2) % n_sp},
        w_rings.to_yp, w_rings.to_ym,
    ]
    for where in partners:
        pl.semaphore_signal(barrier, inc=1, device_id=where, device_id_type=MESH)
    for copy in small:
        copy.wait()
    for i in (0, 1):
        turned = jnp.concatenate([wo_2[i].astype(f32), jnp.zeros((128, 96), f32)], axis=1).T
        begin = 384 + i * 128
        obuf[own_row, begin : begin + 128] = turned[0:PIECE, :].astype(bf16)
    wbuf[:, 256:384] = jnp.concatenate([wstep[...], jnp.zeros((2048, 124), bf16)], axis=1)
    pl.semaphore_wait(barrier, len(partners))

    t_sent = []

    def t_go(src, dst, recv, where):
        copy = remote(src, dst, t_send.at[len(t_sent)], recv, where)
        copy.start()
        t_sent.append(copy)

    def t_came(ref, recv):
        remote(ref, ref, t_send.at[0], recv, to_d).wait_recv()

    def relay_tokens(xx, q, recv, where, onward, slot):
        ref = t_at(xx, c, q)
        t_came(ref, recv)
        if onward:
            t_go(ref, ref, tr_sem.at[q], where)
        t_go(ref, ref, td_sem.at[slot + q], to_d)

    def norm_rows(begin, count):
        part = tokbuf[pl.ds(begin, count), :].astype(f32)
        scaling = lax.rsqrt(jnp.mean(part * part, axis=-1, keepdims=True) + EPSILON)
        normbuf[pl.ds(begin, count), :] = (part * scaling * gain[...]).astype(bf16)

    def norm_block(xx, cc):
        norm_rows(pl.multiple_of(HALO + (xx * 2 + cc) * TOK_ROWS, 16), TOK_ROWS)

    cs = 1 - c

    def token_step(k):
        if k <= 4:
            q = k - 1
            relay_tokens(xm, q, tp_sem.at[q], to_xp, q < 2, 0)
            q = (2, 3, 0, 1)[k - 1]
            relay_tokens(xp, q, tm_sem.at[q], to_xm, q >= 2, 4)
            if k == 2:
                norm_block(x, c)
            if k == 3:
                t_came(t_at(x, cs, 0, TOK_ROWS), td_sem.at[12])
                norm_block(x, cs)
        elif k <= 6:
            for q in (k - 5, k - 3):
                relay_tokens(xo, q, tr_sem.at[q], to_d, False, 8)
            norm_block(xm if k == 5 else xp, c)
        elif k == 7:
            for q in range(4):
                t_came(t_at(xm, cs, q), td_sem.at[q])
                t_came(t_at(xp, cs, q), td_sem.at[4 + q])
            norm_block(xm, cs)
            norm_block(xp, cs)
        else:
            norm_block(xo, c)

    for copy in locals_[:5]:
        copy.wait()
    w_rings.begin()
    locals_[5].wait()
    for q in (0, 1, 2, 3):
        t_go(t_at(x, c, q), t_at(x, c, q), tp_sem.at[q], to_xp)
    for q in (2, 3, 0, 1):
        t_go(t_at(x, c, q), t_at(x, c, q), tm_sem.at[q], to_xm)
    t_go(t_at(x, c, 0, TOK_ROWS), t_at(x, c, 0, TOK_ROWS), td_sem.at[12], to_d)
    w_rings.along_y(0)
    o_rings.begin()
    steps_z = n_sp // 2
    for k in range(1, steps_z + 1):
        w_rings.along_z(k)
        w_rings.along_y(k)
        w_rings.relay(k - 1)
        token_step(k)
        if k > 1:
            o_rings.along_z(k - 1)
        if k > 1:
            o_rings.along_y(k - 2)
    for q in range(4):
        t_came(t_at(xo, cs, q), td_sem.at[8 + q])
    before, after = tokbuf.at[pl.ds(0, HALO), :], tokbuf.at[pl.ds(HALO + rows, HALO), :]
    t_go(tokbuf.at[pl.ds(rows, HALO), :], before, h_sem.at[0], to_zp)
    t_go(tokbuf.at[pl.ds(HALO, HALO), :], after, h_sem.at[1], to_zm)
    w_rings.relay(steps_z)
    norm_block(xo, cs)
    o_rings.along_z(steps_z)
    w_rings.finish()
    for k in range(7, steps_z + 1):
        o_rings.along_y(k)

    def rounded(v):
        return v.astype(bf16).astype(f32)

    def dots(at, count, rhs):
        return jnp.dot(normbuf[at : at + count, :], rhs, preferred_element_type=f32)

    for i in range(4):
        at = HALO + i * 256
        found = dots(at, 256, wbuf[...])
        p32[at : at + 256, 0:256] = rounded(found[:, 0:256])
        raw[i * 256 : (i + 1) * 256, :] = found[:, 256:384]
    edges = ((0, z > 0), (HALO + rows, z < n_sp - 1))
    t_came(before, h_sem.at[0])
    t_came(after, h_sem.at[1])
    for begin, real in edges:
        norm_rows(begin, HALO)
        edge = dots(begin, HALO, wbuf[:, 0:256])
        p32[begin : begin + HALO, 0:256] = jnp.where(real, rounded(edge), 0.0)
    for k in range(3):
        o_rings.relay(k)

    row8 = lax.broadcasted_iota(jnp.int32, (8, 128), 0)

    def by_kind(parts):
        found = jnp.zeros((8, 128), f32)
        for i, part in enumerate(parts):
            found = jnp.where(row8 == i, part, found)
        return found

    kinds = ((0, 0), (0, 1), (1, 0), (1, 1))
    bias8 = by_kind([bias[r, 2 * t + h] for r, h in kinds])
    rate8 = by_kind([rate[r, 2 * t + h] for r, h in kinds])
    steps_l, logs_l = [], []
    for b in range(N_BLOCKS):
        cols = raw[b * SPAN : (b + 1) * SPAN, :].T[0:8, :] + bias8
        steps = jnp.maximum(cols, 0.0) + jnp.log1p(jnp.exp(-jnp.abs(cols)))
        moved = by_kind([shift[0, h, r : r + 1, b * SPAN : (b + 1) * SPAN] for r, h in kinds])
        steps_l.append(steps)
        logs_l.append(jnp.where(row8 < 4, -rate8 * steps - moved, 0.0))
    steps = jnp.concatenate(steps_l, axis=0)
    logs = jnp.concatenate(logs_l, axis=0)
    lane = lax.broadcasted_iota(jnp.int32, (64, 128), 1)
    kind = lax.broadcasted_iota(jnp.int32, (64, 128), 0) % 8
    prefix, suffix = logs, logs
    for k in (1, 2, 4, 8, 16, 32, 64):
        prefix = prefix + jnp.where(lane >= k, pltpu.roll(prefix, k, 1), 0.0)
        suffix = suffix + jnp.where(lane < 128 - k, pltpu.roll(suffix, 128 - k, 1), 0.0)
    cum = jnp.where(kind < 2, prefix, suffix)
    total = jnp.broadcast_to(jnp.sum(logs, axis=1, keepdims=True), (64, 128))
    tail = jnp.exp(jnp.minimum(total - cum, 0.0)) * steps
    decay = jnp.exp(total)
    cum_tail_t = jnp.concatenate([cum, tail], axis=0).T
    reach_t = jnp.concatenate([jnp.exp(cum), jnp.zeros((64, 128), f32)], axis=0).T

    def wide(cols, b, first):
        j = b * 8 + first
        left = jnp.broadcast_to(cols[:, j : j + 1], (128, 64))
        right = jnp.broadcast_to(cols[:, j + 1 : j + 2], (128, 64))
        return jnp.concatenate([left, right], axis=1)

    def tall(rows_, b, first):
        j = b * 8 + first
        top = jnp.broadcast_to(rows_[j : j + 1, :], (64, 128))
        bottom = jnp.broadcast_to(rows_[j + 1 : j + 2, :], (64, 128))
        return jnp.concatenate([top, bottom], axis=0)

    def window(b, j):
        begin = HALO - 8 + b * SPAN
        return p32[begin : begin + SPAN + 16, j * 128 : (j + 1) * 128]

    def conv(b, j, taps):
        v = window(b, j)
        weights = taps[...].astype(f32)
        total_ = v * weights[2:3, :]
        for i in (0, 1, 3, 4):
            total_ = total_ + pltpu.roll(v, (2 - i) % (SPAN + 16), 0) * weights[i : i + 1, :]
        return silu(total_[8 : 8 + SPAN, :])

    for b in range(N_BLOCKS):
        at = slice(b * SPAN, (b + 1) * SPAN)
        values = conv(b, 0, tap_v)
        keys = conv(b, 1, tap_k).astype(bf16)
        xbuf[at, :] = values
        kbuf[at, :] = keys
        both = jnp.concatenate(
            [values * wide(cum_tail_t, b, 64), values * wide(cum_tail_t, b, 66)], axis=1
        )
        ends[b] = lax.dot_general(both.astype(bf16), keys, TN, preferred_element_type=f32)

    forward = ends[0, 0:128, :]
    backward = ends[N_BLOCKS - 1, 128:256, :]
    for i in range(1, N_BLOCKS):
        b = N_BLOCKS - 1 - i
        forward = forward * tall(decay, i, 0) + ends[i, 0:128, :]
        backward = backward * tall(decay, b, 2) + ends[b, 128:256, :]
    sums = total[0:8, :]
    for b in range(1, N_BLOCKS):
        sums = sums + total[b * 8 : b * 8 + 8, :]
    incl[0] = forward
    incl[1] = backward
    excl[...] = jnp.zeros_like(excl)
    itot[...] = jnp.broadcast_to(sums[None], (4, 8, 128))
    etot[...] = jnp.zeros_like(etot)

    def message(way, h, i, where):
        return remote(
            msg_out.at[way, h, i], msg_in.at[way, h, i],
            msg_send.at[way, h, i], msg_recv.at[way, h, i], where,
        )

    def exchange(i, h):
        d = distances[i]
        for way in (0, 1):
            ok = z + d < n_sp if way == 0 else z >= d
            logs8 = itot[2 * way + h]
            high = logs8.astype(bf16)
            low = (logs8 - high.astype(f32)).astype(bf16)
            msg_out[way, h, i, 0:64, :] = incl[way, h * 64 : (h + 1) * 64, :].astype(bf16)
            msg_out[way, h, i, 64:MSG, :] = jnp.concatenate([high, low], axis=0)
            where = {"sp": (z + d) % n_sp if way == 0 else (z + n_sp - d) % n_sp}

            @pl.when(ok)
            def _():
                message(way, h, i, where).start()

    def combine(i, h):
        d = distances[i]
        for way in (0, 1):
            ok = z >= d if way == 0 else z + d < n_sp
            s, r, part = 2 * way + h, 2 * way + h, slice(h * 64, (h + 1) * 64)

            @pl.when(ok)
            def _():
                message(way, h, i, to_d).wait_recv()
                state = msg_in[way, h, i, 0:64, :].astype(f32)
                pair = msg_in[way, h, i, 64:MSG, :].astype(f32)
                logs8 = pair[0:8, :] + pair[8:16, :]
                incl[way, part, :] = incl[way, part, :] + jnp.exp(itot[s][r : r + 1, :]) * state
                itot[s] = itot[s] + logs8
                excl[way, part, :] = excl[way, part, :] + jnp.exp(etot[s][r : r + 1, :]) * state
                etot[s] = etot[s] + logs8

    row = lax.broadcasted_iota(jnp.int32, (128, 128), 0)
    col = lax.broadcasted_iota(jnp.int32, (128, 128), 1)

    def within(b):
        at = slice(b * SPAN, (b + 1) * SPAN)
        queries = conv(b, 2, tap_q).astype(bf16)
        qbuf[at, :] = queries
        scores = lax.dot_general(queries, kbuf[at, :], NT, preferred_element_type=f32)
        masked = []
        for h in (0, 1):
            jf, jb = b * 8 + h, b * 8 + 2 + h
            ahead = cum_tail_t[:, jf : jf + 1] - cum[jf : jf + 1, :]
            behind = cum_tail_t[:, jb : jb + 1] - cum[jb : jb + 1, :]
            gaps = jnp.where(col < row, ahead, jnp.where(col > row, behind, 0.0))
            df, db = steps[jf : jf + 1, :], steps[jb : jb + 1, :]
            sizes = jnp.where(col < row, df, jnp.where(col > row, db, df + db))
            masked.append((scores * jnp.exp(jnp.minimum(gaps, 0.0)) * sizes).astype(bf16))
        values = xbuf[at, :]
        stacked = jnp.concatenate(
            [jnp.where(col < 64, values, 0.0), jnp.where(col >= 64, values, 0.0)], axis=0
        ).astype(bf16)
        ybuf[at, :] = jnp.dot(
            jnp.concatenate(masked, axis=1), stacked, preferred_element_type=f32
        )

    def pool(b):
        at = slice(b * SPAN, (b + 1) * SPAN)
        n = SPAN + 16
        v = window(b, 3)
        w2 = v + pltpu.roll(v, 1, 0)
        w4 = pltpu.roll(w2, 1, 0) + pltpu.roll(w2, n - 1, 0)
        w8 = pltpu.roll(w4, 2, 0) + pltpu.roll(w4, n - 2, 0)
        w16 = pltpu.roll(w8, 4, 0) + pltpu.roll(w8, n - 4, 0)
        which = t % 4
        summed = jnp.where(
            which == 0, w2, jnp.where(which == 1, w4, jnp.where(which == 2, w8, w16))
        )[8 : 8 + SPAN, :]
        reach = jnp.where(which == 0, 1, jnp.where(which == 1, 2, jnp.where(which == 2, 4, 8)))
        place = z * rows + b * SPAN + row
        upper = jnp.minimum(place + reach, n_sp * rows)
        lower = jnp.maximum(place - reach, 0)
        differences = summed / (upper - lower).astype(f32) - v[8 : 8 + SPAN, :]
        mapped = jnp.dot(differences.astype(bf16), pmix[...], preferred_element_type=f32)
        mix[at, 128:256] = (mapped * pgain[...]).astype(bf16)

    def turn(i):
        for h in (0, 1):
            combine(i, h)
            if i + 1 < len(distances):
                exchange(i + 1, h)

    exchange(0, 0)
    exchange(0, 1)
    o_rings.relay(3)
    o_rings.relay(4)
    turn(0)
    o_rings.relay(5)
    o_rings.relay(6)
    turn(1)
    o_rings.relay(7)
    o_rings.relay(8)
    o_rings.finish()
    turn(2)
    for i in range(4):
        at = HALO + i * 256
        found = dots(at, 256, obuf[:, 0:384])
        gates[i * 256 : (i + 1) * 256, :] = found[:, 0:128].astype(bf16)
        p32[at : at + 256, 256:512] = rounded(found[:, 128:384])
    for begin, real in edges:
        edge = dots(begin, HALO, obuf[:, 128:384])
        p32[begin : begin + HALO, 256:512] = jnp.where(real, rounded(edge), 0.0)
    for b in range(N_BLOCKS):
        within(b)
    for b in range(N_BLOCKS):
        pool(b)
    turn(3)

    forward, backward = excl[0], excl[1]
    entering = [None] * N_BLOCKS
    leaving = [None] * N_BLOCKS
    for i in range(N_BLOCKS):
        b = N_BLOCKS - 1 - i
        entering[i] = forward.astype(bf16)
        leaving[b] = backward.astype(bf16)
        forward = forward * tall(decay, i, 0) + ends[i, 0:128, :]
        backward = backward * tall(decay, b, 2) + ends[b, 128:256, :]
    squares = jnp.zeros((128, 128), f32)
    for b in range(N_BLOCKS):
        at = slice(b * SPAN, (b + 1) * SPAN)
        states = jnp.concatenate([entering[b], leaving[b]], axis=0)
        carried = lax.dot_general(qbuf[at, :], states, NT, preferred_element_type=f32)
        heads_out = (
            ybuf[at, :]
            + carried[:, 0:128] * wide(reach_t, b, 0)
            + carried[:, 128:256] * wide(reach_t, b, 2)
        )
        gated = heads_out * silu(gates[at, :].astype(f32))
        ybuf[at, :] = gated
        summed = jnp.sum(gated * gated, axis=1, keepdims=True)
        squares = jnp.where(col == b, summed, squares)
    own_squares = squares.T[0:8, :]
    ss_out[...] = own_squares
    ss_copies = []
    for r in range(1, n_tp):
        copy = remote(
            ss_out, ss_in.at[r - 1], ss_send.at[r - 1], ss_recv.at[r - 1],
            {"tp": (t + r) % n_tp},
        )
        copy.start()
        ss_copies.append(copy)
    all_squares = own_squares
    for r in range(1, n_tp):
        ss_copies[r - 1].wait_recv()
        all_squares = all_squares + ss_in[r - 1]
    scale = lax.rsqrt(all_squares / D_SSM + EPSILON)
    scale_t = jnp.concatenate([scale, jnp.zeros((120, 128), f32)], axis=0).T
    mix_gain_here = mgain[...]
    for b in range(N_BLOCKS):
        at = slice(b * SPAN, (b + 1) * SPAN)
        mix[at, 0:128] = (ybuf[at, :] * scale_t[:, b : b + 1] * mix_gain_here).astype(bf16)

    def partial(xx, cc, begin=0, count=TOK_ROWS):
        at = pl.multiple_of((xx * 2 + cc) * TOK_ROWS + begin, 16)
        return lax.dot_general(
            mix[pl.ds(at, count), :], obuf[:, 384:640], NT, preferred_element_type=f32
        )

    half = TOK_ROWS // 2
    d_copies = []
    for i, xx in enumerate((xo, xp, xm, x)):
        d_out[i] = partial(xx, 1 - c).astype(bf16)
        copy = remote(d_out.at[i], d_in.at[i], d_send.at[i], d_recv.at[i], to_d)
        copy.start()
        d_copies.append(copy)

    def chip(i, xx, begin, count=half):
        return partial(xx, c, begin, count) + d_in[i, begin : begin + count, :].astype(f32)

    def send(i, value, where, out_ref, in_ref, send_sem, recv_sem):
        out_ref[i] = value.astype(bf16)
        copy = remote(out_ref.at[i], in_ref.at[i], send_sem.at[i], recv_sem.at[i], where)
        copy.start()
        return copy

    relay = (r_out, r_in, r_send, r_recv)
    near = (n_out, n_in, n_send, n_recv)
    d_copies[0].wait_recv()
    relay_p = send(0, chip(0, xo, 0), to_xp, *relay)
    relay_m = send(1, chip(0, xo, half), to_xm, *relay)
    d_copies[1].wait_recv()
    dir_p = send(0, chip(1, xp, half), to_xp, *near)
    d_copies[2].wait_recv()
    dir_m = send(1, chip(2, xm, 0), to_xm, *near)
    relay_p.wait_recv()
    comb_p = send(2, chip(1, xp, 0) + r_in[0].astype(f32), to_xp, *near)
    relay_m.wait_recv()
    comb_m = send(3, chip(2, xm, half) + r_in[1].astype(f32), to_xm, *near)
    d_copies[3].wait_recv()
    top, bottom = chip(3, x, 0), chip(3, x, half)
    dir_p.wait_recv()
    dir_m.wait_recv()
    bottom = bottom + n_in[0].astype(f32)
    top = top + n_in[1].astype(f32)
    comb_p.wait_recv()
    out[0, 0:half, :] = (top + n_in[2].astype(f32)).astype(bf16)
    comb_m.wait_recv()
    out[0, half:TOK_ROWS, :] = (bottom + n_in[3].astype(f32)).astype(bf16)

    for i, d in enumerate(distances):
        for way in (0, 1):
            ok = z + d < n_sp if way == 0 else z >= d

            @pl.when(ok)
            def _():
                for h in (0, 1):
                    message(way, h, i, to_d).wait_send()

    last = [relay_p, relay_m, dir_p, dir_m, comb_p, comb_m]
    for copy in t_sent + w_rings.sent + o_rings.sent + ss_copies + d_copies + last:
        copy.wait_send()


N_TOKEN_SENDS = 27
N_RING_SENDS = 66


def mixer(n_sp, n_fs, n_x, *operands):
    any_spec = pl.BlockSpec(memory_space=pl.ANY)
    vmem = pl.BlockSpec(memory_space=pltpu.VMEM)
    dma = pltpu.SemaphoreType.DMA
    f32, bf16 = jnp.float32, jnp.bfloat16
    rows = N_BLOCKS * SPAN
    half = TOK_ROWS // 2

    def ring_sems(counts):
        return [dma((n,)) for n in counts]

    return pl.pallas_call(
        functools.partial(mixer_kernel, n_sp, n_fs, n_x),
        out_shape=jax.ShapeDtypeStruct((1, TOK_ROWS, 2048), bf16),
        in_specs=[any_spec] * 19,
        out_specs=vmem,
        scratch_shapes=[
            pltpu.VMEM((2, 128, 32), bf16),
            pltpu.VMEM((2048, 4), bf16),
            pltpu.VMEM((1, 2048), f32),
            pltpu.SMEM((2, 16), f32),
            pltpu.SMEM((2, 16), f32),
            pltpu.VMEM((1, 2, 2, 1024), f32),
            pltpu.VMEM((5, 128), bf16),
            pltpu.VMEM((5, 128), bf16),
            pltpu.VMEM((5, 128), bf16),
            pltpu.VMEM((1, 128), f32),
            pltpu.VMEM((128, 128), bf16),
            pltpu.VMEM((1, 128), f32),
            dma((13,)),
            pltpu.VMEM((rows + 2 * HALO, 2048), bf16),
            pltpu.VMEM((rows + 2 * HALO, 2048), bf16),
            pltpu.VMEM((2048, 384), bf16),
            pltpu.VMEM((2048, 640), bf16),
            pltpu.VMEM((rows, 128), bf16),
            pltpu.VMEM((rows, 128), f32),
            pltpu.VMEM((rows + 2 * HALO, 512), f32),
            pltpu.VMEM((rows, 128), f32),
            pltpu.VMEM((rows, 128), bf16),
            pltpu.VMEM((rows, 128), bf16),
            pltpu.VMEM((N_BLOCKS, 256, 128), f32),
            pltpu.VMEM((rows, 128), f32),
            pltpu.VMEM((rows, 256), bf16),
            pltpu.VMEM((2, 128, 128), f32),
            pltpu.VMEM((2, 128, 128), f32),
            pltpu.VMEM((4, 8, 128), f32),
            pltpu.VMEM((4, 8, 128), f32),
            pltpu.VMEM((2, 2, 4, MSG, 128), bf16),
            pltpu.VMEM((2, 2, 4, MSG, 128), bf16),
            pltpu.VMEM((8, 128), f32),
            pltpu.VMEM((7, 8, 128), f32),
            pltpu.VMEM((4, TOK_ROWS, 2048), bf16),
            pltpu.VMEM((4, TOK_ROWS, 2048), bf16),
            pltpu.VMEM((2, half, 2048), bf16),
            pltpu.VMEM((2, half, 2048), bf16),
            pltpu.VMEM((4, half, 2048), bf16),
            pltpu.VMEM((4, half, 2048), bf16),
            dma((6,)), dma((4,)), dma((4,)), dma((4,)), dma((13,)), dma((2,)),
            dma((N_TOKEN_SENDS,)),
            *ring_sems((9, 9, 16, 16, 16, N_RING_SENDS)),
            *ring_sems((9, 9, 16, 16, 16, N_RING_SENDS)),
            dma((2, 2, 4)), dma((2, 2, 4)), dma((7,)), dma((7,)),
            dma((4,)), dma((4,)), dma((2,)), dma((2,)), dma((4,)), dma((4,)),
        ],
        compiler_params=pltpu.CompilerParams(
            collective_id=0, has_side_effects=True, vmem_limit_bytes=56 * 1024 * 1024
        ),
        name="mixer",
    )(*operands)


def local(
    tokens, norm_gain, w_gate, w_value, w_bkey, w_query, w_pool_in, w_step, step_bias,
    decay_rate, decay_shift, conv_value, conv_bkey, conv_query, mix_gain, pool_mix, pool_gain,
    w_out_ssd, w_out_pool,
):
    n_tp, n_sp, n_fs = lax.axis_size("tp"), lax.axis_size("sp"), lax.axis_size("fs")
    heads_dev = DUALITY_HEADS // n_tp
    step_cols = lax.dynamic_slice_in_dim(w_step, lax.axis_index("tp") * heads_dev, heads_dev, 2)
    step_cols = step_cols.reshape(w_step.shape[0], 2 * heads_dev)
    return mixer(
        n_sp, n_fs, n_tp // 2, tokens, w_gate, w_value, w_bkey, w_query, w_pool_in,
        w_out_ssd, w_out_pool, step_cols, norm_gain[None], step_bias, decay_rate, decay_shift,
        conv_value, conv_bkey, conv_query, mix_gain[None], pool_mix, pool_gain[None],
    )


def solution(mesh):
    return jax.shard_map(
        local,
        mesh=mesh,
        in_specs=(
            P("fs", ("sp", "tp"), None),
            P(),
            P(("sp", "fs"), "tp"),
            P(("sp", "fs"), "tp"),
            P(("sp", "fs"), "tp"),
            P(("sp", "fs"), "tp"),
            P(("sp", "fs"), "tp"),
            P(),
            P(),
            P(),
            P("fs", "tp", None, "sp"),
            P(),
            P(),
            P(),
            P(),
            P(),
            P(),
            P("tp", ("sp", "fs")),
            P("tp", ("sp", "fs")),
        ),
        out_specs=P("fs", ("sp", "tp"), None),
        check_vma=False,
    )
```

```python
import functools

import jax
import jax.numpy as jnp
from jax import lax
from jax.experimental import pallas as pl
from jax.experimental.pallas import tpu as pltpu
from jax.sharding import PartitionSpec as P

STATE = 128
SPAN = 128
D_SSM = 1024
EPSILON = 1e-06
HIGHEST = lax.Precision.HIGHEST

MESH = pl.DeviceIdType.MESH
HALO = 16
TOK_ROWS = 128
PIECE = 32
NT = (((1,), (1,)), ((), ()))
TN = (((0,), (0,)), ((), ()))
N_BLOCKS = 8
MSG = 64 + 16


def remote(src, dst, send, recv, where):
    return pltpu.make_async_remote_copy(
        src_ref=src, dst_ref=dst, send_sem=send, recv_sem=recv, device_id=where, device_id_type=MESH
    )


def silu(v):
    return v / (1.0 + jnp.exp(-v))


class Rings:

    def __init__(self, buf, cols, stride, sems, send_sem, place, sizes):
        self.buf, self.cols, self.stride = buf, cols, stride
        self.zp_sem, self.zm_sem, self.yp_sem, self.ym_sem, self.yo_sem = sems
        self.send_sem, self.sent = send_sem, []
        self.z, self.y = place
        self.n_sp, self.n_fs = sizes
        z, y, n_sp, n_fs = self.z, self.y, *sizes
        self.yp, self.ym, self.yo = (y + 1) % n_fs, (y + n_fs - 1) % n_fs, (y + 2) % n_fs
        self.to_yp, self.to_ym = {"fs": self.yp}, {"fs": self.ym}
        self.half = n_sp // 2

    def at(self, o, yy):
        zz = (self.z + self.n_sp - o) % self.n_sp
        row = pl.multiple_of((zz * self.n_fs + yy) * PIECE, PIECE)
        return self.buf.at[pl.ds(row, PIECE), pl.ds(*self.cols)]

    def send(self, ref, recv, where):
        copy = remote(ref, ref, self.send_sem.at[len(self.sent)], recv, where)
        copy.start()
        self.sent.append(copy)

    def arrived(self, ref, recv):
        remote(ref, ref, self.send_sem.at[0], recv, self.to_yp).wait_recv()

    def up(self, ref, k, stride):
        if k <= self.half:
            self.send(ref, self.zp_sem.at[k], {"sp": (self.z + stride) % self.n_sp})

    def down(self, ref, k, stride):
        if k < self.half:
            self.send(ref, self.zm_sem.at[k], {"sp": (self.z + self.n_sp - stride) % self.n_sp})

    def begin(self):
        own = self.at(0, self.y)
        for k in range(self.stride, 0, -1):
            self.up(own, k, k)
            self.down(own, k, k)

    def places(self, k):
        if k == 0:
            return (0,)
        return (k, self.n_sp - k) if k < self.half else (k,)

    def along_z(self, k):
        ref = self.at(k, self.y)
        self.arrived(ref, self.zp_sem.at[k])
        self.up(ref, k + self.stride, self.stride)
        if k < self.half:
            ref = self.at(self.n_sp - k, self.y)
            self.arrived(ref, self.zm_sem.at[k])
            self.down(ref, k + self.stride, self.stride)

    def along_y(self, k):
        for o in self.places(k):
            ref = self.at(o, self.y)
            self.send(ref, self.yp_sem.at[o], self.to_yp)
            self.send(ref, self.ym_sem.at[o], self.to_ym)

    def relay(self, k):
        for o in self.places(k):
            low, high = self.at(o, self.ym), self.at(o, self.yp)
            self.arrived(low, self.yp_sem.at[o])
            if o % 2 == 0:
                self.send(low, self.yo_sem.at[o], self.to_yp)
            self.arrived(high, self.ym_sem.at[o])
            if o % 2 == 1:
                self.send(high, self.yo_sem.at[o], self.to_ym)

    def finish(self):
        for o in range(self.n_sp):
            self.arrived(self.at(o, self.yo), self.yo_sem.at[o])


def mixer_kernel(
    n_sp, n_fs, n_x,
    tok, wg, wv, wk, wq, wp, wo_s, wo_p, wstep_in, gain_in,
    bias_in, rate_in, shift_in, tap_v_in, tap_k_in, tap_q_in, mgain_in, pmix_in, pgain_in,
    out,
    wstep, raw_t, gain, bias, rate, shift, tap_v, tap_k, tap_q, mgain, pmix, pgain, small_sem,
    tokbuf, normbuf, wbuf, obuf, gates, raw,
    p32, xbuf, kbuf, qbuf, ends, ybuf, mix,
    incl, excl, itot, etot, msg_out, msg_in, ss_out, ss_in, part_s, part_p, scales,
    d_out, d_in, r_out, r_in, n_out, n_in,
    local_sem, tp_sem, tm_sem, tr_sem, td_sem, h_sem, t_send,
    w_zp, w_zm, w_yp, w_ym, w_yo, w_send,
    o_zp, o_zm, o_yp, o_ym, o_yo, o_send,
    msg_send, msg_recv, ss_send, ss_recv, d_send, d_recv, r_send, r_recv, n_send, n_recv,
):
    f32, bf16 = jnp.float32, jnp.bfloat16
    z, y, t = lax.axis_index("sp"), lax.axis_index("fs"), lax.axis_index("tp")
    x, c = t // 2, t % 2
    n_tp = 2 * n_x
    xp, xm, xo = (x + 1) % n_x, (x + n_x - 1) % n_x, (x + 2) % n_x
    to_xp, to_xm, to_d = {"tp": xp * 2 + c}, {"tp": xm * 2 + c}, {"tp": x * 2 + 1 - c}
    to_zp, to_zm = {"sp": (z + 1) % n_sp}, {"sp": (z + n_sp - 1) % n_sp}
    distances = [1, 2, 4, 8]
    rows = N_BLOCKS * SPAN

    w_rings = Rings(
        wbuf, (0, 256), 2, (w_zp, w_zm, w_yp, w_ym, w_yo), w_send, (z, y), (n_sp, n_fs)
    )
    o_rings = Rings(
        obuf, (0, 640), 2, (o_zp, o_zm, o_yp, o_ym, o_yo), o_send, (z, y), (n_sp, n_fs)
    )

    def t_at(xx, cc, q=0, count=PIECE):
        row = pl.multiple_of(HALO + (xx * 2 + cc) * TOK_ROWS + q * PIECE, 16)
        return tokbuf.at[pl.ds(row, count), :]

    own_row = pl.ds(pl.multiple_of((z * n_fs + y) * PIECE, PIECE), PIECE)
    shards = (
        (wv, wbuf, 0), (wk, wbuf, 1), (wg, obuf, 0), (wq, obuf, 1), (wp, obuf, 2),
        (wo_s, obuf, 3), (wo_p, obuf, 4),
    )
    locals_ = [
        pltpu.make_async_copy(w, buf.at[own_row, pl.ds(i * 128, 128)], local_sem.at[n])
        for n, (w, buf, i) in enumerate(shards)
    ]
    locals_.append(pltpu.make_async_copy(tok.at[0], t_at(x, c, 0, TOK_ROWS), local_sem.at[7]))
    lane0 = pl.multiple_of(t * 128, 128)
    here = pl.ds(lane0, 128)
    small = [
        pltpu.make_async_copy(src, dst, small_sem.at[i])
        for i, (src, dst) in enumerate(
            (
                (gain_in, gain), (wstep_in, wstep),
                (bias_in, bias), (rate_in, rate), (shift_in, shift),
                (tap_v_in.at[:, here], tap_v), (tap_k_in.at[:, here], tap_k),
                (tap_q_in.at[:, here], tap_q), (mgain_in.at[:, here], mgain),
                (pmix_in.at[t], pmix), (pgain_in.at[:, here], pgain),
            )
        )
    ]
    for copy in locals_ + small:
        copy.start()

    barrier = pltpu.get_barrier_semaphore()
    partners = [
        to_xp, to_xm, to_d, to_zp, to_zm, {"sp": (z + 2) % n_sp}, {"sp": (z + n_sp - 2) % n_sp},
        w_rings.to_yp, w_rings.to_ym,
    ]
    for where in partners:
        pl.semaphore_signal(barrier, inc=1, device_id=where, device_id_type=MESH)
    for copy in small:
        copy.wait()
    pl.semaphore_wait(barrier, len(partners))

    t_sent = []

    def t_go(src, dst, recv, where):
        copy = remote(src, dst, t_send.at[len(t_sent)], recv, where)
        copy.start()
        t_sent.append(copy)

    def t_came(ref, recv):
        remote(ref, ref, t_send.at[0], recv, to_d).wait_recv()

    def relay_tokens(xx, q, recv, where, onward, slot):
        ref = t_at(xx, c, q)
        t_came(ref, recv)
        if onward:
            t_go(ref, ref, tr_sem.at[q], where)
        t_go(ref, ref, td_sem.at[slot + q], to_d)

    def norm_rows(begin, count):
        part = tokbuf[pl.ds(begin, count), :].astype(f32)
        scaling = lax.rsqrt(jnp.mean(part * part, axis=-1, keepdims=True) + EPSILON)
        normbuf[pl.ds(begin, count), :] = (part * scaling * gain[...]).astype(bf16)

    def norm_block(xx, cc):
        norm_rows(pl.multiple_of(HALO + (xx * 2 + cc) * TOK_ROWS, 16), TOK_ROWS)

    cs = 1 - c

    def token_step(k):
        if k <= 4:
            q = k - 1
            relay_tokens(xm, q, tp_sem.at[q], to_xp, q < 2, 0)
            q = (2, 3, 0, 1)[k - 1]
            relay_tokens(xp, q, tm_sem.at[q], to_xm, q >= 2, 4)
            if k == 2:
                norm_block(x, c)
            if k == 3:
                t_came(t_at(x, cs, 0, TOK_ROWS), td_sem.at[12])
                norm_block(x, cs)
        elif k <= 6:
            for q in (k - 5, k - 3):
                relay_tokens(xo, q, tr_sem.at[q], to_d, False, 8)
            norm_block(xm if k == 5 else xp, c)
        elif k == 7:
            for q in range(4):
                t_came(t_at(xm, cs, q), td_sem.at[q])
                t_came(t_at(xp, cs, q), td_sem.at[4 + q])
            norm_block(xm, cs)
            norm_block(xp, cs)
        else:
            norm_block(xo, c)

    for copy in locals_[:7]:
        copy.wait()
    w_rings.begin()
    locals_[7].wait()
    for q in (0, 1, 2, 3):
        t_go(t_at(x, c, q), t_at(x, c, q), tp_sem.at[q], to_xp)
    for q in (2, 3, 0, 1):
        t_go(t_at(x, c, q), t_at(x, c, q), tm_sem.at[q], to_xm)
    t_go(t_at(x, c, 0, TOK_ROWS), t_at(x, c, 0, TOK_ROWS), td_sem.at[12], to_d)
    w_rings.along_y(0)
    o_rings.begin()
    for i in range(16):
        cols = [wstep[r, :, i * 128 : (i + 1) * 128].astype(f32) for r in (0, 1)]
        tall_cols = jnp.concatenate([*cols, jnp.zeros((96, 128), f32)], axis=0).T
        wbuf[i * 128 : (i + 1) * 128, 256:384] = tall_cols.astype(bf16)
    steps_z = n_sp // 2
    for k in range(1, steps_z + 1):
        w_rings.along_z(k)
        w_rings.along_y(k)
        w_rings.relay(k - 1)
        token_step(k)
        if k > 1:
            o_rings.along_z(k - 1)
        if k > 1:
            o_rings.along_y(k - 2)
    for q in range(4):
        t_came(t_at(xo, cs, q), td_sem.at[8 + q])
    before, after = tokbuf.at[pl.ds(0, HALO), :], tokbuf.at[pl.ds(HALO + rows, HALO), :]
    t_go(tokbuf.at[pl.ds(rows, HALO), :], before, h_sem.at[0], to_zp)
    t_go(tokbuf.at[pl.ds(HALO, HALO), :], after, h_sem.at[1], to_zm)
    w_rings.relay(steps_z)
    norm_block(xo, cs)
    o_rings.along_z(steps_z)
    w_rings.finish()
    for k in range(7, steps_z + 1):
        o_rings.along_y(k)

    def rounded(v):
        return v.astype(bf16).astype(f32)

    def dots(at, count, rhs):
        return jnp.dot(normbuf[at : at + count, :], rhs, preferred_element_type=f32)

    for i in range(4):
        at = HALO + i * 256
        found = dots(at, 256, wbuf[...])
        p32[at : at + 256, 0:256] = rounded(found[:, 0:256])
        raw[i * 256 : (i + 1) * 256, :] = found[:, 256:384]
    edges = ((0, z > 0), (HALO + rows, z < n_sp - 1))
    t_came(before, h_sem.at[0])
    t_came(after, h_sem.at[1])
    for begin, real in edges:
        norm_rows(begin, HALO)
        edge = dots(begin, HALO, wbuf[:, 0:256])
        p32[begin : begin + HALO, 0:256] = jnp.where(real, rounded(edge), 0.0)
    for k in range(3):
        o_rings.relay(k)

    row8 = lax.broadcasted_iota(jnp.int32, (8, 128), 0)

    def by_kind(parts):
        found = jnp.zeros((8, 128), f32)
        for i, part in enumerate(parts):
            found = jnp.where(row8 == i, part, found)
        return found

    kinds = ((0, 0), (0, 1), (1, 0), (1, 1))
    bias8 = by_kind([bias[r, 2 * t + h] for r, h in kinds])
    rate8 = by_kind([rate[r, 2 * t + h] for r, h in kinds])
    steps_l, logs_l = [], []
    for b in range(N_BLOCKS):
        raw_t[b] = raw[b * SPAN : (b + 1) * SPAN, :].T[0:32, :]
        cols = by_kind([raw_t[b, pl.ds(r * 16 + 2 * t + h, 1), :] for r, h in kinds]) + bias8
        steps = jnp.maximum(cols, 0.0) + jnp.log1p(jnp.exp(-jnp.abs(cols)))
        moved = by_kind([shift[0, h, r : r + 1, b * SPAN : (b + 1) * SPAN] for r, h in kinds])
        steps_l.append(steps)
        logs_l.append(jnp.where(row8 < 4, -rate8 * steps - moved, 0.0))
    steps = jnp.concatenate(steps_l, axis=0)
    logs = jnp.concatenate(logs_l, axis=0)
    lane = lax.broadcasted_iota(jnp.int32, (64, 128), 1)
    kind = lax.broadcasted_iota(jnp.int32, (64, 128), 0) % 8
    prefix, suffix = logs, logs
    for k in (1, 2, 4, 8, 16, 32, 64):
        prefix = prefix + jnp.where(lane >= k, pltpu.roll(prefix, k, 1), 0.0)
        suffix = suffix + jnp.where(lane < 128 - k, pltpu.roll(suffix, 128 - k, 1), 0.0)
    cum = jnp.where(kind < 2, prefix, suffix)
    total = jnp.broadcast_to(jnp.sum(logs, axis=1, keepdims=True), (64, 128))
    tail = jnp.exp(jnp.minimum(total - cum, 0.0)) * steps
    decay = jnp.exp(total)
    cum_tail_t = jnp.concatenate([cum, tail], axis=0).T
    reach_t = jnp.concatenate([jnp.exp(cum), jnp.zeros((64, 128), f32)], axis=0).T

    def wide(cols, b, first):
        j = b * 8 + first
        left = jnp.broadcast_to(cols[:, j : j + 1], (128, 64))
        right = jnp.broadcast_to(cols[:, j + 1 : j + 2], (128, 64))
        return jnp.concatenate([left, right], axis=1)

    def tall(rows_, b, first):
        j = b * 8 + first
        top = jnp.broadcast_to(rows_[j : j + 1, :], (64, 128))
        bottom = jnp.broadcast_to(rows_[j + 1 : j + 2, :], (64, 128))
        return jnp.concatenate([top, bottom], axis=0)

    def window(b, j):
        begin = HALO - 8 + b * SPAN
        return p32[begin : begin + SPAN + 16, j * 128 : (j + 1) * 128]

    def conv(b, j, taps):
        v = window(b, j)
        weights = taps[...].astype(f32)
        total_ = v * weights[2:3, :]
        for i in (0, 1, 3, 4):
            total_ = total_ + pltpu.roll(v, (2 - i) % (SPAN + 16), 0) * weights[i : i + 1, :]
        return silu(total_[8 : 8 + SPAN, :])

    for b in range(N_BLOCKS):
        at = slice(b * SPAN, (b + 1) * SPAN)
        values = conv(b, 0, tap_v)
        keys = conv(b, 1, tap_k).astype(bf16)
        xbuf[at, :] = values
        kbuf[at, :] = keys
        both = jnp.concatenate(
            [values * wide(cum_tail_t, b, 64), values * wide(cum_tail_t, b, 66)], axis=1
        )
        ends[b] = lax.dot_general(both.astype(bf16), keys, TN, preferred_element_type=f32)

    forward = ends[0, 0:128, :]
    backward = ends[N_BLOCKS - 1, 128:256, :]
    for i in range(1, N_BLOCKS):
        b = N_BLOCKS - 1 - i
        forward = forward * tall(decay, i, 0) + ends[i, 0:128, :]
        backward = backward * tall(decay, b, 2) + ends[b, 128:256, :]
    sums = total[0:8, :]
    for b in range(1, N_BLOCKS):
        sums = sums + total[b * 8 : b * 8 + 8, :]
    incl[0] = forward
    incl[1] = backward
    excl[...] = jnp.zeros_like(excl)
    itot[...] = jnp.broadcast_to(sums[None], (4, 8, 128))
    etot[...] = jnp.zeros_like(etot)

    def message(way, h, i, where):
        return remote(
            msg_out.at[way, h, i], msg_in.at[way, h, i],
            msg_send.at[way, h, i], msg_recv.at[way, h, i], where,
        )

    def exchange(i, h):
        d = distances[i]
        for way in (0, 1):
            ok = z + d < n_sp if way == 0 else z >= d
            logs8 = itot[2 * way + h]
            high = logs8.astype(bf16)
            low = (logs8 - high.astype(f32)).astype(bf16)
            msg_out[way, h, i, 0:64, :] = incl[way, h * 64 : (h + 1) * 64, :].astype(bf16)
            msg_out[way, h, i, 64:MSG, :] = jnp.concatenate([high, low], axis=0)
            where = {"sp": (z + d) % n_sp if way == 0 else (z + n_sp - d) % n_sp}

            @pl.when(ok)
            def _():
                message(way, h, i, where).start()

    def combine(i, h):
        d = distances[i]
        for way in (0, 1):
            ok = z >= d if way == 0 else z + d < n_sp
            s, r, part = 2 * way + h, 2 * way + h, slice(h * 64, (h + 1) * 64)

            @pl.when(ok)
            def _():
                message(way, h, i, to_d).wait_recv()
                state = msg_in[way, h, i, 0:64, :].astype(f32)
                pair = msg_in[way, h, i, 64:MSG, :].astype(f32)
                logs8 = pair[0:8, :] + pair[8:16, :]
                incl[way, part, :] = incl[way, part, :] + jnp.exp(itot[s][r : r + 1, :]) * state
                itot[s] = itot[s] + logs8
                excl[way, part, :] = excl[way, part, :] + jnp.exp(etot[s][r : r + 1, :]) * state
                etot[s] = etot[s] + logs8

    row = lax.broadcasted_iota(jnp.int32, (128, 128), 0)
    col = lax.broadcasted_iota(jnp.int32, (128, 128), 1)

    def within(b):
        at = slice(b * SPAN, (b + 1) * SPAN)
        queries = conv(b, 2, tap_q).astype(bf16)
        qbuf[at, :] = queries
        scores = lax.dot_general(queries, kbuf[at, :], NT, preferred_element_type=f32)
        masked = []
        for h in (0, 1):
            jf, jb = b * 8 + h, b * 8 + 2 + h
            ahead = cum_tail_t[:, jf : jf + 1] - cum[jf : jf + 1, :]
            behind = cum_tail_t[:, jb : jb + 1] - cum[jb : jb + 1, :]
            gaps = jnp.where(col < row, ahead, jnp.where(col > row, behind, 0.0))
            df, db = steps[jf : jf + 1, :], steps[jb : jb + 1, :]
            sizes = jnp.where(col < row, df, jnp.where(col > row, db, df + db))
            masked.append((scores * jnp.exp(jnp.minimum(gaps, 0.0)) * sizes).astype(bf16))
        values = xbuf[at, :]
        stacked = jnp.concatenate(
            [jnp.where(col < 64, values, 0.0), jnp.where(col >= 64, values, 0.0)], axis=0
        ).astype(bf16)
        ybuf[at, :] = jnp.dot(
            jnp.concatenate(masked, axis=1), stacked, preferred_element_type=f32
        )

    def pool(b):
        at = slice(b * SPAN, (b + 1) * SPAN)
        n = SPAN + 16
        v = window(b, 3)
        w2 = v + pltpu.roll(v, 1, 0)
        w4 = pltpu.roll(w2, 1, 0) + pltpu.roll(w2, n - 1, 0)
        w8 = pltpu.roll(w4, 2, 0) + pltpu.roll(w4, n - 2, 0)
        w16 = pltpu.roll(w8, 4, 0) + pltpu.roll(w8, n - 4, 0)
        which = t % 4
        summed = jnp.where(
            which == 0, w2, jnp.where(which == 1, w4, jnp.where(which == 2, w8, w16))
        )[8 : 8 + SPAN, :]
        reach = jnp.where(which == 0, 1, jnp.where(which == 1, 2, jnp.where(which == 2, 4, 8)))
        place = z * rows + b * SPAN + row
        upper = jnp.minimum(place + reach, n_sp * rows)
        lower = jnp.maximum(place - reach, 0)
        differences = summed / (upper - lower).astype(f32) - v[8 : 8 + SPAN, :]
        mapped = jnp.dot(differences.astype(bf16), pmix[...], preferred_element_type=f32)
        mix[at, 128:256] = (mapped * pgain[...]).astype(bf16)

    def turn(i):
        for h in (0, 1):
            combine(i, h)
            if i + 1 < len(distances):
                exchange(i + 1, h)

    exchange(0, 0)
    exchange(0, 1)
    o_rings.relay(3)
    o_rings.relay(4)
    turn(0)
    o_rings.relay(5)
    o_rings.relay(6)
    turn(1)
    o_rings.relay(7)
    o_rings.relay(8)
    o_rings.finish()
    turn(2)
    for i in range(4):
        at = HALO + i * 256
        found = dots(at, 256, obuf[:, 0:384])
        gates[i * 256 : (i + 1) * 256, :] = found[:, 0:128].astype(bf16)
        p32[at : at + 256, 256:512] = rounded(found[:, 128:384])
    for begin, real in edges:
        edge = dots(begin, HALO, obuf[:, 128:384])
        p32[begin : begin + HALO, 256:512] = jnp.where(real, rounded(edge), 0.0)
    for b in range(N_BLOCKS):
        within(b)
    for b in range(N_BLOCKS):
        pool(b)
    order = (xo, xp, xm, x)
    for i, xx in enumerate(order):
        pair = pl.ds(pl.multiple_of(xx * 2 * TOK_ROWS, 2 * TOK_ROWS), 2 * TOK_ROWS)
        part_p[i] = lax.dot_general(
            mix[pair, 128:256], obuf[:, 512:640], NT, preferred_element_type=f32
        )
    turn(3)

    forward, backward = excl[0], excl[1]
    entering = [None] * N_BLOCKS
    leaving = [None] * N_BLOCKS
    for i in range(N_BLOCKS):
        b = N_BLOCKS - 1 - i
        entering[i] = forward.astype(bf16)
        leaving[b] = backward.astype(bf16)
        forward = forward * tall(decay, i, 0) + ends[i, 0:128, :]
        backward = backward * tall(decay, b, 2) + ends[b, 128:256, :]
    squares = jnp.zeros((128, 128), f32)
    for b in range(N_BLOCKS):
        at = slice(b * SPAN, (b + 1) * SPAN)
        states = jnp.concatenate([entering[b], leaving[b]], axis=0)
        carried = lax.dot_general(qbuf[at, :], states, NT, preferred_element_type=f32)
        heads_out = (
            ybuf[at, :]
            + carried[:, 0:128] * wide(reach_t, b, 0)
            + carried[:, 128:256] * wide(reach_t, b, 2)
        )
        gated = heads_out * silu(gates[at, :].astype(f32))
        mix[at, 0:128] = (gated * mgain[...]).astype(bf16)
        summed = jnp.sum(gated * gated, axis=1, keepdims=True)
        squares = jnp.where(col == b, summed, squares)
    own_squares = squares.T[0:8, :]
    ss_out[...] = own_squares
    ss_copies = []
    for r in range(1, n_tp):
        copy = remote(
            ss_out, ss_in.at[r - 1], ss_send.at[r - 1], ss_recv.at[r - 1],
            {"tp": (t + r) % n_tp},
        )
        copy.start()
        ss_copies.append(copy)
    for i, xx in enumerate(order):
        pair = pl.ds(pl.multiple_of(xx * 2 * TOK_ROWS, 2 * TOK_ROWS), 2 * TOK_ROWS)
        part_s[i] = lax.dot_general(
            mix[pair, 0:128], obuf[:, 384:512], NT, preferred_element_type=f32
        )
    all_squares = own_squares
    for r in range(1, n_tp):
        ss_copies[r - 1].wait_recv()
        all_squares = all_squares + ss_in[r - 1]
    scale = lax.rsqrt(all_squares / D_SSM + EPSILON)
    scale_t = jnp.concatenate([scale, jnp.zeros((120, 128), f32)], axis=0).T
    for b in range(N_BLOCKS):
        scales[b * SPAN : (b + 1) * SPAN, :] = jnp.broadcast_to(scale_t[:, b : b + 1], (128, 128))

    def partial(i, cc, begin=0, count=TOK_ROWS):
        at = pl.multiple_of(cc * TOK_ROWS + begin, 16)
        there = pl.multiple_of(order[i] * 2 * TOK_ROWS + at, 16)
        scaling = scales[pl.ds(there, count), :][:, 0:1]
        return part_s[i, pl.ds(at, count), :] * scaling + part_p[i, pl.ds(at, count), :]

    half = TOK_ROWS // 2
    d_copies = []
    for i in range(4):
        d_out[i] = partial(i, 1 - c).astype(bf16)
        copy = remote(d_out.at[i], d_in.at[i], d_send.at[i], d_recv.at[i], to_d)
        copy.start()
        d_copies.append(copy)

    def chip(i, begin, count=half):
        return partial(i, c, begin, count) + d_in[i, begin : begin + count, :].astype(f32)

    def send(i, value, where, out_ref, in_ref, send_sem, recv_sem):
        out_ref[i] = value.astype(bf16)
        copy = remote(out_ref.at[i], in_ref.at[i], send_sem.at[i], recv_sem.at[i], where)
        copy.start()
        return copy

    relay = (r_out, r_in, r_send, r_recv)
    near = (n_out, n_in, n_send, n_recv)
    d_copies[0].wait_recv()
    relay_p = send(0, chip(0, 0), to_xp, *relay)
    relay_m = send(1, chip(0, half), to_xm, *relay)
    d_copies[1].wait_recv()
    dir_p = send(0, chip(1, half), to_xp, *near)
    d_copies[2].wait_recv()
    dir_m = send(1, chip(2, 0), to_xm, *near)
    relay_p.wait_recv()
    comb_p = send(2, chip(1, 0) + r_in[0].astype(f32), to_xp, *near)
    relay_m.wait_recv()
    comb_m = send(3, chip(2, half) + r_in[1].astype(f32), to_xm, *near)
    d_copies[3].wait_recv()
    top, bottom = chip(3, 0), chip(3, half)
    dir_p.wait_recv()
    dir_m.wait_recv()
    bottom = bottom + n_in[0].astype(f32)
    top = top + n_in[1].astype(f32)
    comb_p.wait_recv()
    out[0, 0:half, :] = (top + n_in[2].astype(f32)).astype(bf16)
    comb_m.wait_recv()
    out[0, half:TOK_ROWS, :] = (bottom + n_in[3].astype(f32)).astype(bf16)

    for i, d in enumerate(distances):
        for way in (0, 1):
            ok = z + d < n_sp if way == 0 else z >= d

            @pl.when(ok)
            def _():
                for h in (0, 1):
                    message(way, h, i, to_d).wait_send()

    last = [relay_p, relay_m, dir_p, dir_m, comb_p, comb_m]
    for copy in t_sent + w_rings.sent + o_rings.sent + ss_copies + d_copies + last:
        copy.wait_send()


N_TOKEN_SENDS = 27
N_RING_SENDS = 66


def mixer(n_sp, n_fs, n_x, *operands):
    any_spec = pl.BlockSpec(memory_space=pl.ANY)
    vmem = pl.BlockSpec(memory_space=pltpu.VMEM)
    dma = pltpu.SemaphoreType.DMA
    f32, bf16 = jnp.float32, jnp.bfloat16
    rows = N_BLOCKS * SPAN
    half = TOK_ROWS // 2

    def ring_sems(counts):
        return [dma((n,)) for n in counts]

    return pl.pallas_call(
        functools.partial(mixer_kernel, n_sp, n_fs, n_x),
        out_shape=jax.ShapeDtypeStruct((1, TOK_ROWS, 2048), bf16),
        in_specs=[any_spec] * 19,
        out_specs=vmem,
        scratch_shapes=[
            pltpu.VMEM((2, 16, 2048), bf16),
            pltpu.VMEM((N_BLOCKS, 32, 128), f32),
            pltpu.VMEM((1, 2048), f32),
            pltpu.SMEM((2, 16), f32),
            pltpu.SMEM((2, 16), f32),
            pltpu.VMEM((1, 2, 2, 1024), f32),
            pltpu.VMEM((5, 128), bf16),
            pltpu.VMEM((5, 128), bf16),
            pltpu.VMEM((5, 128), bf16),
            pltpu.VMEM((1, 128), f32),
            pltpu.VMEM((128, 128), bf16),
            pltpu.VMEM((1, 128), f32),
            dma((11,)),
            pltpu.VMEM((rows + 2 * HALO, 2048), bf16),
            pltpu.VMEM((rows + 2 * HALO, 2048), bf16),
            pltpu.VMEM((2048, 384), bf16),
            pltpu.VMEM((2048, 640), bf16),
            pltpu.VMEM((rows, 128), bf16),
            pltpu.VMEM((rows, 128), f32),
            pltpu.VMEM((rows + 2 * HALO, 512), f32),
            pltpu.VMEM((rows, 128), f32),
            pltpu.VMEM((rows, 128), bf16),
            pltpu.VMEM((rows, 128), bf16),
            pltpu.VMEM((N_BLOCKS, 256, 128), f32),
            pltpu.VMEM((rows, 128), f32),
            pltpu.VMEM((rows, 256), bf16),
            pltpu.VMEM((2, 128, 128), f32),
            pltpu.VMEM((2, 128, 128), f32),
            pltpu.VMEM((4, 8, 128), f32),
            pltpu.VMEM((4, 8, 128), f32),
            pltpu.VMEM((2, 2, 4, MSG, 128), bf16),
            pltpu.VMEM((2, 2, 4, MSG, 128), bf16),
            pltpu.VMEM((8, 128), f32),
            pltpu.VMEM((7, 8, 128), f32),
            pltpu.VMEM((4, 2 * TOK_ROWS, 2048), f32),
            pltpu.VMEM((4, 2 * TOK_ROWS, 2048), f32),
            pltpu.VMEM((rows, 128), f32),
            pltpu.VMEM((4, TOK_ROWS, 2048), bf16),
            pltpu.VMEM((4, TOK_ROWS, 2048), bf16),
            pltpu.VMEM((2, half, 2048), bf16),
            pltpu.VMEM((2, half, 2048), bf16),
            pltpu.VMEM((4, half, 2048), bf16),
            pltpu.VMEM((4, half, 2048), bf16),
            dma((8,)), dma((4,)), dma((4,)), dma((4,)), dma((13,)), dma((2,)),
            dma((N_TOKEN_SENDS,)),
            *ring_sems((9, 9, 16, 16, 16, N_RING_SENDS)),
            *ring_sems((9, 9, 16, 16, 16, N_RING_SENDS)),
            dma((2, 2, 4)), dma((2, 2, 4)), dma((7,)), dma((7,)),
            dma((4,)), dma((4,)), dma((2,)), dma((2,)), dma((4,)), dma((4,)),
        ],
        compiler_params=pltpu.CompilerParams(
            collective_id=0, has_side_effects=True, vmem_limit_bytes=56 * 1024 * 1024
        ),
        name="mixer",
    )(*operands)


def local(
    tokens, norm_gain, w_gate, w_value, w_bkey, w_query, w_pool_in, w_step, step_bias,
    decay_rate, decay_shift, conv_value, conv_bkey, conv_query, mix_gain, pool_mix, pool_gain,
    w_out_ssd, w_out_pool,
):
    n_tp, n_sp, n_fs = lax.axis_size("tp"), lax.axis_size("sp"), lax.axis_size("fs")
    return mixer(
        n_sp, n_fs, n_tp // 2, tokens, w_gate, w_value, w_bkey, w_query, w_pool_in,
        w_out_ssd.T, w_out_pool.T, w_step.transpose(1, 2, 0), norm_gain[None], step_bias, decay_rate, decay_shift,
        conv_value, conv_bkey, conv_query, mix_gain[None], pool_mix, pool_gain[None],
    )


def solution(mesh):
    return jax.shard_map(
        local,
        mesh=mesh,
        in_specs=(
            P("fs", ("sp", "tp"), None),
            P(),
            P(("sp", "fs"), "tp"),
            P(("sp", "fs"), "tp"),
            P(("sp", "fs"), "tp"),
            P(("sp", "fs"), "tp"),
            P(("sp", "fs"), "tp"),
            P(),
            P(),
            P(),
            P("fs", "tp", None, "sp"),
            P(),
            P(),
            P(),
            P(),
            P(),
            P(),
            P("tp", ("sp", "fs")),
            P("tp", ("sp", "fs")),
        ),
        out_specs=P("fs", ("sp", "tp"), None),
        check_vma=False,
    )
```

```python
import functools

import jax
import jax.numpy as jnp
from jax import lax
from jax.experimental import pallas as pl
from jax.experimental.pallas import tpu as pltpu
from jax.sharding import PartitionSpec as P

STATE = 128
SPAN = 128
D_SSM = 1024
EPSILON = 1e-06
HIGHEST = lax.Precision.HIGHEST

MESH = pl.DeviceIdType.MESH
HALO = 16
TOK_ROWS = 128
PIECE = 32
NT = (((1,), (1,)), ((), ()))
TN = (((0,), (0,)), ((), ()))
N_BLOCKS = 8
MSG = 64 + 16


def remote(src, dst, send, recv, where):
    return pltpu.make_async_remote_copy(
        src_ref=src, dst_ref=dst, send_sem=send, recv_sem=recv, device_id=where, device_id_type=MESH
    )


def silu(v):
    return v / (1.0 + jnp.exp(-v))


class Rings:

    def __init__(self, buf, cols, stride, sems, send_sem, place, sizes):
        self.buf, self.cols, self.stride = buf, cols, stride
        self.zp_sem, self.zm_sem, self.yp_sem, self.ym_sem, self.yo_sem = sems
        self.send_sem, self.sent = send_sem, []
        self.z, self.y = place
        self.n_sp, self.n_fs = sizes
        z, y, n_sp, n_fs = self.z, self.y, *sizes
        self.yp, self.ym, self.yo = (y + 1) % n_fs, (y + n_fs - 1) % n_fs, (y + 2) % n_fs
        self.to_yp, self.to_ym = {"fs": self.yp}, {"fs": self.ym}
        self.half = n_sp // 2

    def at(self, o, yy):
        zz = (self.z + self.n_sp - o) % self.n_sp
        row = pl.multiple_of((zz * self.n_fs + yy) * PIECE, PIECE)
        return self.buf.at[pl.ds(row, PIECE), pl.ds(*self.cols)]

    def send(self, ref, recv, where):
        copy = remote(ref, ref, self.send_sem.at[len(self.sent)], recv, where)
        copy.start()
        self.sent.append(copy)

    def arrived(self, ref, recv):
        remote(ref, ref, self.send_sem.at[0], recv, self.to_yp).wait_recv()

    def up(self, ref, k, stride):
        if k <= self.half:
            self.send(ref, self.zp_sem.at[k], {"sp": (self.z + stride) % self.n_sp})

    def down(self, ref, k, stride):
        if k < self.half:
            self.send(ref, self.zm_sem.at[k], {"sp": (self.z + self.n_sp - stride) % self.n_sp})

    def begin(self):
        own = self.at(0, self.y)
        for k in range(self.stride, 0, -1):
            self.up(own, k, k)
            self.down(own, k, k)

    def places(self, k):
        if k == 0:
            return (0,)
        return (k, self.n_sp - k) if k < self.half else (k,)

    def along_z(self, k):
        ref = self.at(k, self.y)
        self.arrived(ref, self.zp_sem.at[k])
        self.up(ref, k + self.stride, self.stride)
        if k < self.half:
            ref = self.at(self.n_sp - k, self.y)
            self.arrived(ref, self.zm_sem.at[k])
            self.down(ref, k + self.stride, self.stride)

    def along_y(self, k):
        for o in self.places(k):
            ref = self.at(o, self.y)
            self.send(ref, self.yp_sem.at[o], self.to_yp)
            self.send(ref, self.ym_sem.at[o], self.to_ym)

    def relay(self, k):
        for o in self.places(k):
            low, high = self.at(o, self.ym), self.at(o, self.yp)
            self.arrived(low, self.yp_sem.at[o])
            if o % 2 == 0:
                self.send(low, self.yo_sem.at[o], self.to_yp)
            self.arrived(high, self.ym_sem.at[o])
            if o % 2 == 1:
                self.send(high, self.yo_sem.at[o], self.to_ym)

    def finish(self):
        for o in range(self.n_sp):
            self.arrived(self.at(o, self.yo), self.yo_sem.at[o])


def mixer_kernel(
    n_sp, n_fs, n_x,
    tok, wg, wv, wk, wq, wp, wo_s, wo_p, wstep_in, gain_in,
    bias_in, rate_in, shift_in, tap_v_in, tap_k_in, tap_q_in, mgain_in, pmix_in, pgain_in,
    out,
    wstep, raw_t, gain, bias, rate, shift, tap_v, tap_k, tap_q, mgain, pmix, pgain, small_sem,
    tokbuf, normbuf, wbuf, obuf, gates, raw,
    p32, xbuf, kbuf, qbuf, ends, ybuf, mix,
    incl, excl, itot, etot, msg_out, msg_in, ss_out, ss_in, part_s, part_p, scales,
    d_out, d_in, r_out, r_in, n_out, n_in,
    local_sem, tp_sem, tm_sem, tr_sem, td_sem, h_sem, t_send,
    w_zp, w_zm, w_yp, w_ym, w_yo, w_send,
    o_zp, o_zm, o_yp, o_ym, o_yo, o_send,
    msg_send, msg_recv, ss_send, ss_recv, d_send, d_recv, r_send, r_recv, n_send, n_recv,
):
    f32, bf16 = jnp.float32, jnp.bfloat16
    z, y, t = lax.axis_index("sp"), lax.axis_index("fs"), lax.axis_index("tp")
    x, c = t // 2, t % 2
    n_tp = 2 * n_x
    xp, xm, xo = (x + 1) % n_x, (x + n_x - 1) % n_x, (x + 2) % n_x
    to_xp, to_xm, to_d = {"tp": xp * 2 + c}, {"tp": xm * 2 + c}, {"tp": x * 2 + 1 - c}
    to_zp, to_zm = {"sp": (z + 1) % n_sp}, {"sp": (z + n_sp - 1) % n_sp}
    distances = [1, 2, 4, 8]
    rows = N_BLOCKS * SPAN

    w_rings = Rings(
        wbuf, (0, 256), 2, (w_zp, w_zm, w_yp, w_ym, w_yo), w_send, (z, y), (n_sp, n_fs)
    )
    o_rings = Rings(
        obuf, (0, 640), 2, (o_zp, o_zm, o_yp, o_ym, o_yo), o_send, (z, y), (n_sp, n_fs)
    )

    def t_at(xx, cc, q=0, count=PIECE):
        row = pl.multiple_of(HALO + (xx * 2 + cc) * TOK_ROWS + q * PIECE, 16)
        return tokbuf.at[pl.ds(row, count), :]

    own_row = pl.ds(pl.multiple_of((z * n_fs + y) * PIECE, PIECE), PIECE)
    shards = (
        (wv, wbuf, 0), (wk, wbuf, 1), (wg, obuf, 0), (wq, obuf, 1), (wp, obuf, 2),
        (wo_s, obuf, 3), (wo_p, obuf, 4),
    )
    locals_ = [
        pltpu.make_async_copy(w, buf.at[own_row, pl.ds(i * 128, 128)], local_sem.at[n])
        for n, (w, buf, i) in enumerate(shards)
    ]
    locals_.append(pltpu.make_async_copy(tok.at[0], t_at(x, c, 0, TOK_ROWS), local_sem.at[7]))
    lane0 = pl.multiple_of(t * 128, 128)
    here = pl.ds(lane0, 128)
    small = [
        pltpu.make_async_copy(src, dst, small_sem.at[i])
        for i, (src, dst) in enumerate(
            (
                (gain_in, gain), (wstep_in, wstep),
                (bias_in, bias), (rate_in, rate), (shift_in, shift),
                (tap_v_in.at[:, here], tap_v), (tap_k_in.at[:, here], tap_k),
                (tap_q_in.at[:, here], tap_q), (mgain_in.at[:, here], mgain),
                (pmix_in.at[t], pmix), (pgain_in.at[:, here], pgain),
            )
        )
    ]
    for copy in locals_ + small:
        copy.start()

    barrier = pltpu.get_barrier_semaphore()
    partners = [
        to_xp, to_xm, to_d, to_zp, to_zm, {"sp": (z + 2) % n_sp}, {"sp": (z + n_sp - 2) % n_sp},
        w_rings.to_yp, w_rings.to_ym,
    ]
    for where in partners:
        pl.semaphore_signal(barrier, inc=1, device_id=where, device_id_type=MESH)
    for copy in small:
        copy.wait()
    pl.semaphore_wait(barrier, len(partners))

    t_sent = []

    def t_go(src, dst, recv, where):
        copy = remote(src, dst, t_send.at[len(t_sent)], recv, where)
        copy.start()
        t_sent.append(copy)

    def t_came(ref, recv):
        remote(ref, ref, t_send.at[0], recv, to_d).wait_recv()

    def relay_tokens(xx, q, recv, where, onward, slot):
        ref = t_at(xx, c, q)
        t_came(ref, recv)
        if onward:
            t_go(ref, ref, tr_sem.at[q], where)
        t_go(ref, ref, td_sem.at[slot + q], to_d)

    def norm_rows(begin, count):
        part = tokbuf[pl.ds(begin, count), :].astype(f32)
        scaling = lax.rsqrt(jnp.mean(part * part, axis=-1, keepdims=True) + EPSILON)
        normbuf[pl.ds(begin, count), :] = (part * scaling * gain[...]).astype(bf16)

    def norm_block(xx, cc):
        norm_rows(pl.multiple_of(HALO + (xx * 2 + cc) * TOK_ROWS, 16), TOK_ROWS)

    cs = 1 - c

    def token_step(k):
        if k <= 4:
            q = k - 1
            relay_tokens(xm, q, tp_sem.at[q], to_xp, q < 2, 0)
            q = (2, 3, 0, 1)[k - 1]
            relay_tokens(xp, q, tm_sem.at[q], to_xm, q >= 2, 4)
            if k == 2:
                norm_block(x, c)
            if k == 3:
                t_came(t_at(x, cs, 0, TOK_ROWS), td_sem.at[12])
                norm_block(x, cs)
        elif k <= 6:
            for q in (k - 5, k - 3):
                relay_tokens(xo, q, tr_sem.at[q], to_d, False, 8)
            norm_block(xm if k == 5 else xp, c)
        elif k == 7:
            for q in range(4):
                t_came(t_at(xm, cs, q), td_sem.at[q])
                t_came(t_at(xp, cs, q), td_sem.at[4 + q])
            norm_block(xm, cs)
            norm_block(xp, cs)
        else:
            norm_block(xo, c)

    for copy in locals_[:7]:
        copy.wait()
    w_rings.begin()
    locals_[7].wait()
    for q in (0, 1, 2, 3):
        t_go(t_at(x, c, q), t_at(x, c, q), tp_sem.at[q], to_xp)
    for q in (2, 3, 0, 1):
        t_go(t_at(x, c, q), t_at(x, c, q), tm_sem.at[q], to_xm)
    t_go(t_at(x, c, 0, TOK_ROWS), t_at(x, c, 0, TOK_ROWS), td_sem.at[12], to_d)
    w_rings.along_y(0)
    o_rings.begin()
    for i in range(16):
        cols = [wstep[r, :, i * 128 : (i + 1) * 128].astype(f32) for r in (0, 1)]
        tall_cols = jnp.concatenate([*cols, jnp.zeros((96, 128), f32)], axis=0).T
        wbuf[i * 128 : (i + 1) * 128, 256:384] = tall_cols.astype(bf16)
    steps_z = n_sp // 2
    for k in range(1, steps_z + 1):
        w_rings.along_z(k)
        w_rings.along_y(k)
        w_rings.relay(k - 1)
        token_step(k)
        if k > 1:
            o_rings.along_z(k - 1)
        if k > 1:
            o_rings.along_y(k - 2)
    def rounded(v):
        return v.astype(bf16).astype(f32)

    def dots(at, count, rhs):
        return jnp.dot(normbuf[pl.ds(at, count), :], rhs, preferred_element_type=f32)

    def project(xx):
        at = pl.multiple_of(xx * 256, 256)
        found = dots(pl.multiple_of(HALO + at, 16), 256, wbuf[...])
        p32[pl.ds(pl.multiple_of(HALO + at, 16), 256), 0:256] = rounded(found[:, 0:256])
        raw[pl.ds(at, 256), :] = found[:, 256:384]

    w_rings.relay(steps_z)
    o_rings.along_z(steps_z)
    for q in range(4):
        t_came(t_at(xo, cs, q), td_sem.at[8 + q])
    before, after = tokbuf.at[pl.ds(0, HALO), :], tokbuf.at[pl.ds(HALO + rows, HALO), :]
    t_go(tokbuf.at[pl.ds(rows, HALO), :], before, h_sem.at[0], to_zp)
    t_go(tokbuf.at[pl.ds(HALO, HALO), :], after, h_sem.at[1], to_zm)
    w_rings.finish()
    for xx in (x, xm, xp):
        project(xx)
    norm_block(xo, cs)
    for k in range(7, steps_z + 1):
        o_rings.along_y(k)

    project(xo)
    edges = ((0, z > 0), (HALO + rows, z < n_sp - 1))
    t_came(before, h_sem.at[0])
    t_came(after, h_sem.at[1])
    for begin, real in edges:
        norm_rows(begin, HALO)
        edge = dots(begin, HALO, wbuf[:, 0:256])
        p32[begin : begin + HALO, 0:256] = jnp.where(real, rounded(edge), 0.0)
    for k in range(3):
        o_rings.relay(k)

    row8 = lax.broadcasted_iota(jnp.int32, (8, 128), 0)

    def by_kind(parts):
        found = jnp.zeros((8, 128), f32)
        for i, part in enumerate(parts):
            found = jnp.where(row8 == i, part, found)
        return found

    kinds = ((0, 0), (0, 1), (1, 0), (1, 1))
    bias8 = by_kind([bias[r, 2 * t + h] for r, h in kinds])
    rate8 = by_kind([rate[r, 2 * t + h] for r, h in kinds])
    steps_l, logs_l = [], []
    for b in range(N_BLOCKS):
        raw_t[b] = raw[b * SPAN : (b + 1) * SPAN, :].T[0:32, :]
        cols = by_kind([raw_t[b, pl.ds(r * 16 + 2 * t + h, 1), :] for r, h in kinds]) + bias8
        steps = jnp.maximum(cols, 0.0) + jnp.log1p(jnp.exp(-jnp.abs(cols)))
        moved = by_kind([shift[0, h, r : r + 1, b * SPAN : (b + 1) * SPAN] for r, h in kinds])
        steps_l.append(steps)
        logs_l.append(jnp.where(row8 < 4, -rate8 * steps - moved, 0.0))
    steps = jnp.concatenate(steps_l, axis=0)
    logs = jnp.concatenate(logs_l, axis=0)
    lane = lax.broadcasted_iota(jnp.int32, (64, 128), 1)
    kind = lax.broadcasted_iota(jnp.int32, (64, 128), 0) % 8
    prefix, suffix = logs, logs
    for k in (1, 2, 4, 8, 16, 32, 64):
        prefix = prefix + jnp.where(lane >= k, pltpu.roll(prefix, k, 1), 0.0)
        suffix = suffix + jnp.where(lane < 128 - k, pltpu.roll(suffix, 128 - k, 1), 0.0)
    cum = jnp.where(kind < 2, prefix, suffix)
    total = jnp.broadcast_to(jnp.sum(logs, axis=1, keepdims=True), (64, 128))
    tail = jnp.exp(jnp.minimum(total - cum, 0.0)) * steps
    decay = jnp.exp(total)
    cum_tail_t = jnp.concatenate([cum, tail], axis=0).T
    reach_t = jnp.concatenate([jnp.exp(cum), jnp.zeros((64, 128), f32)], axis=0).T

    def wide(cols, b, first):
        j = b * 8 + first
        left = jnp.broadcast_to(cols[:, j : j + 1], (128, 64))
        right = jnp.broadcast_to(cols[:, j + 1 : j + 2], (128, 64))
        return jnp.concatenate([left, right], axis=1)

    def tall(rows_, b, first):
        j = b * 8 + first
        top = jnp.broadcast_to(rows_[j : j + 1, :], (64, 128))
        bottom = jnp.broadcast_to(rows_[j + 1 : j + 2, :], (64, 128))
        return jnp.concatenate([top, bottom], axis=0)

    def window(b, j):
        begin = HALO - 8 + b * SPAN
        return p32[begin : begin + SPAN + 16, j * 128 : (j + 1) * 128]

    def conv(b, j, taps):
        v = window(b, j)
        weights = taps[...].astype(f32)
        total_ = v * weights[2:3, :]
        for i in (0, 1, 3, 4):
            total_ = total_ + pltpu.roll(v, (2 - i) % (SPAN + 16), 0) * weights[i : i + 1, :]
        return silu(total_[8 : 8 + SPAN, :])

    for b in range(N_BLOCKS):
        at = slice(b * SPAN, (b + 1) * SPAN)
        values = conv(b, 0, tap_v)
        keys = conv(b, 1, tap_k).astype(bf16)
        xbuf[at, :] = values
        kbuf[at, :] = keys
        both = jnp.concatenate(
            [values * wide(cum_tail_t, b, 64), values * wide(cum_tail_t, b, 66)], axis=1
        )
        ends[b] = lax.dot_general(both.astype(bf16), keys, TN, preferred_element_type=f32)

    forward = ends[0, 0:128, :]
    backward = ends[N_BLOCKS - 1, 128:256, :]
    for i in range(1, N_BLOCKS):
        b = N_BLOCKS - 1 - i
        forward = forward * tall(decay, i, 0) + ends[i, 0:128, :]
        backward = backward * tall(decay, b, 2) + ends[b, 128:256, :]
    sums = total[0:8, :]
    for b in range(1, N_BLOCKS):
        sums = sums + total[b * 8 : b * 8 + 8, :]
    incl[0] = forward
    incl[1] = backward
    excl[...] = jnp.zeros_like(excl)
    itot[...] = jnp.broadcast_to(sums[None], (4, 8, 128))
    etot[...] = jnp.zeros_like(etot)

    def message(way, h, i, where):
        return remote(
            msg_out.at[way, h, i], msg_in.at[way, h, i],
            msg_send.at[way, h, i], msg_recv.at[way, h, i], where,
        )

    def exchange(i, h):
        d = distances[i]
        for way in (0, 1):
            ok = z + d < n_sp if way == 0 else z >= d
            logs8 = itot[2 * way + h]
            high = logs8.astype(bf16)
            low = (logs8 - high.astype(f32)).astype(bf16)
            msg_out[way, h, i, 0:64, :] = incl[way, h * 64 : (h + 1) * 64, :].astype(bf16)
            msg_out[way, h, i, 64:MSG, :] = jnp.concatenate([high, low], axis=0)
            where = {"sp": (z + d) % n_sp if way == 0 else (z + n_sp - d) % n_sp}

            @pl.when(ok)
            def _():
                message(way, h, i, where).start()

    def combine(i, h):
        d = distances[i]
        for way in (0, 1):
            ok = z >= d if way == 0 else z + d < n_sp
            s, r, part = 2 * way + h, 2 * way + h, slice(h * 64, (h + 1) * 64)

            @pl.when(ok)
            def _():
                message(way, h, i, to_d).wait_recv()
                state = msg_in[way, h, i, 0:64, :].astype(f32)
                pair = msg_in[way, h, i, 64:MSG, :].astype(f32)
                logs8 = pair[0:8, :] + pair[8:16, :]
                incl[way, part, :] = incl[way, part, :] + jnp.exp(itot[s][r : r + 1, :]) * state
                itot[s] = itot[s] + logs8
                excl[way, part, :] = excl[way, part, :] + jnp.exp(etot[s][r : r + 1, :]) * state
                etot[s] = etot[s] + logs8

    row = lax.broadcasted_iota(jnp.int32, (128, 128), 0)
    col = lax.broadcasted_iota(jnp.int32, (128, 128), 1)

    def within(b):
        at = slice(b * SPAN, (b + 1) * SPAN)
        queries = conv(b, 2, tap_q).astype(bf16)
        qbuf[at, :] = queries
        scores = lax.dot_general(queries, kbuf[at, :], NT, preferred_element_type=f32)
        masked = []
        for h in (0, 1):
            jf, jb = b * 8 + h, b * 8 + 2 + h
            ahead = cum_tail_t[:, jf : jf + 1] - cum[jf : jf + 1, :]
            behind = cum_tail_t[:, jb : jb + 1] - cum[jb : jb + 1, :]
            gaps = jnp.where(col < row, ahead, jnp.where(col > row, behind, 0.0))
            df, db = steps[jf : jf + 1, :], steps[jb : jb + 1, :]
            sizes = jnp.where(col < row, df, jnp.where(col > row, db, df + db))
            masked.append((scores * jnp.exp(jnp.minimum(gaps, 0.0)) * sizes).astype(bf16))
        values = xbuf[at, :]
        stacked = jnp.concatenate(
            [jnp.where(col < 64, values, 0.0), jnp.where(col >= 64, values, 0.0)], axis=0
        ).astype(bf16)
        ybuf[at, :] = jnp.dot(
            jnp.concatenate(masked, axis=1), stacked, preferred_element_type=f32
        )

    def pool(b):
        at = slice(b * SPAN, (b + 1) * SPAN)
        n = SPAN + 16
        v = window(b, 3)
        w2 = v + pltpu.roll(v, 1, 0)
        w4 = pltpu.roll(w2, 1, 0) + pltpu.roll(w2, n - 1, 0)
        w8 = pltpu.roll(w4, 2, 0) + pltpu.roll(w4, n - 2, 0)
        w16 = pltpu.roll(w8, 4, 0) + pltpu.roll(w8, n - 4, 0)
        which = t % 4
        summed = jnp.where(
            which == 0, w2, jnp.where(which == 1, w4, jnp.where(which == 2, w8, w16))
        )[8 : 8 + SPAN, :]
        reach = jnp.where(which == 0, 1, jnp.where(which == 1, 2, jnp.where(which == 2, 4, 8)))
        place = z * rows + b * SPAN + row
        upper = jnp.minimum(place + reach, n_sp * rows)
        lower = jnp.maximum(place - reach, 0)
        differences = summed / (upper - lower).astype(f32) - v[8 : 8 + SPAN, :]
        mapped = jnp.dot(differences.astype(bf16), pmix[...], preferred_element_type=f32)
        mix[at, 128:256] = (mapped * pgain[...]).astype(bf16)

    def turn(i):
        for h in (0, 1):
            combine(i, h)
            if i + 1 < len(distances):
                exchange(i + 1, h)

    exchange(0, 0)
    exchange(0, 1)
    o_rings.relay(3)
    o_rings.relay(4)
    turn(0)
    o_rings.relay(5)
    o_rings.relay(6)
    turn(1)
    o_rings.relay(7)
    o_rings.relay(8)
    o_rings.finish()
    turn(2)
    for i in range(4):
        at = HALO + i * 256
        found = dots(at, 256, obuf[:, 0:384])
        gates[i * 256 : (i + 1) * 256, :] = found[:, 0:128].astype(bf16)
        p32[at : at + 256, 256:512] = rounded(found[:, 128:384])
    for begin, real in edges:
        edge = dots(begin, HALO, obuf[:, 128:384])
        p32[begin : begin + HALO, 256:512] = jnp.where(real, rounded(edge), 0.0)
    for b in range(N_BLOCKS):
        within(b)
    for b in range(N_BLOCKS):
        pool(b)
    order = (xo, xp, xm, x)
    for i, xx in enumerate(order):
        pair = pl.ds(pl.multiple_of(xx * 2 * TOK_ROWS, 2 * TOK_ROWS), 2 * TOK_ROWS)
        part_p[i] = lax.dot_general(
            mix[pair, 128:256], obuf[:, 512:640], NT, preferred_element_type=f32
        )
    turn(3)

    forward, backward = excl[0], excl[1]
    entering = [None] * N_BLOCKS
    leaving = [None] * N_BLOCKS
    for i in range(N_BLOCKS):
        b = N_BLOCKS - 1 - i
        entering[i] = forward.astype(bf16)
        leaving[b] = backward.astype(bf16)
        forward = forward * tall(decay, i, 0) + ends[i, 0:128, :]
        backward = backward * tall(decay, b, 2) + ends[b, 128:256, :]
    squares = jnp.zeros((128, 128), f32)
    for b in range(N_BLOCKS):
        at = slice(b * SPAN, (b + 1) * SPAN)
        states = jnp.concatenate([entering[b], leaving[b]], axis=0)
        carried = lax.dot_general(qbuf[at, :], states, NT, preferred_element_type=f32)
        heads_out = (
            ybuf[at, :]
            + carried[:, 0:128] * wide(reach_t, b, 0)
            + carried[:, 128:256] * wide(reach_t, b, 2)
        )
        gated = heads_out * silu(gates[at, :].astype(f32))
        mix[at, 0:128] = (gated * mgain[...]).astype(bf16)
        summed = jnp.sum(gated * gated, axis=1, keepdims=True)
        squares = jnp.where(col == b, summed, squares)
    own_squares = squares.T[0:8, :]
    ss_out[...] = own_squares
    ss_copies = []
    for r in range(1, n_tp):
        copy = remote(
            ss_out, ss_in.at[r - 1], ss_send.at[r - 1], ss_recv.at[r - 1],
            {"tp": (t + r) % n_tp},
        )
        copy.start()
        ss_copies.append(copy)
    for i, xx in enumerate(order):
        pair = pl.ds(pl.multiple_of(xx * 2 * TOK_ROWS, 2 * TOK_ROWS), 2 * TOK_ROWS)
        part_s[i] = lax.dot_general(
            mix[pair, 0:128], obuf[:, 384:512], NT, preferred_element_type=f32
        )
    all_squares = own_squares
    for r in range(1, n_tp):
        ss_copies[r - 1].wait_recv()
        all_squares = all_squares + ss_in[r - 1]
    scale = lax.rsqrt(all_squares / D_SSM + EPSILON)
    scale_t = jnp.concatenate([scale, jnp.zeros((120, 128), f32)], axis=0).T
    for b in range(N_BLOCKS):
        scales[b * SPAN : (b + 1) * SPAN, :] = jnp.broadcast_to(scale_t[:, b : b + 1], (128, 128))

    def partial(i, cc, begin=0, count=TOK_ROWS):
        at = pl.multiple_of(cc * TOK_ROWS + begin, 16)
        there = pl.multiple_of(order[i] * 2 * TOK_ROWS + at, 16)
        scaling = scales[pl.ds(there, count), :][:, 0:1]
        return part_s[i, pl.ds(at, count), :] * scaling + part_p[i, pl.ds(at, count), :]

    half = TOK_ROWS // 2
    d_copies = []
    for i in range(4):
        d_out[i] = partial(i, 1 - c).astype(bf16)
        copy = remote(d_out.at[i], d_in.at[i], d_send.at[i], d_recv.at[i], to_d)
        copy.start()
        d_copies.append(copy)

    def chip(i, begin, count=half):
        return partial(i, c, begin, count) + d_in[i, begin : begin + count, :].astype(f32)

    def send(i, value, where, out_ref, in_ref, send_sem, recv_sem):
        out_ref[i] = value.astype(bf16)
        copy = remote(out_ref.at[i], in_ref.at[i], send_sem.at[i], recv_sem.at[i], where)
        copy.start()
        return copy

    relay = (r_out, r_in, r_send, r_recv)
    near = (n_out, n_in, n_send, n_recv)
    d_copies[0].wait_recv()
    relay_p = send(0, chip(0, 0), to_xp, *relay)
    relay_m = send(1, chip(0, half), to_xm, *relay)
    d_copies[1].wait_recv()
    dir_p = send(0, chip(1, half), to_xp, *near)
    d_copies[2].wait_recv()
    dir_m = send(1, chip(2, 0), to_xm, *near)
    relay_p.wait_recv()
    comb_p = send(2, chip(1, 0) + r_in[0].astype(f32), to_xp, *near)
    relay_m.wait_recv()
    comb_m = send(3, chip(2, half) + r_in[1].astype(f32), to_xm, *near)
    d_copies[3].wait_recv()
    top, bottom = chip(3, 0), chip(3, half)
    dir_p.wait_recv()
    dir_m.wait_recv()
    bottom = bottom + n_in[0].astype(f32)
    top = top + n_in[1].astype(f32)
    comb_p.wait_recv()
    out[0, 0:half, :] = (top + n_in[2].astype(f32)).astype(bf16)
    comb_m.wait_recv()
    out[0, half:TOK_ROWS, :] = (bottom + n_in[3].astype(f32)).astype(bf16)

    for i, d in enumerate(distances):
        for way in (0, 1):
            ok = z + d < n_sp if way == 0 else z >= d

            @pl.when(ok)
            def _():
                for h in (0, 1):
                    message(way, h, i, to_d).wait_send()

    last = [relay_p, relay_m, dir_p, dir_m, comb_p, comb_m]
    for copy in t_sent + w_rings.sent + o_rings.sent + ss_copies + d_copies + last:
        copy.wait_send()


N_TOKEN_SENDS = 27
N_RING_SENDS = 66


def mixer(n_sp, n_fs, n_x, *operands):
    any_spec = pl.BlockSpec(memory_space=pl.ANY)
    vmem = pl.BlockSpec(memory_space=pltpu.VMEM)
    dma = pltpu.SemaphoreType.DMA
    f32, bf16 = jnp.float32, jnp.bfloat16
    rows = N_BLOCKS * SPAN
    half = TOK_ROWS // 2

    def ring_sems(counts):
        return [dma((n,)) for n in counts]

    return pl.pallas_call(
        functools.partial(mixer_kernel, n_sp, n_fs, n_x),
        out_shape=jax.ShapeDtypeStruct((1, TOK_ROWS, 2048), bf16),
        in_specs=[any_spec] * 19,
        out_specs=vmem,
        scratch_shapes=[
            pltpu.VMEM((2, 16, 2048), bf16),
            pltpu.VMEM((N_BLOCKS, 32, 128), f32),
            pltpu.VMEM((1, 2048), f32),
            pltpu.SMEM((2, 16), f32),
            pltpu.SMEM((2, 16), f32),
            pltpu.VMEM((1, 2, 2, 1024), f32),
            pltpu.VMEM((5, 128), bf16),
            pltpu.VMEM((5, 128), bf16),
            pltpu.VMEM((5, 128), bf16),
            pltpu.VMEM((1, 128), f32),
            pltpu.VMEM((128, 128), bf16),
            pltpu.VMEM((1, 128), f32),
            dma((11,)),
            pltpu.VMEM((rows + 2 * HALO, 2048), bf16),
            pltpu.VMEM((rows + 2 * HALO, 2048), bf16),
            pltpu.VMEM((2048, 384), bf16),
            pltpu.VMEM((2048, 640), bf16),
            pltpu.VMEM((rows, 128), bf16),
            pltpu.VMEM((rows, 128), f32),
            pltpu.VMEM((rows + 2 * HALO, 512), f32),
            pltpu.VMEM((rows, 128), f32),
            pltpu.VMEM((rows, 128), bf16),
            pltpu.VMEM((rows, 128), bf16),
            pltpu.VMEM((N_BLOCKS, 256, 128), f32),
            pltpu.VMEM((rows, 128), f32),
            pltpu.VMEM((rows, 256), bf16),
            pltpu.VMEM((2, 128, 128), f32),
            pltpu.VMEM((2, 128, 128), f32),
            pltpu.VMEM((4, 8, 128), f32),
            pltpu.VMEM((4, 8, 128), f32),
            pltpu.VMEM((2, 2, 4, MSG, 128), bf16),
            pltpu.VMEM((2, 2, 4, MSG, 128), bf16),
            pltpu.VMEM((8, 128), f32),
            pltpu.VMEM((7, 8, 128), f32),
            pltpu.VMEM((4, 2 * TOK_ROWS, 2048), f32),
            pltpu.VMEM((4, 2 * TOK_ROWS, 2048), f32),
            pltpu.VMEM((rows, 128), f32),
            pltpu.VMEM((4, TOK_ROWS, 2048), bf16),
            pltpu.VMEM((4, TOK_ROWS, 2048), bf16),
            pltpu.VMEM((2, half, 2048), bf16),
            pltpu.VMEM((2, half, 2048), bf16),
            pltpu.VMEM((4, half, 2048), bf16),
            pltpu.VMEM((4, half, 2048), bf16),
            dma((8,)), dma((4,)), dma((4,)), dma((4,)), dma((13,)), dma((2,)),
            dma((N_TOKEN_SENDS,)),
            *ring_sems((9, 9, 16, 16, 16, N_RING_SENDS)),
            *ring_sems((9, 9, 16, 16, 16, N_RING_SENDS)),
            dma((2, 2, 4)), dma((2, 2, 4)), dma((7,)), dma((7,)),
            dma((4,)), dma((4,)), dma((2,)), dma((2,)), dma((4,)), dma((4,)),
        ],
        compiler_params=pltpu.CompilerParams(
            collective_id=0, has_side_effects=True, vmem_limit_bytes=56 * 1024 * 1024
        ),
        name="mixer",
    )(*operands)


def local(
    tokens, norm_gain, w_gate, w_value, w_bkey, w_query, w_pool_in, w_step, step_bias,
    decay_rate, decay_shift, conv_value, conv_bkey, conv_query, mix_gain, pool_mix, pool_gain,
    w_out_ssd, w_out_pool,
):
    n_tp, n_sp, n_fs = lax.axis_size("tp"), lax.axis_size("sp"), lax.axis_size("fs")
    return mixer(
        n_sp, n_fs, n_tp // 2, tokens, w_gate, w_value, w_bkey, w_query, w_pool_in,
        w_out_ssd.T, w_out_pool.T, w_step.transpose(1, 2, 0), norm_gain[None], step_bias, decay_rate, decay_shift,
        conv_value, conv_bkey, conv_query, mix_gain[None], pool_mix, pool_gain[None],
    )


def solution(mesh):
    return jax.shard_map(
        local,
        mesh=mesh,
        in_specs=(
            P("fs", ("sp", "tp"), None),
            P(),
            P(("sp", "fs"), "tp"),
            P(("sp", "fs"), "tp"),
            P(("sp", "fs"), "tp"),
            P(("sp", "fs"), "tp"),
            P(("sp", "fs"), "tp"),
            P(),
            P(),
            P(),
            P("fs", "tp", None, "sp"),
            P(),
            P(),
            P(),
            P(),
            P(),
            P(),
            P("tp", ("sp", "fs")),
            P("tp", ("sp", "fs")),
        ),
        out_specs=P("fs", ("sp", "tp"), None),
        check_vma=False,
    )
```
